512 devices in a mesh: sp: 128 (over z, y, core), tp: 4 (over x).
Axes of the slice: x: 4, y: 8, z: 8, core: 2. Of those that a mesh axis runs over, the one named last changes fastest.
Arguments:
- stream: bfloat16 [32768, 2048], P('sp', 'tp'), may hold values from -6 to 6
- norm_gain: float32 [2, 2048], replicated, may hold values from 0.1 to 1.9
- w_value: bfloat16 [2, 2048, 1024], P(None, 'sp', 'tp'), may hold values from -0.125 to 0.125
- w_gate: bfloat16 [2, 2048, 1024], P(None, 'sp', 'tp'), may hold values from -0.125 to 0.125
- conv_taps: float32 [2, 128, 1024], P(None, None, 'tp'), as said below
- channel_gain: float32 [2, 1024], P(None, 'tp'), may hold values from 0.1 to 1.9
- w_out: bfloat16 [2, 1024, 2048], P(None, 'tp', 'sp'), may hold values from -0.1875 to 0.1875
Outputs:
- result: bfloat16 [32768, 2048], P('sp', 'tp')
The draws below stay inside these ranges and needn't reach their ends.
Inputs may be any that keep to these rules, and one draw needn't show every extreme that they name: `conv_taps`: taps of each block of 128 consecutive channels share a scale factor of its own.
All inputs are finite; a program needn't handle non-finite values.
Results may differ from the reference program's by a relative error of at most 0.012.
Values may be sent and summed in bfloat16 or wider, within the bound.
No kernel may reach another device: no remote copies, remote signals or barrier semaphores. Data moves between devices by JAX's collectives and lax.ppermute only.
A program may use at most 64 MiB of HBM per device.

```python
import jax
import jax.numpy as jnp
from jax import lax

D = 2048
C = 1024
KW = 128
LAYERS = 2
TOKENS = 32768


def draw_conv_taps(key, part):
    first, second = jax.random.split(key)
    base = jax.random.normal(first, (LAYERS, KW, 8, C // 8), jnp.float32)
    scales = jnp.exp(jax.random.uniform(second, (LAYERS, 1, 8, 1), jnp.float32, -1.2039728, 1.0986123))
    taps = base * scales * KW ** (-0.5)
    return taps.reshape(LAYERS, KW, C).astype(jnp.float32)


def shard_levels(key, dims, pieces, least, high):
    level, own = 1.0, jax.random.fold_in(key, 6)
    for axis_at, blocks in pieces:
        draws = jnp.exp(jax.random.uniform(jax.random.fold_in(own, axis_at), (blocks,), jnp.float32, least / len(pieces), high / len(pieces)))
        level = level * jnp.repeat(draws, dims[axis_at] // blocks).reshape([-1 if axis == axis_at else 1 for axis in range(len(dims))])
    return level


def normal_values(key, extent, scale, limit, cuts=(), held_as=jnp.bfloat16):
    factor_of = shard_levels(key, extent, cuts, -0.22, 0.18) if cuts else 1.0
    values = jax.random.normal(key, extent, jnp.float32) * scale * factor_of
    return jnp.minimum(jnp.maximum(values, -limit), limit).astype(held_as)


def setup_inputs(seed: int = 0) -> dict:
    key_list = jax.random.split(jax.random.key(seed), 8)
    stream = normal_values(key_list[0], (TOKENS, D), 1.0, 6.0, ((0, 128), (1, 4)))
    norm_gain = jnp.clip(1.0 + 0.18 * jax.random.normal(key_list[1], (LAYERS, D), jnp.float32), 0.1, 1.9)
    w_value = normal_values(key_list[2], (LAYERS, D, C), D ** -0.5, 0.125, ((1, 128), (2, 4)))
    w_gate = normal_values(key_list[3], (LAYERS, D, C), D ** -0.5, 0.125, ((1, 128), (2, 4)))
    conv_taps = draw_conv_taps(jax.random.fold_in(key_list[7], 71), 0)
    channel_gain = jnp.clip(1.0 + 0.18 * jax.random.normal(key_list[5], (LAYERS, C), jnp.float32), 0.1, 1.9)
    w_out = normal_values(key_list[6], (LAYERS, C, D), C ** -0.5, 0.1875, ((1, 4), (2, 128)))
    return {"stream": stream, "norm_gain": norm_gain, "w_value": w_value, "w_gate": w_gate, "conv_taps": conv_taps, "channel_gain": channel_gain, "w_out": w_out}


def causal_conv(glu, taps):
    padded = jnp.concatenate([jnp.zeros((KW - 1, C), jnp.float32), glu.astype(jnp.float32)], axis=0)

    def add_tap(index, total):
        offset = jnp.asarray(index).astype(jnp.int32)
        window = lax.dynamic_slice_in_dim(padded, offset, TOKENS, 0)
        row = lax.dynamic_slice_in_dim(taps, offset, 1, 0)
        return total + window * row
    return lax.fori_loop(0, KW, add_tap, jnp.zeros((TOKENS, C), jnp.float32))

def reference(stream, norm_gain, w_value, w_gate, conv_taps, channel_gain, w_out):
    x = stream
    for layer in range(LAYERS):
        xf = x.astype(jnp.float32)
        normed = (xf * lax.rsqrt(lax.optimization_barrier(jnp.mean(xf * xf, axis=1, keepdims=True)) + 1e-06) * norm_gain[layer]).astype(jnp.bfloat16)
        value = jnp.dot(normed, w_value[layer], preferred_element_type=jnp.float32)
        gate = jnp.dot(normed, w_gate[layer], preferred_element_type=jnp.float32)
        glu = (value * jax.nn.sigmoid(gate)).astype(jnp.bfloat16)
        conv = causal_conv(glu, conv_taps[layer])
        mean = lax.optimization_barrier(jnp.mean(conv, axis=1, keepdims=True))
        centred = conv - mean
        spread = lax.optimization_barrier(jnp.mean(centred * centred, axis=1, keepdims=True))
        act = jax.nn.silu(centred * lax.rsqrt(spread + 1e-05) * channel_gain[layer]).astype(jnp.bfloat16)
        branch = jnp.dot(act, w_out[layer], preferred_element_type=jnp.float32)
        x = (xf + branch).astype(jnp.bfloat16)
    return x
```

```python
import jax
import jax.numpy as jnp
from jax import lax
from jax.sharding import Mesh
from jax.sharding import PartitionSpec as P

C = 1024
LAYERS = 2
SP = ("z", "y", "c")
BF = jnp.bfloat16
F32 = jnp.float32


def spread_copies(block, axes):
    n = lax.axis_size(axes)
    copies = jnp.broadcast_to(block, (n, *block.shape))
    return lax.all_to_all(copies, axes, split_axis=0, concat_axis=0, tiled=True)


def swap_cores(v):
    return lax.ppermute(v, "c", [(0, 1), (1, 0)])


def by_core(first, mine, other):
    return jnp.where(first, mine, other), jnp.where(first, other, mine)


def to_column_owner(v, flip):
    nz, nc, nx = lax.axis_size("z"), lax.axis_size("c"), lax.axis_size("x")
    nb = nz // nx
    pairs = []
    for z in range(nz):
        for c in range(nc):
            for x in range(nx):
                a, b = divmod(z, nb)
                to = ((x * nb + b) * nc + (c ^ flip)) * nx + a
                pairs.append(((z * nc + c) * nx + x, to))
    return lax.ppermute(v, ("z", "c", "x"), pairs)


def split_three(v):
    hi = lax.reduce_precision(v, 8, 7)
    rest = v - hi
    mid = lax.reduce_precision(rest, 8, 7)
    return jnp.stack([hi, mid, rest - mid]).astype(BF)


def shards(stream, norm_gain, w_value, w_gate, conv_taps, channel_gain, w_out):
    x = stream
    tokens = stream.shape[0]
    ch = w_value.shape[2]
    taps = conv_taps.shape[1]
    nx = lax.axis_size("x")
    first = lax.axis_index("c") == 0

    keep, send = by_core(first, w_value, w_gate)
    top, bottom = by_core(first, keep, swap_cores(send))
    half_proj = jnp.concatenate([top, bottom], axis=1)

    out_t = jnp.swapaxes(w_out, 1, 2)
    keep, send = by_core(first, out_t[:, :, : ch // 2], out_t[:, :, ch // 2 :])
    top, bottom = by_core(first, to_column_owner(keep, 0), to_column_owner(send, 1))
    half_out = jnp.concatenate([top, bottom], axis=1)

    for layer in range(LAYERS):
        proj_mine = spread_copies(half_proj[layer], ("z", "y")).reshape(-1, ch)
        proj_other = swap_cores(proj_mine)
        out_mine = spread_copies(half_out[layer], ("z", "y")).reshape(nx, -1, ch // 2)
        out_other = swap_cores(out_mine)

        whole = spread_copies(x, "x").astype(F32)
        mean_sq = jnp.sum(whole * whole, axis=(0, 2), keepdims=True) / (nx * x.shape[1])
        normed = whole * lax.rsqrt(mean_sq + 1e-06) * norm_gain[layer].reshape(nx, 1, -1)
        normed = jnp.moveaxis(normed.astype(BF), 0, 1).reshape(tokens, -1)
        a = jnp.dot(normed, proj_mine, preferred_element_type=F32)
        b = jnp.dot(normed, proj_other, preferred_element_type=F32)
        value, gate = by_core(first, a, b)
        glu = (value * jax.nn.sigmoid(gate)).astype(BF)
        count = lax.axis_size(SP)
        before = lax.ppermute(glu[tokens - taps :], SP, [(i, i + 1) for i in range(count - 1)])
        padded = jnp.concatenate([before[1:], glu], axis=0).astype(F32)
        conv = lax.conv_general_dilated(
            padded[None],
            conv_taps[layer][:, None, :],
            (1,),
            "VALID",
            dimension_numbers=("NWC", "WIO", "NWC"),
            feature_group_count=ch,
            precision=lax.Precision.HIGHEST,
        )[0]
        mean_here = jnp.mean(conv, axis=1)
        centred = (conv - mean_here[:, None]).astype(BF)
        extra = jnp.concatenate(
            [split_three(mean_here), split_three(channel_gain[layer]), jnp.zeros((10, ch), BF)]
        )
        everyone = spread_copies(jnp.concatenate([centred, extra]), "x")
        tail = everyone[:, tokens:].astype(F32)
        means = tail[:, 0] + tail[:, 1] + tail[:, 2]
        gains = tail[:, 3] + tail[:, 4] + tail[:, 5]
        shift = means - jnp.mean(means, axis=0)
        centred = everyone[:, :tokens].astype(F32) + shift[:, :, None]
        spread = jnp.sum(centred * centred, axis=(0, 2)) / C
        act = jax.nn.silu(centred * lax.rsqrt(spread + 1e-05)[None, :, None] * gains[:, None, :]).astype(BF)
        act_mine, act_other = by_core(first, act[:, :, : ch // 2], act[:, :, ch // 2 :])
        branch = jnp.einsum("ktr,knr->tn", act_mine, out_mine, preferred_element_type=F32)
        branch += jnp.einsum("ktr,knr->tn", act_other, out_other, preferred_element_type=F32)
        x = (x.astype(F32) + branch).astype(BF)
    return x


def solution(mesh):
    finer = Mesh(mesh.devices.reshape(8, 8, 2, mesh.shape["tp"]), ("z", "y", "c", "x"))
    in_specs = (
        P(SP, "x"),
        P(),
        P(None, SP, "x"),
        P(None, SP, "x"),
        P(None, None, "x"),
        P(None, "x"),
        P(None, "x", SP),
    )
    return jax.shard_map(shards, mesh=finer, in_specs=in_specs, out_specs=P(SP, "x"), check_vma=False)
```

```python
import jax
import jax.numpy as jnp
from jax import lax
from jax.sharding import Mesh
from jax.sharding import PartitionSpec as P

C = 1024
LAYERS = 2
NZ, NY = 8, 8
BF = jnp.bfloat16
F32 = jnp.float32


def at(z, y, c):
    return (z * NY + y) * 2 + c


ALONG_Y = [[at(z, y, 0) for y in range(NY)] for z in range(NZ)]
ALONG_Z = [[at(z, y, 1) for z in range(NZ)] for y in range(NY)]
ALONG_Y1 = [[at(z, y, 1) for y in range(NY)] for z in range(NZ)]
ALONG_Z0 = [[at(z, y, 0) for z in range(NZ)] for y in range(NY)]


def to_group(block, groups):
    n = len(groups[0])
    copies = jnp.broadcast_to(block, (n, *block.shape))
    return lax.all_to_all(
        copies, "sp", split_axis=0, concat_axis=0, tiled=True, axis_index_groups=groups
    )


def lines(block):
    return to_group(block, ALONG_Y + ALONG_Z)


def plane(once):
    return to_group(once, ALONG_Z0 + ALONG_Y1)


def after(v, earlier):
    return lax.optimization_barrier((v, earlier))[0]


def swap_cores(v):
    count = lax.axis_size("sp")
    return lax.ppermute(v, "sp", [(i, i ^ 1) for i in range(count)])


def by_core(first, mine, other):
    return jnp.where(first, mine, other), jnp.where(first, other, mine)


def to_column_owner(v, flip):
    nx = lax.axis_size("x")
    nb = NZ // nx
    pairs = []
    for z in range(NZ):
        a, b = divmod(z, nb)
        for y in range(NY):
            for c in range(2):
                for x in range(nx):
                    half = c ^ flip
                    place = (x * nb + b, y) if half == 0 else (y, x * nb + b)
                    pairs.append((at(z, y, c) * nx + x, at(*place, half) * nx + a))
    return lax.ppermute(v, ("sp", "x"), pairs)


def from_all_x(v):
    nx = lax.axis_size("x")
    here = lax.axis_index("x")
    parts = [v]
    for step in range(1, nx):
        parts.append(lax.ppermute(v, "x", [(i, (i + step) % nx) for i in range(nx)]))
    ordered = []
    for owner in range(nx):
        step = (here - owner) % nx
        part = parts[nx - 1]
        for k in range(nx - 1):
            part = jnp.where(step == k, parts[k], part)
        ordered.append(part)
    return jnp.stack(ordered)


def split_three(v):
    hi = lax.reduce_precision(v, 8, 7)
    rest = v - hi
    mid = lax.reduce_precision(rest, 8, 7)
    return jnp.stack([hi, mid, rest - mid]).astype(BF)


def shards(stream, norm_gain, w_value, w_gate, conv_taps, channel_gain, w_out):
    x = stream
    tokens = stream.shape[0]
    ch = w_value.shape[2]
    taps = conv_taps.shape[1]
    nx = lax.axis_size("x")
    rows = 2 * w_value.shape[1]
    first = lax.axis_index("sp") % 2 == 0

    keep, send = by_core(first, w_value, w_gate)
    top, bottom = by_core(first, keep, swap_cores(send))
    half_proj = jnp.concatenate([top, bottom], axis=1)
    out_t = jnp.swapaxes(w_out, 1, 2)
    keep, send = by_core(first, out_t[:, :, : ch // 2], out_t[:, :, ch // 2 :])
    left, right = by_core(first, to_column_owner(keep, 0), to_column_owner(send, 1))
    half_out = jnp.concatenate([left, right], axis=2)
    blocks = jnp.concatenate([half_proj, half_out], axis=1)

    def proj_of(w):
        return w[:, :rows].reshape(NZ * NY * rows, ch)

    def out_of(w):
        w = w[:, rows:].reshape(nx, -1, rows // 2, 2, ch // 2)
        return jnp.swapaxes(w, 2, 3).reshape(nx, -1, ch // 2)

    gathered = plane(lines(blocks[0]))
    for layer in range(LAYERS):
        following = lines(after(blocks[layer + 1], gathered)) if layer + 1 < LAYERS else None
        mine = gathered.reshape(NZ, NY, *blocks.shape[1:])
        turned = jnp.swapaxes(mine[:, :, :rows], 0, 1)
        proj = jnp.where(first, mine[:, :, :rows], turned)
        mine = jnp.concatenate([proj, mine[:, :, rows:]], axis=2).reshape(-1, *blocks.shape[1:])
        other = swap_cores(mine)

        whole = from_all_x(x).astype(F32)
        mean_sq = jnp.sum(whole * whole, axis=(0, 2), keepdims=True) / (nx * x.shape[1])
        normed = whole * lax.rsqrt(mean_sq + 1e-06) * norm_gain[layer].reshape(nx, 1, -1)
        normed = jnp.moveaxis(normed.astype(BF), 0, 1).reshape(tokens, -1)
        a = jnp.dot(normed, proj_of(mine), preferred_element_type=F32)
        b = jnp.dot(normed, proj_of(other), preferred_element_type=F32)
        value, gate = by_core(first, a, b)
        glu = (value * jax.nn.sigmoid(gate)).astype(BF)
        if layer + 1 < LAYERS:
            gathered = plane(after(following, glu))
        count = lax.axis_size("sp")
        before = lax.ppermute(glu[tokens - taps :], "sp", [(i, i + 1) for i in range(count - 1)])
        padded = jnp.concatenate([before[1:], glu], axis=0).astype(F32)
        conv = lax.conv_general_dilated(
            padded[None],
            conv_taps[layer][:, None, :],
            (1,),
            "VALID",
            dimension_numbers=("NWC", "WIO", "NWC"),
            feature_group_count=ch,
            precision=lax.Precision.HIGHEST,
        )[0]
        mean_here = jnp.mean(conv, axis=1)
        centred = (conv - mean_here[:, None]).astype(BF)
        extra = jnp.concatenate(
            [split_three(mean_here), split_three(channel_gain[layer]), jnp.zeros((10, ch), BF)]
        )
        everyone = from_all_x(jnp.concatenate([centred, extra]))
        tail = everyone[:, tokens:].astype(F32)
        means = tail[:, 0] + tail[:, 1] + tail[:, 2]
        gains = tail[:, 3] + tail[:, 4] + tail[:, 5]
        shift = means - jnp.mean(means, axis=0)
        centred = everyone[:, :tokens].astype(F32) + shift[:, :, None]
        spread = jnp.sum(centred * centred, axis=(0, 2)) / C
        act = jax.nn.silu(centred * lax.rsqrt(spread + 1e-05)[None, :, None] * gains[:, None, :]).astype(BF)
        act_mine, act_other = by_core(first, act[:, :, : ch // 2], act[:, :, ch // 2 :])
        branch = jnp.einsum("ktr,knr->tn", act_mine, out_of(mine), preferred_element_type=F32)
        branch += jnp.einsum("ktr,knr->tn", act_other, out_of(other), preferred_element_type=F32)
        x = (x.astype(F32) + branch).astype(BF)
    return x


def solution(mesh):
    flat = Mesh(mesh.devices, ("sp", "x"))
    in_specs = (
        P("sp", "x"),
        P(),
        P(None, "sp", "x"),
        P(None, "sp", "x"),
        P(None, None, "x"),
        P(None, "x"),
        P(None, "x", "sp"),
    )
    return jax.shard_map(shards, mesh=flat, in_specs=in_specs, out_specs=P("sp", "x"), check_vma=False)
```

```python
import jax
import jax.numpy as jnp
from jax import lax
from jax.experimental import pallas as pl
from jax.experimental.pallas import tpu as pltpu
from jax.sharding import Mesh
from jax.sharding import PartitionSpec as P


C = 1024
LAYERS = 2
NZ, NY, NX = 8, 8, 4
TOK, CH, TAPS, FEAT = 256, 256, 128, 512
ROWS = 32
PACK = TOK + 16
BF = jnp.bfloat16
F32 = jnp.float32
INTERPRET = False


def at(z, y, c):
    return (z * NY + y) * 2 + c


ALONG_Y = [[at(z, y, 0) for y in range(NY)] for z in range(NZ)]
ALONG_Z = [[at(z, y, 1) for z in range(NZ)] for y in range(NY)]
ALONG_Y1 = [[at(z, y, 1) for y in range(NY)] for z in range(NZ)]
ALONG_Z0 = [[at(z, y, 0) for z in range(NZ)] for y in range(NY)]


def to_group(block, groups):
    n = len(groups[0])
    copies = jnp.broadcast_to(block, (n, *block.shape))
    return lax.all_to_all(
        copies, "sp", split_axis=0, concat_axis=0, tiled=True, axis_index_groups=groups
    )


def lines(block):
    return to_group(block, ALONG_Y + ALONG_Z)


def plane(once):
    return to_group(once, ALONG_Z0 + ALONG_Y1)


def after(v, earlier):
    return lax.optimization_barrier((v, earlier))[0]


def swap_cores(v):
    count = lax.axis_size("sp")
    return lax.ppermute(v, "sp", [(i, i ^ 1) for i in range(count)])


def by_core(first, mine, other):
    return jnp.where(first, mine, other), jnp.where(first, other, mine)


def to_column_owner(v, flip):
    nb = NZ // NX
    pairs = []
    for z in range(NZ):
        a, b = divmod(z, nb)
        for y in range(NY):
            for c in range(2):
                for x in range(NX):
                    half = c ^ flip
                    place = (x * nb + b, y) if half == 0 else (y, x * nb + b)
                    pairs.append((at(z, y, c) * NX + x, at(*place, half) * NX + a))
    return lax.ppermute(v, ("sp", "x"), pairs)


def from_all_x(v):
    return [v] + [
        lax.ppermute(v, "x", [(i, (i + step) % NX) for i in range(NX)]) for step in range(1, NX)
    ]


def exchange_x(copies):
    return [lax.all_to_all(copies, "x", split_axis=0, concat_axis=0, tiled=True)]


def part_of(refs, k):
    if len(refs) == 1:
        return refs[0].at[k], k
    return refs[k], (lax.axis_index("x") + NX - k) % NX


def core_here():
    return lax.axis_index("sp") % 2


def norm_kernel(layer, n, *refs):
    parts, (gain, xs) = refs[:n], refs[n:]

    def rows_at(i, _):
        rows = pl.ds(pl.multiple_of(i * 16, 16), 16)
        total = jnp.zeros((16, 128), F32)
        held = []
        for k in range(NX):
            ref, owner = part_of(parts, k)
            v = ref[rows, :].astype(F32)
            held.append((v, owner))
            sq = v * v
            for q in range(FEAT // 128):
                total += sq[:, q * 128 : (q + 1) * 128]
        scale = lax.rsqrt(jnp.sum(total, axis=1, keepdims=True) / (NX * FEAT) + 1e-06)
        for v, owner in held:
            g = gain[layer * NX + owner]
            xs[owner, rows, :] = (v * scale * g).astype(BF)
        return 0

    lax.fori_loop(0, TOK // 16, rows_at, 0)


def mix_kernel(xs, mine, other, glu, vs, gs):
    def fill(zy, yz):
        for z in range(NZ):
            rows = slice(z * NY * ROWS, (z + 1) * NY * ROWS)
            vs[rows, :] = zy[z, :, :ROWS, :].reshape(NY * ROWS, CH)
            gs[rows, :] = yz[:, z, :ROWS, :].reshape(NY * ROWS, CH)

    @pl.when(core_here() == 0)
    def _():
        fill(mine, other)

    @pl.when(core_here() == 1)
    def _():
        fill(other, mine)

    value = jnp.zeros((TOK, CH), F32)
    gate = jnp.zeros((TOK, CH), F32)
    for k in range(NX):
        rows = slice(k * FEAT, (k + 1) * FEAT)
        value += jnp.dot(xs[k], vs[rows, :], preferred_element_type=F32)
        gate += jnp.dot(xs[k], gs[rows, :], preferred_element_type=F32)
    glu[...] = (value * jax.nn.sigmoid(gate)).astype(BF)


def split_three(v):
    hi = v.astype(BF).astype(F32)
    mid = (v - hi).astype(BF).astype(F32)
    return [hi, mid, v - hi - mid]


def conv_kernel(layer, copies, before, glu, taps, gain, out, ext, shifted, conv):
    ext[:TAPS, :] = before[...].astype(F32)
    ext[TAPS:, :] = glu[...].astype(F32)
    span = TOK + TAPS - 8
    for b in range(8):
        shifted[b] = ext[1 + b : 1 + b + span, :]
    for lane in range(0, CH, 128):
        for base in range(0, TOK, 128):

            def step(a, acc):
                start = pl.multiple_of(a * 8, 8)
                tap = taps[layer, pl.ds(start, 8), lane : lane + 128]
                for b in range(8):
                    window = shifted[b, pl.ds(start + base, 128), lane : lane + 128]
                    acc += window * tap[b : b + 1]
                return acc

            acc = lax.fori_loop(0, TAPS // 8, step, jnp.zeros((128, 128), F32))
            conv[base : base + 128, lane : lane + 128] = acc

    def centre(i, _):
        rows = pl.ds(pl.multiple_of(i * 32, 32), 32)
        v = conv[rows, :]
        d = (v - jnp.mean(v, axis=1, keepdims=True)).astype(BF)
        for k in range(copies):
            out[k, rows, :] = d
        return 0

    lax.fori_loop(0, TOK // 32, centre, 0)
    ones = jnp.full((8, CH), 1.0 / CH, F32)
    means = lax.dot_general(
        ones, conv[...], (((1,), (1,)), ((), ())), precision=lax.Precision.HIGHEST,
        preferred_element_type=F32,
    )[:1]
    extra = split_three(means) + split_three(gain[layer : layer + 1, :])
    extra = jnp.concatenate(extra + [jnp.zeros((10, CH), F32)], axis=0).astype(BF)
    for k in range(copies):
        out[k, TOK:, :] = extra


def out_kernel(n, copies, *refs):
    parts, rest = refs[:n], refs[n:]
    x, mine, other, out, means, acts, wt = rest
    pick = (lax.broadcasted_iota(jnp.int32, (16, 128), 0) < 3).astype(BF)
    total = jnp.zeros((TOK, 128), F32)
    for k in range(NX):
        ref, _ = part_of(parts, k)
        m = lax.dot_general(
            ref[TOK:, :], pick, (((0,), (0,)), ((), ())), preferred_element_type=F32
        )
        means[k] = m
        total += m
    means[NX] = total / NX

    def rows_at(i, _):
        rows = pl.ds(pl.multiple_of(i * 16, 16), 16)
        held = []
        square = jnp.zeros((16, 128), F32)
        for k in range(NX):
            ref, owner = part_of(parts, k)
            shift = means[k, rows, :] - means[NX, rows, :]
            v = ref[rows, :].astype(F32)
            v = jnp.concatenate([v[:, :128] + shift, v[:, 128:] + shift], axis=1)
            sq = v * v
            square += sq[:, :128] + sq[:, 128:]
            tail = ref[TOK:, :].astype(F32)
            g = tail[3:4] + tail[4:5] + tail[5:6]
            held.append((v, g, owner))
        scale = lax.rsqrt(jnp.sum(square, axis=1, keepdims=True) / C + 1e-05)
        for v, g, owner in held:
            u = v * scale * g
            acts[owner, rows, :] = (u / (1.0 + jnp.exp(-u))).astype(BF)
        return 0

    lax.fori_loop(0, TOK // 16, rows_at, 0)

    def fill(halves):
        for k in range(NX):
            for h, ref in enumerate(halves):
                for q in range(2):
                    for i in range(2):
                        w = ref[k * 2 + i, :, ROWS:, q * 128 : (q + 1) * 128]
                        wt[k, i * NY : (i + 1) * NY, q, :, h * 128 : (h + 1) * 128] = w

    @pl.when(core_here() == 0)
    def _():
        fill((mine, other))

    @pl.when(core_here() == 1)
    def _():
        fill((other, mine))

    branch = jnp.zeros((TOK, FEAT), F32)
    for k in range(NX):
        branch += lax.dot_general(
            acts[k], wt[k].reshape(FEAT, CH), (((1,), (1,)), ((), ())),
            preferred_element_type=F32,
        )
    new = (x[...].astype(F32) + branch).astype(BF)
    for k in range(copies):
        out[k] = new


def call(body, out, ins, scratch, flops):
    return pl.pallas_call(
        body,
        out_shape=out,
        in_specs=[pl.BlockSpec(memory_space=pltpu.VMEM)] * len(ins),
        out_specs=pl.BlockSpec(memory_space=pltpu.VMEM),
        scratch_shapes=scratch,
        cost_estimate=pl.CostEstimate(flops=flops, transcendentals=0, bytes_accessed=1 << 20),
        compiler_params=pltpu.CompilerParams(vmem_limit_bytes=40 << 20),
        interpret=INTERPRET,
    )(*ins)


def normalise(layer, parts, gain):
    def body(*refs):
        norm_kernel(layer, len(parts), *refs)

    return call(
        body, jax.ShapeDtypeStruct((NX, TOK, FEAT), BF), [*parts, gain], [], 8 * NX * TOK * FEAT
    )


def mix(xs, mine, other):
    return call(
        mix_kernel,
        jax.ShapeDtypeStruct((TOK, CH), BF),
        [xs, mine, other],
        [pltpu.VMEM((NX * FEAT, CH), BF), pltpu.VMEM((NX * FEAT, CH), BF)],
        4 * NX * TOK * FEAT * CH,
    )


def convolve(layer, copies, before, glu, taps, gain):
    def body(*refs):
        conv_kernel(layer, copies, *refs)

    return call(
        body,
        jax.ShapeDtypeStruct((copies, PACK, CH), BF),
        [before, glu, taps, gain],
        [
            pltpu.VMEM((TAPS + TOK, CH), F32),
            pltpu.VMEM((8, TOK + TAPS - 8, CH), F32),
            pltpu.VMEM((TOK, CH), F32),
        ],
        2 * TOK * CH * TAPS,
    )


def project(copies, parts, x, mine, other):
    def body(*refs):
        out_kernel(len(parts), copies, *refs)

    return call(
        body,
        jax.ShapeDtypeStruct((copies, TOK, FEAT), BF),
        [*parts, x, mine, other],
        [
            pltpu.VMEM((NX + 1, TOK, 128), F32),
            pltpu.VMEM((NX, TOK, CH), BF),
            pltpu.VMEM((NX, 2 * NY, 2, 16, CH), BF),
        ],
        2 * NX * TOK * CH * FEAT,
    )


def shards(stream, norm_gain, w_value, w_gate, conv_taps, channel_gain, w_out):
    first = core_here() == 0
    gain = norm_gain.reshape(LAYERS * NX, 1, FEAT)

    keep, send = by_core(first, w_value, w_gate)
    top, bottom = by_core(first, keep, swap_cores(send))
    half_proj = jnp.concatenate([top, bottom], axis=1)
    out_t = jnp.swapaxes(w_out, 1, 2)
    keep, send = by_core(first, out_t[:, :, : CH // 2], out_t[:, :, CH // 2 :])
    left, right = by_core(first, to_column_owner(keep, 0), to_column_owner(send, 1))
    half_out = jnp.concatenate([left, right], axis=2)
    blocks = jnp.concatenate([half_proj, half_out], axis=1)

    x = stream
    count = lax.axis_size("sp")
    once = lines(blocks[0])
    parts = from_all_x(after(x, once))
    gathered = plane(once)
    for layer in range(LAYERS):
        last = layer + 1 == LAYERS
        mine = gathered
        other = swap_cores(mine)
        if not last:
            following = lines(after(blocks[layer + 1], gathered))
        normed = normalise(layer, parts, gain)
        glu = mix(normed, mine, other)
        if not last:
            gathered = plane(after(following, glu))
        before = lax.ppermute(glu[TOK - TAPS :], "sp", [(i, i + 1) for i in range(count - 1)])
        packed = convolve(layer, NX if last else 1, before, glu, conv_taps, channel_gain)
        parts = exchange_x(packed) if last else from_all_x(packed[0])
        new = project(1 if last else NX, parts, x, mine, other)
        x = new[0]
        if not last:
            parts = exchange_x(new)
    return x


def solution(mesh):
    flat = Mesh(mesh.devices, ("sp", "x"))
    in_specs = (
        P("sp", "x"),
        P(),
        P(None, "sp", "x"),
        P(None, "sp", "x"),
        P(None, None, "x"),
        P(None, "x"),
        P(None, "x", "sp"),
    )

    return jax.shard_map(shards, mesh=flat, in_specs=in_specs, out_specs=P("sp", "x"), check_vma=False)
```

```python
import jax
import jax.numpy as jnp
from jax import lax
from jax.experimental import pallas as pl
from jax.experimental.pallas import tpu as pltpu
from jax.sharding import Mesh
from jax.sharding import PartitionSpec as P


C = 1024
LAYERS = 2
NZ, NY, NX = 8, 8, 4
TOK, CH, TAPS, FEAT = 256, 256, 128, 512
PACK = TOK + 16
HALF = TOK // 2
SPAN = HALF + TAPS - 8
BF = jnp.bfloat16
F32 = jnp.float32
INTERPRET = False


def at(z, y, c):
    return (z * NY + y) * 2 + c


ALONG_Y = [[at(z, y, 0) for y in range(NY)] for z in range(NZ)]
ALONG_Z = [[at(z, y, 1) for z in range(NZ)] for y in range(NY)]
ALONG_Y1 = [[at(z, y, 1) for y in range(NY)] for z in range(NZ)]
ALONG_Z0 = [[at(z, y, 0) for z in range(NZ)] for y in range(NY)]


def to_group(block, groups):
    n = len(groups[0])
    copies = jnp.broadcast_to(block, (n, *block.shape))
    return lax.all_to_all(
        copies, "sp", split_axis=0, concat_axis=0, tiled=True, axis_index_groups=groups
    )


def lines(block):
    return to_group(block, ALONG_Y + ALONG_Z)


def plane(once):
    return to_group(once, ALONG_Z0 + ALONG_Y1)


def after(v, earlier):
    return lax.optimization_barrier((v, earlier))[0]


def swap_cores(v):
    count = lax.axis_size("sp")
    return lax.ppermute(v, "sp", [(i, i ^ 1) for i in range(count)])


def to_column_owner(v):
    nb = NZ // NX
    pairs = []
    for z in range(NZ):
        a, b = divmod(z, nb)
        for y in range(NY):
            for c in range(2):
                for x in range(NX):
                    place = (x * nb + b, y) if c == 0 else (y, x * nb + b)
                    pairs.append((at(z, y, c) * NX + x, at(*place, c) * NX + a))
    return lax.ppermute(v, ("sp", "x"), pairs)


def from_all_x(v):
    return [v] + [
        lax.ppermute(v, "x", [(i, (i + step) % NX) for i in range(NX)]) for step in range(1, NX)
    ]


def exchange_x(copies):
    return [lax.all_to_all(copies, "x", split_axis=0, concat_axis=0, tiled=True)]


def part_of(refs, k):
    if len(refs) == 1:
        return refs[0].at[k], k
    return refs[k], (lax.axis_index("x") + NX - k) % NX


def core_here():
    return lax.axis_index("sp") % 2


def norm_kernel(layer, n, *refs):
    parts, (gain, xs, scale) = refs[:n], refs[n:]

    def squares(i, _):
        rows = pl.ds(pl.multiple_of(i * 16, 16), 16)
        total = jnp.zeros((16, 128), F32)
        for k in range(NX):
            v = part_of(parts, k)[0][rows, :].astype(F32)
            sq = v * v
            for q in range(FEAT // 128):
                total += sq[:, q * 128 : (q + 1) * 128]
        scale[rows, :] = total
        return 0

    lax.fori_loop(0, TOK // 16, squares, 0, unroll=2)
    mean = jnp.sum(scale[...], axis=1, keepdims=True) / (NX * FEAT)
    scale[...] = jnp.broadcast_to(lax.rsqrt(mean + 1e-06), (TOK, 128))

    def apply(i, _):
        rows = pl.ds(pl.multiple_of(i * 16, 16), 16)
        factor = jnp.concatenate([scale[rows, :]] * (FEAT // 128), axis=1)
        for k in range(NX):
            ref, owner = part_of(parts, k)
            xs[owner, rows, :] = (ref[rows, :].astype(F32) * factor * gain[layer * NX + owner]).astype(BF)
        return 0

    lax.fori_loop(0, TOK // 16, apply, 0, unroll=2)


def mix_kernel(xs, mine, other, glu, vs, gs):
    def fill(zy, yz):
        for z in range(NZ):
            for c, w in enumerate((zy.at[z], yz.at[:, z])):
                vs[z, :, c] = w[:, :16, :]
                gs[z, :, c] = w[:, 16:32, :]

    @pl.when(core_here() == 0)
    def _():
        fill(mine, other)

    @pl.when(core_here() == 1)
    def _():
        fill(other, mine)

    value = jnp.zeros((TOK, CH), F32)
    gate = jnp.zeros((TOK, CH), F32)
    for k in range(NX):
        planes = slice(2 * k, 2 * k + 2)
        value += jnp.dot(xs[k], vs[planes].reshape(FEAT, CH), preferred_element_type=F32)
        gate += jnp.dot(xs[k], gs[planes].reshape(FEAT, CH), preferred_element_type=F32)
    glu[...] = (value * jax.nn.sigmoid(gate)).astype(BF)


def split_three(v):
    hi = v.astype(BF).astype(F32)
    mid = (v - hi).astype(BF).astype(F32)
    return [hi, mid, v - hi - mid]


def conv_half(layer, ext, taps, conv, shifted, base):
    for b in range(8):
        shifted[b] = ext[1 + b : 1 + b + SPAN, :]
    for lane in range(0, CH, 128):

        def step(a, acc):
            start = pl.multiple_of(a * 8, 8)
            tap = taps[layer, pl.ds(start, 8), lane : lane + 128]
            for b in range(8):
                acc += shifted[b, pl.ds(start, HALF), lane : lane + 128] * tap[b : b + 1]
            return acc

        acc = lax.fori_loop(0, TAPS // 8, step, jnp.zeros((HALF, 128), F32))
        conv[base : base + HALF, lane : lane + 128] = acc


def late_kernel(layer, glu, taps, conv, ext, shifted):
    ext[...] = glu[...].astype(F32)
    conv_half(layer, ext, taps, conv, shifted, 0)


def conv_kernel(layer, copies, before, glu, late, taps, gain, out, ext, shifted, conv):
    ext[:TAPS, :] = before[...].astype(F32)
    ext[TAPS:, :] = glu[:HALF, :].astype(F32)
    conv_half(layer, ext, taps, conv, shifted, 0)
    conv[HALF:, :] = late[...]
    ones = jnp.full((8, CH), 1.0 / CH, F32)
    means = lax.dot_general(
        ones, conv[...], (((1,), (1,)), ((), ())), precision=lax.Precision.HIGHEST,
        preferred_element_type=F32,
    )[:1]
    extra = split_three(means) + split_three(gain[layer : layer + 1, :])
    extra = jnp.concatenate(extra + [jnp.zeros((10, CH), F32)], axis=0).astype(BF)
    v = conv[...]
    d = (v - jnp.mean(v, axis=1, keepdims=True)).astype(BF)
    for k in range(copies):
        out[k, TOK:, :] = extra
        out[k, :TOK, :] = d


def arrange_kernel(mine, other, wt):
    def fill(zy, yz):
        for k in range(NX):
            for c, w in enumerate((zy, yz)):
                wt[k, :, :, c] = w[2 * k : 2 * k + 2, :, 32:, :]

    @pl.when(core_here() == 0)
    def _():
        fill(mine, other)

    @pl.when(core_here() == 1)
    def _():
        fill(other, mine)


def out_kernel(n, copies, *refs):
    parts, rest = refs[:n], refs[n:]
    x, wt, out, means, scale, acts = rest
    pick = (lax.broadcasted_iota(jnp.int32, (16, 128), 0) < 3).astype(BF)
    total = jnp.zeros((TOK, 128), F32)
    for k in range(NX):
        m = lax.dot_general(
            part_of(parts, k)[0][TOK:, :], pick, (((0,), (0,)), ((), ())),
            preferred_element_type=F32,
        )
        means[k] = m
        total += m
    for k in range(NX):
        means[k] = means[k] - total / NX

    def shifted_part(k, rows):
        ref, owner = part_of(parts, k)
        v = ref[rows, :].astype(F32)
        shift = means[k, rows, :]
        return jnp.concatenate([v[:, :128] + shift, v[:, 128:] + shift], axis=1), owner

    def squares(i, _):
        rows = pl.ds(pl.multiple_of(i * 16, 16), 16)
        square = jnp.zeros((16, 128), F32)
        for k in range(NX):
            v, _ = shifted_part(k, rows)
            sq = v * v
            square += sq[:, :128] + sq[:, 128:]
        scale[rows, :] = square
        return 0

    lax.fori_loop(0, TOK // 16, squares, 0, unroll=2)
    spread = jnp.sum(scale[...], axis=1, keepdims=True) / C
    scale[...] = jnp.broadcast_to(lax.rsqrt(spread + 1e-05), (TOK, 128))
    gains = []
    for k in range(NX):
        tail = part_of(parts, k)[0][TOK:, :].astype(F32)
        gains.append(tail[3:4] + tail[4:5] + tail[5:6])

    def activate(i, _):
        rows = pl.ds(pl.multiple_of(i * 16, 16), 16)
        factor = jnp.concatenate([scale[rows, :]] * 2, axis=1)
        for k in range(NX):
            v, owner = shifted_part(k, rows)
            u = v * factor * gains[k]
            acts[owner, rows, :] = (u / (1.0 + jnp.exp(-u))).astype(BF)
        return 0

    lax.fori_loop(0, TOK // 16, activate, 0, unroll=2)
    branch = jnp.zeros((TOK, FEAT), F32)
    for k in range(NX):
        branch += lax.dot_general(
            acts[k], wt[k].reshape(FEAT, CH), (((1,), (1,)), ((), ())),
            preferred_element_type=F32,
        )
    new = (x[...].astype(F32) + branch).astype(BF)
    for k in range(copies):
        out[k] = new


def call(body, out, ins, scratch, flops):
    return pl.pallas_call(
        body,
        out_shape=out,
        in_specs=[pl.BlockSpec(memory_space=pltpu.VMEM)] * len(ins),
        out_specs=pl.BlockSpec(memory_space=pltpu.VMEM),
        scratch_shapes=scratch,
        cost_estimate=pl.CostEstimate(flops=flops, transcendentals=0, bytes_accessed=1 << 20),
        compiler_params=pltpu.CompilerParams(vmem_limit_bytes=14 << 20),
        interpret=INTERPRET,
    )(*ins)


def normalise(layer, parts, gain):
    def body(*refs):
        norm_kernel(layer, len(parts), *refs)

    return call(
        body,
        jax.ShapeDtypeStruct((NX, TOK, FEAT), BF),
        [*parts, gain],
        [pltpu.VMEM((TOK, 128), F32)],
        8 * NX * TOK * FEAT,
    )


def mix(xs, mine, other):
    return call(
        mix_kernel,
        jax.ShapeDtypeStruct((TOK, CH), BF),
        [xs, mine, other],
        [pltpu.VMEM((NZ, NY, 2, 16, CH), BF), pltpu.VMEM((NZ, NY, 2, 16, CH), BF)],
        4 * NX * TOK * FEAT * CH,
    )


def conv_late(layer, glu, taps):
    def body(*refs):
        late_kernel(layer, *refs)

    return call(
        body,
        jax.ShapeDtypeStruct((HALF, CH), F32),
        [glu, taps],
        [pltpu.VMEM((TOK, CH), F32), pltpu.VMEM((8, SPAN, CH), F32)],
        2 * HALF * CH * TAPS,
    )


def convolve(layer, copies, before, glu, late, taps, gain):
    def body(*refs):
        conv_kernel(layer, copies, *refs)

    return call(
        body,
        jax.ShapeDtypeStruct((copies, PACK, CH), BF),
        [before, glu, late, taps, gain],
        [
            pltpu.VMEM((TAPS + HALF, CH), F32),
            pltpu.VMEM((8, SPAN, CH), F32),
            pltpu.VMEM((TOK, CH), F32),
        ],
        2 * HALF * CH * TAPS,
    )


def arrange(mine, other):
    return call(
        arrange_kernel, jax.ShapeDtypeStruct((NX, 2, NY, 2, 16, CH), BF), [mine, other], [], 1 << 26
    )


def project(copies, parts, x, wt):
    def body(*refs):
        out_kernel(len(parts), copies, *refs)

    return call(
        body,
        jax.ShapeDtypeStruct((copies, TOK, FEAT), BF),
        [*parts, x, wt],
        [
            pltpu.VMEM((NX, TOK, 128), F32),
            pltpu.VMEM((TOK, 128), F32),
            pltpu.VMEM((NX, TOK, CH), BF),
        ],
        2 * NX * TOK * CH * FEAT,
    )


def shards(stream, norm_gain, w_value, w_gate, conv_taps, channel_gain, w_out):
    gain = norm_gain.reshape(LAYERS * NX, 1, FEAT)
    out_t = to_column_owner(jnp.swapaxes(w_out, 1, 2))
    blocks = jnp.concatenate([w_value, w_gate, out_t], axis=1)

    x = stream
    count = lax.axis_size("sp")
    once = lines(blocks)
    parts = from_all_x(after(x, blocks))
    gathered = plane(once[:, 0])
    for layer in range(LAYERS):
        last = layer + 1 == LAYERS
        mine = gathered
        other = swap_cores(mine)
        normed = normalise(layer, parts, gain)
        glu = mix(normed, mine, other)
        before = lax.ppermute(glu[TOK - TAPS :], "sp", [(i, i + 1) for i in range(count - 1)])
        late = conv_late(layer, glu, conv_taps)
        if not last:
            gathered = plane(after(once[:, layer + 1], before))
        packed = convolve(layer, NX if last else 1, before, glu, late, conv_taps, channel_gain)
        parts = exchange_x(packed) if last else from_all_x(packed[0])
        wt = arrange(after(mine, packed), other)
        new = project(1 if last else NX, parts, x, wt)
        x = new[0]
        if not last:
            parts = exchange_x(new)
    return x


def solution(mesh):
    flat = Mesh(mesh.devices, ("sp", "x"))
    in_specs = (
        P("sp", "x"),
        P(),
        P(None, "sp", "x"),
        P(None, "sp", "x"),
        P(None, None, "x"),
        P(None, "x"),
        P(None, "x", "sp"),
    )

    return jax.shard_map(shards, mesh=flat, in_specs=in_specs, out_specs=P("sp", "x"), check_vma=False)
```

```python
import jax
import jax.numpy as jnp
from jax import lax
from jax.experimental import pallas as pl
from jax.experimental.pallas import tpu as pltpu
from jax.sharding import Mesh
from jax.sharding import PartitionSpec as P


C = 1024
LAYERS = 2
NZ, NY, NX = 8, 8, 4
TOK, CH, TAPS, FEAT = 256, 256, 128, 512
PACK = TOK + 16
HALF = TOK // 2
SPAN = HALF + TAPS - 8
BF = jnp.bfloat16
F32 = jnp.float32
INTERPRET = False


def at(z, y, c):
    return (z * NY + y) * 2 + c


ALONG_Y = [[at(z, y, 0) for y in range(NY)] for z in range(NZ)]
ALONG_Z = [[at(z, y, 1) for z in range(NZ)] for y in range(NY)]
ALONG_Y1 = [[at(z, y, 1) for y in range(NY)] for z in range(NZ)]
ALONG_Z0 = [[at(z, y, 0) for z in range(NZ)] for y in range(NY)]


def to_group(block, groups):
    n = len(groups[0])
    copies = jnp.broadcast_to(block, (n, *block.shape))
    return lax.all_to_all(
        copies, "sp", split_axis=0, concat_axis=0, tiled=True, axis_index_groups=groups
    )


def lines(block):
    return to_group(block, ALONG_Y + ALONG_Z)


def plane(copies):
    return lax.all_to_all(
        copies, "sp", split_axis=0, concat_axis=0, tiled=True,
        axis_index_groups=ALONG_Z0 + ALONG_Y1,
    )


def after(v, earlier):
    return lax.optimization_barrier((v, earlier))[0]


def swap_cores(v):
    count = lax.axis_size("sp")
    return lax.ppermute(v, "sp", [(i, i ^ 1) for i in range(count)])


def to_column_owner(v):
    nb = NZ // NX
    pairs = []
    for z in range(NZ):
        a, b = divmod(z, nb)
        for y in range(NY):
            for c in range(2):
                for x in range(NX):
                    place = (x * nb + b, y) if c == 0 else (y, x * nb + b)
                    pairs.append((at(z, y, c) * NX + x, at(*place, c) * NX + a))
    return lax.ppermute(v, ("sp", "x"), pairs)


def from_all_x(v):
    return [v] + [
        lax.ppermute(v, "x", [(i, (i + step) % NX) for i in range(NX)]) for step in range(1, NX)
    ]


def part_of(refs, k):
    if len(refs) == 1:
        return refs[0].at[k], k
    return refs[k], (lax.axis_index("x") + NX - k) % NX


def core_here():
    return lax.axis_index("sp") % 2


def norm_kernel(layer, n, *refs):
    parts, (gain, xs, scale) = refs[:n], refs[n:]

    def squares(i, _):
        rows = pl.ds(pl.multiple_of(i * 16, 16), 16)
        total = jnp.zeros((16, 128), F32)
        for k in range(NX):
            v = part_of(parts, k)[0][rows, :].astype(F32)
            sq = v * v
            for q in range(FEAT // 128):
                total += sq[:, q * 128 : (q + 1) * 128]
        scale[rows, :] = total
        return 0

    lax.fori_loop(0, TOK // 16, squares, 0, unroll=2)
    mean = jnp.sum(scale[...], axis=1, keepdims=True) / (NX * FEAT)
    scale[...] = jnp.broadcast_to(lax.rsqrt(mean + 1e-06), (TOK, 128))

    def apply(i, _):
        rows = pl.ds(pl.multiple_of(i * 16, 16), 16)
        factor = jnp.concatenate([scale[rows, :]] * (FEAT // 128), axis=1)
        for k in range(NX):
            ref, owner = part_of(parts, k)
            xs[owner, rows, :] = (ref[rows, :].astype(F32) * factor * gain[layer * NX + owner]).astype(BF)
        return 0

    lax.fori_loop(0, TOK // 16, apply, 0, unroll=2)


def mix_kernel(xs, mine, other, glu, vs, gs):
    def fill(zy, yz):
        for z in range(NZ):
            for c, w in enumerate((zy.at[z], yz.at[:, z])):
                vs[z, :, c] = w[:, :16, :]
                gs[z, :, c] = w[:, 16:32, :]

    @pl.when(core_here() == 0)
    def _():
        fill(mine, other)

    @pl.when(core_here() == 1)
    def _():
        fill(other, mine)

    value = jnp.zeros((TOK, CH), F32)
    gate = jnp.zeros((TOK, CH), F32)
    for k in range(NX):
        planes = slice(2 * k, 2 * k + 2)
        value += jnp.dot(xs[k], vs[planes].reshape(FEAT, CH), preferred_element_type=F32)
        gate += jnp.dot(xs[k], gs[planes].reshape(FEAT, CH), preferred_element_type=F32)
    glu[...] = (value * jax.nn.sigmoid(gate)).astype(BF)


def split_three(v):
    hi = v.astype(BF).astype(F32)
    mid = (v - hi).astype(BF).astype(F32)
    return [hi, mid, v - hi - mid]


def conv_half(layer, ext, taps, conv, shifted, base):
    for b in range(8):
        shifted[b] = ext[1 + b : 1 + b + SPAN, :]
    for lane in range(0, CH, 128):

        def step(a, acc):
            start = pl.multiple_of(a * 8, 8)
            tap = taps[layer, pl.ds(start, 8), lane : lane + 128]
            for b in range(8):
                acc += shifted[b, pl.ds(start, HALF), lane : lane + 128] * tap[b : b + 1]
            return acc

        acc = lax.fori_loop(0, TAPS // 8, step, jnp.zeros((HALF, 128), F32))
        conv[base : base + HALF, lane : lane + 128] = acc


def late_kernel(layer, glu, taps, conv, ext, shifted):
    ext[...] = glu[...].astype(F32)
    conv_half(layer, ext, taps, conv, shifted, 0)


def spread_kernel(layer, once, out, sems):
    copies = [pltpu.make_async_copy(once.at[:, layer], out.at[k], sems.at[k]) for k in range(NZ)]
    for c in copies:
        c.start()
    for c in copies:
        c.wait()


def conv_kernel(layer, before, glu, late, taps, gain, out, ext, shifted, conv):
    ext[:TAPS, :] = before[...].astype(F32)
    ext[TAPS:, :] = glu[:HALF, :].astype(F32)
    conv_half(layer, ext, taps, conv, shifted, 0)
    conv[HALF:, :] = late[...]
    ones = jnp.full((8, CH), 1.0 / CH, F32)
    means = lax.dot_general(
        ones, conv[...], (((1,), (1,)), ((), ())), precision=lax.Precision.HIGHEST,
        preferred_element_type=F32,
    )[:1]
    extra = split_three(means) + split_three(gain[layer : layer + 1, :])
    extra = jnp.concatenate(extra + [jnp.zeros((10, CH), F32)], axis=0).astype(BF)
    v = conv[...]
    d = (v - jnp.mean(v, axis=1, keepdims=True)).astype(BF)
    out[TOK:, :] = extra
    out[:TOK, :] = d


def arrange_kernel(mine, other, wt):
    def fill(zy, yz):
        for k in range(NX):
            for c, w in enumerate((zy, yz)):
                wt[k, :, :, c] = w[2 * k : 2 * k + 2, :, 32:, :]

    @pl.when(core_here() == 0)
    def _():
        fill(mine, other)

    @pl.when(core_here() == 1)
    def _():
        fill(other, mine)


def out_kernel(n, *refs):
    parts, rest = refs[:n], refs[n:]
    x, wt, out, means, scale, acts = rest
    pick = (lax.broadcasted_iota(jnp.int32, (16, 128), 0) < 3).astype(BF)
    total = jnp.zeros((TOK, 128), F32)
    for k in range(NX):
        m = lax.dot_general(
            part_of(parts, k)[0][TOK:, :], pick, (((0,), (0,)), ((), ())),
            preferred_element_type=F32,
        )
        means[k] = m
        total += m
    for k in range(NX):
        means[k] = means[k] - total / NX

    def shifted_part(k, rows):
        ref, owner = part_of(parts, k)
        v = ref[rows, :].astype(F32)
        shift = means[k, rows, :]
        return jnp.concatenate([v[:, :128] + shift, v[:, 128:] + shift], axis=1), owner

    def squares(i, _):
        rows = pl.ds(pl.multiple_of(i * 16, 16), 16)
        square = jnp.zeros((16, 128), F32)
        for k in range(NX):
            v, _ = shifted_part(k, rows)
            sq = v * v
            square += sq[:, :128] + sq[:, 128:]
        scale[rows, :] = square
        return 0

    lax.fori_loop(0, TOK // 16, squares, 0, unroll=2)
    spread = jnp.sum(scale[...], axis=1, keepdims=True) / C
    scale[...] = jnp.broadcast_to(lax.rsqrt(spread + 1e-05), (TOK, 128))
    gains = []
    for k in range(NX):
        tail = part_of(parts, k)[0][TOK:, :].astype(F32)
        gains.append(tail[3:4] + tail[4:5] + tail[5:6])

    def activate(i, _):
        rows = pl.ds(pl.multiple_of(i * 16, 16), 16)
        factor = jnp.concatenate([scale[rows, :]] * 2, axis=1)
        for k in range(NX):
            v, owner = shifted_part(k, rows)
            u = v * factor * gains[k]
            acts[owner, rows, :] = (u / (1.0 + jnp.exp(-u))).astype(BF)
        return 0

    lax.fori_loop(0, TOK // 16, activate, 0, unroll=2)
    branch = jnp.zeros((TOK, FEAT), F32)
    for k in range(NX):
        branch += lax.dot_general(
            acts[k], wt[k].reshape(FEAT, CH), (((1,), (1,)), ((), ())),
            preferred_element_type=F32,
        )
    out[...] = (x[...].astype(F32) + branch).astype(BF)


def call(body, out, ins, scratch, flops, place=pltpu.VMEM):
    return pl.pallas_call(
        body,
        out_shape=out,
        in_specs=[pl.BlockSpec(memory_space=pltpu.VMEM)] * len(ins),
        out_specs=pl.BlockSpec(memory_space=place),
        scratch_shapes=scratch,
        cost_estimate=pl.CostEstimate(flops=flops, transcendentals=0, bytes_accessed=1 << 20),
        compiler_params=pltpu.CompilerParams(vmem_limit_bytes=14 << 20),
        interpret=INTERPRET,
    )(*ins)


def normalise(layer, parts, gain):
    def body(*refs):
        norm_kernel(layer, len(parts), *refs)

    return call(
        body,
        jax.ShapeDtypeStruct((NX, TOK, FEAT), BF),
        [*parts, gain],
        [pltpu.VMEM((TOK, 128), F32)],
        8 * NX * TOK * FEAT,
    )


def mix(xs, mine, other):
    return call(
        mix_kernel,
        jax.ShapeDtypeStruct((TOK, CH), BF),
        [xs, mine, other],
        [pltpu.VMEM((NZ, NY, 2, 16, CH), BF), pltpu.VMEM((NZ, NY, 2, 16, CH), BF)],
        4 * NX * TOK * FEAT * CH,
    )


def conv_late(layer, glu, taps):
    def body(*refs):
        late_kernel(layer, *refs)

    return call(
        body,
        jax.ShapeDtypeStruct((HALF, CH), F32),
        [glu, taps],
        [pltpu.VMEM((TOK, CH), F32), pltpu.VMEM((8, SPAN, CH), F32)],
        2 * HALF * CH * TAPS,
    )


def convolve(layer, before, glu, late, taps, gain):
    def body(*refs):
        conv_kernel(layer, *refs)

    return call(
        body,
        jax.ShapeDtypeStruct((PACK, CH), BF),
        [before, glu, late, taps, gain],
        [
            pltpu.VMEM((TAPS + HALF, CH), F32),
            pltpu.VMEM((8, SPAN, CH), F32),
            pltpu.VMEM((TOK, CH), F32),
        ],
        2 * HALF * CH * TAPS,
    )


def spread(layer, once):
    def body(*refs):
        spread_kernel(layer, *refs)

    return call(
        body,
        jax.ShapeDtypeStruct((NZ, NZ, 48, CH), BF),
        [once],
        [pltpu.SemaphoreType.DMA((NZ,))],
        1 << 26,
        pltpu.HBM,
    )


def arrange(mine, other):
    return call(
        arrange_kernel, jax.ShapeDtypeStruct((NX, 2, NY, 2, 16, CH), BF), [mine, other], [], 1 << 26
    )


def project(parts, x, wt):
    def body(*refs):
        out_kernel(len(parts), *refs)

    return call(
        body,
        jax.ShapeDtypeStruct((TOK, FEAT), BF),
        [*parts, x, wt],
        [
            pltpu.VMEM((NX, TOK, 128), F32),
            pltpu.VMEM((TOK, 128), F32),
            pltpu.VMEM((NX, TOK, CH), BF),
        ],
        2 * NX * TOK * CH * FEAT,
    )


def shards(stream, norm_gain, w_value, w_gate, conv_taps, channel_gain, w_out):
    gain = norm_gain.reshape(LAYERS * NX, 1, FEAT)
    out_t = to_column_owner(jnp.swapaxes(w_out, 1, 2))
    blocks = jnp.concatenate([w_value, w_gate, out_t], axis=1)

    x = stream
    count = lax.axis_size("sp")
    once = lines(blocks)
    parts = from_all_x(after(x, blocks))
    ready = spread(0, once)
    gathered = plane(ready)
    ready = spread(1, once)
    for layer in range(LAYERS):
        last = layer + 1 == LAYERS
        mine = gathered
        other = swap_cores(mine)
        normed = normalise(layer, parts, gain)
        glu = mix(normed, mine, other)
        before = lax.ppermute(glu[TOK - TAPS :], "sp", [(i, i + 1) for i in range(count - 1)])
        late = conv_late(layer, glu, conv_taps)
        packed = convolve(layer, before, glu, late, conv_taps, channel_gain)
        parts = from_all_x(packed)
        if not last:
            gathered = plane(after(ready, packed))
        wt = arrange(after(mine, packed), other)
        x = project(parts, x, wt)
        if not last:
            parts = from_all_x(x)
    return x


def solution(mesh):
    flat = Mesh(mesh.devices, ("sp", "x"))
    in_specs = (
        P("sp", "x"),
        P(),
        P(None, "sp", "x"),
        P(None, "sp", "x"),
        P(None, None, "x"),
        P(None, "x"),
        P(None, "x", "sp"),
    )

    return jax.shard_map(shards, mesh=flat, in_specs=in_specs, out_specs=P("sp", "x"), check_vma=False)
```

```python
import jax
import jax.numpy as jnp
from jax import lax
from jax.experimental import pallas as pl
from jax.experimental.pallas import tpu as pltpu
from jax.sharding import Mesh
from jax.sharding import PartitionSpec as P


C = 1024
LAYERS = 2
NZ, NY, NX = 8, 8, 4
TOK, CH, TAPS, FEAT = 256, 256, 128, 512
PACK = TOK + 16
HALF = TOK // 2
SPAN = HALF + TAPS - 8
BF = jnp.bfloat16
F32 = jnp.float32
INTERPRET = False


def at(z, y, c):
    return (z * NY + y) * 2 + c


ALONG_Y = [[at(z, y, 0) for y in range(NY)] for z in range(NZ)]
ALONG_Z = [[at(z, y, 1) for z in range(NZ)] for y in range(NY)]
ALONG_Y1 = [[at(z, y, 1) for y in range(NY)] for z in range(NZ)]
ALONG_Z0 = [[at(z, y, 0) for z in range(NZ)] for y in range(NY)]


def to_group(block, groups):
    n = len(groups[0])
    copies = jnp.broadcast_to(block, (n, *block.shape))
    return lax.all_to_all(
        copies, "sp", split_axis=0, concat_axis=0, tiled=True, axis_index_groups=groups
    )


def lines(block):
    return to_group(block, ALONG_Y + ALONG_Z)


def plane(copies):
    return lax.all_to_all(
        copies, "sp", split_axis=0, concat_axis=0, tiled=True,
        axis_index_groups=ALONG_Z0 + ALONG_Y1,
    )


def after(v, earlier):
    return lax.optimization_barrier((v, earlier))[0]


def swap_cores(v):
    count = lax.axis_size("sp")
    return lax.ppermute(v, "sp", [(i, i ^ 1) for i in range(count)])


def to_column_owner(v):
    nb = NZ // NX
    pairs = []
    for z in range(NZ):
        a, b = divmod(z, nb)
        for y in range(NY):
            for c in range(2):
                for x in range(NX):
                    place = (x * nb + b, y) if c == 0 else (y, x * nb + b)
                    pairs.append((at(z, y, c) * NX + x, at(*place, c) * NX + a))
    return lax.ppermute(v, ("sp", "x"), pairs)


def from_all_x(v):
    return [v] + [
        lax.ppermute(v, "x", [(i, (i + step) % NX) for i in range(NX)]) for step in range(1, NX)
    ]


def part_of(refs, k):
    if len(refs) == 1:
        return refs[0].at[k], k
    return refs[k], (lax.axis_index("x") + NX - k) % NX


def core_here():
    return lax.axis_index("sp") % 2


def norm_kernel(layer, n, *refs):
    parts, (gain, xs, scale) = refs[:n], refs[n:]

    def squares(i, _):
        rows = pl.ds(pl.multiple_of(i * 16, 16), 16)
        total = jnp.zeros((16, 128), F32)
        for k in range(NX):
            v = part_of(parts, k)[0][rows, :].astype(F32)
            sq = v * v
            for q in range(FEAT // 128):
                total += sq[:, q * 128 : (q + 1) * 128]
        scale[rows, :] = total
        return 0

    steps = scale.shape[0] // 16
    lax.fori_loop(0, steps, squares, 0, unroll=2)
    mean = jnp.sum(scale[...], axis=1, keepdims=True) / (NX * FEAT)
    scale[...] = jnp.broadcast_to(lax.rsqrt(mean + 1e-06), scale.shape)

    def apply(i, _):
        rows = pl.ds(pl.multiple_of(i * 16, 16), 16)
        factor = jnp.concatenate([scale[rows, :]] * (FEAT // 128), axis=1)
        for k in range(NX):
            ref, owner = part_of(parts, k)
            xs[owner, rows, :] = (ref[rows, :].astype(F32) * factor * gain[layer * NX + owner]).astype(BF)
        return 0

    lax.fori_loop(0, steps, apply, 0, unroll=2)


def mix_kernel(xs, mine, other, glu, wt, vs, gs):
    def fill(zy, yz):
        for z in range(NZ):
            for c, w in enumerate((zy.at[z], yz.at[:, z])):
                vs[z, :, c] = w[:, :16, :]
                gs[z, :, c] = w[:, 16:32, :]
        for k in range(NX):
            for c, w in enumerate((zy, yz)):
                wt[k, :, :, c] = w[2 * k : 2 * k + 2, :, 32:, :]

    @pl.when(core_here() == 0)
    def _():
        fill(mine, other)

    @pl.when(core_here() == 1)
    def _():
        fill(other, mine)

    value = jnp.zeros(glu.shape, F32)
    gate = jnp.zeros(glu.shape, F32)
    for k in range(NX):
        planes = slice(2 * k, 2 * k + 2)
        value += jnp.dot(xs[k], vs[planes].reshape(FEAT, CH), preferred_element_type=F32)
        gate += jnp.dot(xs[k], gs[planes].reshape(FEAT, CH), preferred_element_type=F32)
    glu[...] = (value * jax.nn.sigmoid(gate)).astype(BF)


def split_three(v):
    hi = v.astype(BF).astype(F32)
    mid = (v - hi).astype(BF).astype(F32)
    return [hi, mid, v - hi - mid]


def send_all(src, out, sems):
    copies = [pltpu.make_async_copy(src, out.at[k], sems.at[k]) for k in range(out.shape[0])]
    for c in copies:
        c.start()
    for c in copies:
        c.wait()


def spread_kernel(layer, once, out, sems):
    send_all(once.at[:, layer], out, sems)


def taps_over(layer, ext, taps, conv, shifted):
    rows = conv.shape[0]
    for b in range(8):
        shifted[b] = ext[1 + b : 1 + b + rows + TAPS - 8, :]
    for lane in range(0, CH, 128):
        for base in range(0, rows, HALF):

            def step(a, acc):
                start = pl.multiple_of(a * 8, 8)
                tap = taps[layer, pl.ds(start, 8), lane : lane + 128]
                for b in range(8):
                    window = shifted[b, pl.ds(start + base, HALF), lane : lane + 128]
                    acc += window * tap[b : b + 1]
                return acc

            acc = lax.fori_loop(0, TAPS // 8, step, jnp.zeros((HALF, 128), F32))
            conv[base : base + HALF, lane : lane + 128] = acc


def pack(layer, conv, gain, out):
    ones = jnp.full((8, CH), 1.0 / CH, F32)
    means = lax.dot_general(
        ones, conv[...], (((1,), (1,)), ((), ())), precision=lax.Precision.HIGHEST,
        preferred_element_type=F32,
    )[:1]
    extra = split_three(means) + split_three(gain[layer : layer + 1, :])
    out[TOK:, :] = jnp.concatenate(extra + [jnp.zeros((10, CH), F32)], axis=0).astype(BF)
    v = conv[...]
    out[:TOK, :] = (v - jnp.mean(v, axis=1, keepdims=True)).astype(BF)


def whole_kernel(layer, glu, taps, gain, out, ext, shifted, conv):
    ext[...] = glu[...].astype(F32)
    taps_over(layer, ext, taps, conv, shifted)
    pack(layer, conv, gain, out)


def late_kernel(layer, glu, taps, conv, ext, shifted):
    ext[...] = glu[...].astype(F32)
    taps_over(layer, ext, taps, conv, shifted)


def conv_kernel(layer, before, glu, late, taps, gain, out, ext, shifted, conv):
    ext[:TAPS, :] = before[...].astype(F32)
    ext[TAPS:, :] = glu[:HALF, :].astype(F32)
    taps_over(layer, ext, taps, conv.at[:HALF], shifted)
    conv[HALF:, :] = late[...]
    pack(layer, conv, gain, out)


def out_kernel(n, *refs):
    parts, rest = refs[:n], refs[n:]
    x, wt, out, *rest = rest
    copies = rest[0] if len(rest) == 6 else None
    means, scale, acts, held, sems = rest[-5:]
    fetch = pltpu.make_async_copy(x, held, sems.at[0])
    fetch.start()
    pick = (lax.broadcasted_iota(jnp.int32, (16, 128), 0) < 3).astype(BF)
    total = jnp.zeros((TOK, 128), F32)
    for k in range(NX):
        m = lax.dot_general(
            part_of(parts, k)[0][TOK:, :], pick, (((0,), (0,)), ((), ())),
            preferred_element_type=F32,
        )
        means[k] = m
        total += m
    for k in range(NX):
        means[k] = means[k] - total / NX

    def shifted_part(k, rows):
        ref, owner = part_of(parts, k)
        v = ref[rows, :].astype(F32)
        shift = means[k, rows, :]
        return jnp.concatenate([v[:, :128] + shift, v[:, 128:] + shift], axis=1), owner

    def squares(i, _):
        rows = pl.ds(pl.multiple_of(i * 16, 16), 16)
        square = jnp.zeros((16, 128), F32)
        for k in range(NX):
            v, _ = shifted_part(k, rows)
            sq = v * v
            square += sq[:, :128] + sq[:, 128:]
        scale[rows, :] = square
        return 0

    lax.fori_loop(0, TOK // 16, squares, 0, unroll=2)
    spread = jnp.sum(scale[...], axis=1, keepdims=True) / C
    scale[...] = jnp.broadcast_to(lax.rsqrt(spread + 1e-05), (TOK, 128))
    gains = []
    for k in range(NX):
        tail = part_of(parts, k)[0][TOK:, :].astype(F32)
        gains.append(tail[3:4] + tail[4:5] + tail[5:6])

    def activate(i, _):
        rows = pl.ds(pl.multiple_of(i * 16, 16), 16)
        factor = jnp.concatenate([scale[rows, :]] * 2, axis=1)
        for k in range(NX):
            v, owner = shifted_part(k, rows)
            u = v * factor * gains[k]
            acts[owner, rows, :] = (u / (1.0 + jnp.exp(-u))).astype(BF)
        return 0

    lax.fori_loop(0, TOK // 16, activate, 0, unroll=2)
    branch = jnp.zeros((TOK, FEAT), F32)
    for k in range(NX):
        branch += lax.dot_general(
            acts[k], wt[k].reshape(FEAT, CH), (((1,), (1,)), ((), ())),
            preferred_element_type=F32,
        )
    fetch.wait()
    out[...] = (held[...].astype(F32) + branch).astype(BF)
    if copies is not None:
        send_all(out, copies, sems)


def call(body, out, ins, scratch, flops, place=pltpu.VMEM):
    spec = pl.BlockSpec(memory_space=place)
    return pl.pallas_call(
        body,
        out_shape=out,
        in_specs=[pl.BlockSpec(memory_space=pltpu.VMEM)] * len(ins),
        out_specs=(spec,) * len(out) if isinstance(out, tuple) else spec,
        scratch_shapes=scratch,
        cost_estimate=pl.CostEstimate(flops=flops, transcendentals=0, bytes_accessed=1 << 20),
        compiler_params=pltpu.CompilerParams(vmem_limit_bytes=14 << 20),
        interpret=INTERPRET,
    )(*ins)


def normalise(layer, parts, gain):
    def body(*refs):
        norm_kernel(layer, len(parts), *refs)

    return call(
        body,
        jax.ShapeDtypeStruct((NX, parts[0].shape[-2], FEAT), BF),
        [*parts, gain],
        [pltpu.VMEM((parts[0].shape[-2], 128), F32)],
        8 * NX * TOK * FEAT,
    )


def mix(xs, mine, other):
    return call(
        mix_kernel,
        (
            jax.ShapeDtypeStruct((xs.shape[1], CH), BF),
            jax.ShapeDtypeStruct((NX, 2, NY, 2, 16, CH), BF),
        ),
        [xs, mine, other],
        [pltpu.VMEM((NZ, NY, 2, 16, CH), BF), pltpu.VMEM((NZ, NY, 2, 16, CH), BF)],
        4 * NX * TOK * FEAT * CH,
    )


def conv_late(layer, glu, taps):
    def body(*refs):
        late_kernel(layer, *refs)

    return call(
        body,
        jax.ShapeDtypeStruct((HALF, CH), F32),
        [glu, taps],
        [pltpu.VMEM((TOK, CH), F32), pltpu.VMEM((8, SPAN, CH), F32)],
        2 * HALF * CH * TAPS,
    )


def conv_whole(layer, glu, taps, gain):
    def body(*refs):
        whole_kernel(layer, *refs)

    return call(
        body,
        jax.ShapeDtypeStruct((PACK, CH), BF),
        [glu, taps, gain],
        [
            pltpu.VMEM((TAPS + TOK, CH), F32),
            pltpu.VMEM((8, TOK + TAPS - 8, CH), F32),
            pltpu.VMEM((TOK, CH), F32),
        ],
        2 * TOK * CH * TAPS,
    )


def convolve(layer, before, glu, late, taps, gain):
    def body(*refs):
        conv_kernel(layer, *refs)

    return call(
        body,
        jax.ShapeDtypeStruct((PACK, CH), BF),
        [before, glu, late, taps, gain],
        [
            pltpu.VMEM((TAPS + HALF, CH), F32),
            pltpu.VMEM((8, SPAN, CH), F32),
            pltpu.VMEM((TOK, CH), F32),
        ],
        2 * HALF * CH * TAPS,
    )


def spread(layer, once):
    def body(*refs):
        spread_kernel(layer, *refs)

    return call(
        body,
        jax.ShapeDtypeStruct((NZ, NZ, 48, CH), BF),
        [once],
        [pltpu.SemaphoreType.DMA((NZ,))],
        1 << 26,
        pltpu.HBM,
    )


def project(parts, x, wt, to_all):
    def body(*refs):
        out_kernel(len(parts), *refs)

    shape = jax.ShapeDtypeStruct((TOK, FEAT), BF)
    copies = pltpu.HBM((NX, TOK, FEAT), BF)
    inside, anywhere = pl.BlockSpec(memory_space=pltpu.VMEM), pl.BlockSpec(memory_space=pl.ANY)
    return pl.pallas_call(
        body,
        out_shape=(shape, copies) if to_all else shape,
        in_specs=[inside] * len(parts) + [anywhere, inside],
        out_specs=(inside, pl.BlockSpec(memory_space=pltpu.HBM)) if to_all else inside,
        scratch_shapes=[
            pltpu.VMEM((NX, TOK, 128), F32),
            pltpu.VMEM((TOK, 128), F32),
            pltpu.VMEM((NX, TOK, CH), BF),
            pltpu.VMEM((TOK, FEAT), BF),
            pltpu.SemaphoreType.DMA((NX,)),
        ],
        cost_estimate=pl.CostEstimate(
            flops=2 * NX * TOK * CH * FEAT, transcendentals=0, bytes_accessed=1 << 20
        ),
        compiler_params=pltpu.CompilerParams(vmem_limit_bytes=14 << 20),
        interpret=INTERPRET,
    )(*parts, x, wt)


def shards(stream, norm_gain, w_value, w_gate, conv_taps, channel_gain, w_out):
    gain = norm_gain.reshape(LAYERS * NX, 1, FEAT)
    out_t = to_column_owner(jnp.swapaxes(w_out, 1, 2))
    blocks = jnp.concatenate([w_value, w_gate, out_t], axis=1)

    x = stream
    count = lax.axis_size("sp")
    chain = [(i, i + 1) for i in range(count - 1)]
    extended = jnp.concatenate([lax.ppermute(x[TOK - TAPS :], "sp", chain), x])
    once = lines(blocks)
    parts = from_all_x(after(extended, blocks))
    ready = spread(0, once)
    gathered = plane(ready)
    ready = spread(1, once)
    normed = normalise(0, parts, gain)
    other = swap_cores(gathered)
    following = plane(after(ready, gathered))
    glu, wt = mix(normed, gathered, other)
    packed = conv_whole(0, glu, conv_taps, channel_gain)
    parts = from_all_x(packed)
    x, copies = project(parts, x, wt, True)

    parts = [lax.all_to_all(copies, "x", split_axis=0, concat_axis=0, tiled=True)]
    other = swap_cores(following)
    normed = normalise(1, parts, gain)
    glu, wt = mix(normed, following, other)
    before = lax.ppermute(glu[TOK - TAPS :], "sp", chain)
    late = conv_late(1, glu, conv_taps)
    packed = convolve(1, before, glu, late, conv_taps, channel_gain)
    parts = from_all_x(packed)
    x = project(parts, x, wt, False)
    return x


def solution(mesh):
    flat = Mesh(mesh.devices, ("sp", "x"))
    in_specs = (
        P("sp", "x"),
        P(),
        P(None, "sp", "x"),
        P(None, "sp", "x"),
        P(None, None, "x"),
        P(None, "x"),
        P(None, "x", "sp"),
    )

    return jax.shard_map(shards, mesh=flat, in_specs=in_specs, out_specs=P("sp", "x"), check_vma=False)
```

```python
import jax
import jax.numpy as jnp
from jax import lax
from jax.experimental import pallas as pl
from jax.experimental.pallas import tpu as pltpu
from jax.sharding import Mesh
from jax.sharding import PartitionSpec as P


C = 1024
LAYERS = 2
NZ, NY, NX = 8, 8, 4
TOK, CH, TAPS, FEAT = 256, 256, 128, 512
PACK = TOK + 16
HALF = TOK // 2
SPAN = HALF + TAPS - 8
BF = jnp.bfloat16
F32 = jnp.float32
INTERPRET = False


def at(z, y, c):
    return (z * NY + y) * 2 + c


ALONG_Y = [[at(z, y, 0) for y in range(NY)] for z in range(NZ)]
ALONG_Z = [[at(z, y, 1) for z in range(NZ)] for y in range(NY)]
ALONG_Y1 = [[at(z, y, 1) for y in range(NY)] for z in range(NZ)]
ALONG_Z0 = [[at(z, y, 0) for z in range(NZ)] for y in range(NY)]


def to_group(block, groups):
    n = len(groups[0])
    copies = jnp.broadcast_to(block, (n, *block.shape))
    return lax.all_to_all(
        copies, "sp", split_axis=0, concat_axis=0, tiled=True, axis_index_groups=groups
    )


def lines(block):
    return to_group(block, ALONG_Y + ALONG_Z)


def plane(copies):
    return lax.all_to_all(
        copies, "sp", split_axis=0, concat_axis=0, tiled=True,
        axis_index_groups=ALONG_Z0 + ALONG_Y1,
    )


def after(v, earlier):
    return lax.optimization_barrier((v, earlier))[0]


def swap_cores(v):
    count = lax.axis_size("sp")
    return lax.ppermute(v, "sp", [(i, i ^ 1) for i in range(count)])


def to_column_owner(v):
    nb = NZ // NX
    pairs = []
    for z in range(NZ):
        a, b = divmod(z, nb)
        for y in range(NY):
            for c in range(2):
                for x in range(NX):
                    place = (x * nb + b, y) if c == 0 else (y, x * nb + b)
                    pairs.append((at(z, y, c) * NX + x, at(*place, c) * NX + a))
    return lax.ppermute(v, ("sp", "x"), pairs)


def along_x(v, step):
    return lax.ppermute(v, "x", [(i, (i + step) % NX) for i in range(NX)])


def from_all_x(v):
    return [v] + [along_x(v, step) for step in range(1, NX)]


def exchange_x(copies):
    return [lax.all_to_all(copies, "x", split_axis=0, concat_axis=0, tiled=True)]


def part_of(refs, k):
    if len(refs) == 1:
        return refs[0].at[k], k
    return refs[k], (lax.axis_index("x") + NX - k) % NX


def core_here():
    return lax.axis_index("sp") % 2


def norm_kernel(layer, n, *refs):
    parts, (gain, out, scale, xs, sem) = refs[:n], refs[n:]

    def squares(i, _):
        rows = pl.ds(pl.multiple_of(i * 16, 16), 16)
        total = jnp.zeros((16, 128), F32)
        for k in range(NX):
            v = part_of(parts, k)[0][rows, :].astype(F32)
            sq = v * v
            for q in range(FEAT // 128):
                total += sq[:, q * 128 : (q + 1) * 128]
        scale[rows, :] = total
        return 0

    steps = scale.shape[0] // 16
    lax.fori_loop(0, steps, squares, 0, unroll=2)
    mean = jnp.sum(scale[...], axis=1, keepdims=True) / (NX * FEAT)
    scale[...] = jnp.broadcast_to(lax.rsqrt(mean + 1e-06), scale.shape)

    def apply(i, _):
        rows = pl.ds(pl.multiple_of(i * 16, 16), 16)
        factor = jnp.concatenate([scale[rows, :]] * (FEAT // 128), axis=1)
        for k in range(NX):
            ref, owner = part_of(parts, k)
            xs[owner, rows, :] = (ref[rows, :].astype(F32) * factor * gain[layer * NX + owner]).astype(BF)
        return 0

    lax.fori_loop(0, steps, apply, 0, unroll=2)
    done = pltpu.make_async_copy(xs, out, sem)
    done.start()
    done.wait()


def mix_kernel(source, mine, other, glu, vs, gs, xs, sem):
    fetch = pltpu.make_async_copy(source, xs, sem)
    fetch.start()

    def fill(zy, yz):
        for z in range(NZ):
            for c, w in enumerate((zy.at[z], yz.at[:, z])):
                vs[z, :, c] = w[:, :16, :]
                gs[z, :, c] = w[:, 16:32, :]

    @pl.when(core_here() == 0)
    def _():
        fill(mine, other)

    @pl.when(core_here() == 1)
    def _():
        fill(other, mine)

    fetch.wait()
    value = jnp.zeros(glu.shape, F32)
    gate = jnp.zeros(glu.shape, F32)
    for k in range(NX):
        planes = slice(2 * k, 2 * k + 2)
        value += jnp.dot(xs[k], vs[planes].reshape(FEAT, CH), preferred_element_type=F32)
        gate += jnp.dot(xs[k], gs[planes].reshape(FEAT, CH), preferred_element_type=F32)
    glu[...] = (value * jax.nn.sigmoid(gate)).astype(BF)


def split_three(v):
    hi = v.astype(BF).astype(F32)
    mid = (v - hi).astype(BF).astype(F32)
    return [hi, mid, v - hi - mid]


def send_all(src, out, sems):
    copies = [pltpu.make_async_copy(src, out.at[k], sems.at[k]) for k in range(out.shape[0])]
    for c in copies:
        c.start()
    for c in copies:
        c.wait()


def spread_kernel(layer, once, out, sems):
    send_all(once.at[:, layer], out, sems)


def taps_over(layer, ext, taps, conv, shifted):
    rows = conv.shape[0]
    for b in range(8):
        shifted[b] = ext[1 + b : 1 + b + rows + TAPS - 8, :]
    for lane in range(0, CH, 128):
        for base in range(0, rows, HALF):

            def step(a, acc):
                start = pl.multiple_of(a * 8, 8)
                tap = taps[layer, pl.ds(start, 8), lane : lane + 128]
                for b in range(8):
                    window = shifted[b, pl.ds(start + base, HALF), lane : lane + 128]
                    acc += window * tap[b : b + 1]
                return acc

            acc = lax.fori_loop(0, TAPS // 8, step, jnp.zeros((HALF, 128), F32))
            conv[base : base + HALF, lane : lane + 128] = acc


def pack(layer, conv, gain, out):
    ones = jnp.full((8, CH), 1.0 / CH, F32)
    means = lax.dot_general(
        ones, conv[...], (((1,), (1,)), ((), ())), precision=lax.Precision.HIGHEST,
        preferred_element_type=F32,
    )[:1]
    extra = split_three(means) + split_three(gain[layer : layer + 1, :])
    out[TOK:, :] = jnp.concatenate(extra + [jnp.zeros((10, CH), F32)], axis=0).astype(BF)
    v = conv[...]
    out[:TOK, :] = (v - jnp.mean(v, axis=1, keepdims=True)).astype(BF)


def whole_kernel(layer, glu, taps, gain, out, ext, shifted, conv):
    ext[...] = glu[...].astype(F32)
    taps_over(layer, ext, taps, conv, shifted)
    pack(layer, conv, gain, out)


def late_kernel(layer, glu, taps, conv, ext, shifted):
    ext[...] = glu[...].astype(F32)
    taps_over(layer, ext, taps, conv, shifted)


def conv_kernel(layer, before, glu, late, taps, gain, out, ext, shifted, conv, packed, sems):
    ext[:TAPS, :] = before[...].astype(F32)
    ext[TAPS:, :] = glu[:HALF, :].astype(F32)
    taps_over(layer, ext, taps, conv.at[:HALF], shifted)
    conv[HALF:, :] = late[...]
    pack(layer, conv, gain, packed)
    send_all(packed, out, sems)


def out_kernel(n, *refs):
    parts, rest = refs[:n], refs[n:]
    x, source, out, means, scale, acts, held, wt, sems = rest
    weights = pltpu.make_async_copy(source, wt, sems.at[1])
    weights.start()
    mine = x if len(x.shape) == 2 else x.at[lax.axis_index("x")]
    fetch = pltpu.make_async_copy(mine, held, sems.at[0])
    fetch.start()
    pick = (lax.broadcasted_iota(jnp.int32, (16, 128), 0) < 3).astype(BF)
    total = jnp.zeros((TOK, 128), F32)
    for k in range(NX):
        m = lax.dot_general(
            part_of(parts, k)[0][TOK:, :], pick, (((0,), (0,)), ((), ())),
            preferred_element_type=F32,
        )
        means[k] = m
        total += m
    for k in range(NX):
        means[k] = means[k] - total / NX

    def shifted_part(k, rows):
        ref, owner = part_of(parts, k)
        v = ref[rows, :].astype(F32)
        shift = means[k, rows, :]
        return jnp.concatenate([v[:, :128] + shift, v[:, 128:] + shift], axis=1), owner

    def squares(i, _):
        rows = pl.ds(pl.multiple_of(i * 16, 16), 16)
        square = jnp.zeros((16, 128), F32)
        for k in range(NX):
            v, _ = shifted_part(k, rows)
            sq = v * v
            square += sq[:, :128] + sq[:, 128:]
        scale[rows, :] = square
        return 0

    lax.fori_loop(0, TOK // 16, squares, 0, unroll=2)
    spread = jnp.sum(scale[...], axis=1, keepdims=True) / C
    scale[...] = jnp.broadcast_to(lax.rsqrt(spread + 1e-05), (TOK, 128))
    gains = []
    for k in range(NX):
        tail = part_of(parts, k)[0][TOK:, :].astype(F32)
        gains.append(tail[3:4] + tail[4:5] + tail[5:6])

    def activate(i, _):
        rows = pl.ds(pl.multiple_of(i * 16, 16), 16)
        factor = jnp.concatenate([scale[rows, :]] * 2, axis=1)
        for k in range(NX):
            v, owner = shifted_part(k, rows)
            u = v * factor * gains[k]
            acts[owner, rows, :] = (u / (1.0 + jnp.exp(-u))).astype(BF)
        return 0

    lax.fori_loop(0, TOK // 16, activate, 0, unroll=2)
    weights.wait()
    branch = jnp.zeros((TOK, FEAT), F32)
    for k in range(NX):
        branch += lax.dot_general(
            acts[k], wt[k].reshape(FEAT, CH), (((1,), (1,)), ((), ())),
            preferred_element_type=F32,
        )
    fetch.wait()
    new = (held[...].astype(F32) + branch).astype(BF)
    if len(out.shape) == 2:
        out[...] = new
    else:
        held[...] = new
        send_all(held, out, sems)


def in_hbm(v):
    return v if INTERPRET else pltpu.with_memory_space_constraint(v, pltpu.HBM)


def call(body, out, ins, scratch, flops, place=pltpu.VMEM, loose=(), far=()):
    def spot(i):
        return pltpu.HBM if i in far else pl.ANY if i in loose else pltpu.VMEM

    spec = pl.BlockSpec(memory_space=place)
    return pl.pallas_call(
        body,
        out_shape=out,
        in_specs=[pl.BlockSpec(memory_space=spot(i)) for i in range(len(ins))],
        out_specs=spec,
        scratch_shapes=scratch,
        cost_estimate=pl.CostEstimate(flops=flops, transcendentals=0, bytes_accessed=1 << 20),
        compiler_params=pltpu.CompilerParams(vmem_limit_bytes=14 << 20),
        interpret=INTERPRET,
    )(*(in_hbm(v) if i in far else v for i, v in enumerate(ins)))


def normalise(layer, parts, gain):
    def body(*refs):
        norm_kernel(layer, len(parts), *refs)

    return call(
        body,
        pltpu.HBM((NX, parts[0].shape[-2], FEAT), BF),
        [*parts, gain],
        [
            pltpu.VMEM((parts[0].shape[-2], 128), F32),
            pltpu.VMEM((NX, parts[0].shape[-2], FEAT), BF),
            pltpu.SemaphoreType.DMA(()),
        ],
        8 * NX * TOK * FEAT,
        pltpu.HBM,
    )


def mix(xs, mine, other):
    weights = pltpu.VMEM((NZ, NY, 2, 16, CH), BF)
    return call(
        mix_kernel,
        jax.ShapeDtypeStruct((xs.shape[1], CH), BF),
        [xs, mine, other],
        [weights, weights, pltpu.VMEM(xs.shape, BF), pltpu.SemaphoreType.DMA(())],
        4 * NX * TOK * FEAT * CH,
        far=(0,),
    )


def arrange_kernel(mine, other, wt, sems):
    def fill(halves):
        copies = []
        for k in range(NX):
            for c, w in enumerate(halves):
                part = w.at[2 * k : 2 * k + 2, :, 32:, :]
                copies.append(
                    pltpu.make_async_copy(part, wt.at[k, :, :, c], sems.at[2 * k + c])
                )
        for one in copies:
            one.start()
        for one in copies:
            one.wait()

    @pl.when(core_here() == 0)
    def _():
        fill((mine, other))

    @pl.when(core_here() == 1)
    def _():
        fill((other, mine))


def arrange(mine, other):
    return call(
        arrange_kernel,
        pltpu.HBM((NX, 2, NY, 2, 16, CH), BF),
        [mine, other],
        [pltpu.SemaphoreType.DMA((2 * NX,))],
        1 << 26,
        pltpu.HBM,
        (0, 1),
    )


def conv_late(layer, glu, taps):
    def body(*refs):
        late_kernel(layer, *refs)

    return call(
        body,
        jax.ShapeDtypeStruct((HALF, CH), F32),
        [glu, taps],
        [pltpu.VMEM((TOK, CH), F32), pltpu.VMEM((8, SPAN, CH), F32)],
        2 * HALF * CH * TAPS,
    )


def conv_whole(layer, glu, taps, gain):
    def body(*refs):
        whole_kernel(layer, *refs)

    return call(
        body,
        jax.ShapeDtypeStruct((PACK, CH), BF),
        [glu, taps, gain],
        [
            pltpu.VMEM((TAPS + TOK, CH), F32),
            pltpu.VMEM((8, TOK + TAPS - 8, CH), F32),
            pltpu.VMEM((TOK, CH), F32),
        ],
        2 * TOK * CH * TAPS,
    )


def convolve(layer, before, glu, late, taps, gain):
    def body(*refs):
        conv_kernel(layer, *refs)

    return call(
        body,
        pltpu.HBM((NX, PACK, CH), BF),
        [before, glu, late, taps, gain],
        [
            pltpu.VMEM((TAPS + HALF, CH), F32),
            pltpu.VMEM((8, SPAN, CH), F32),
            pltpu.VMEM((TOK, CH), F32),
            pltpu.VMEM((PACK, CH), BF),
            pltpu.SemaphoreType.DMA((NX,)),
        ],
        2 * HALF * CH * TAPS,
        pltpu.HBM,
    )


def spread(layer, once):
    def body(*refs):
        spread_kernel(layer, *refs)

    return call(
        body,
        jax.ShapeDtypeStruct((NZ, NZ, 48, CH), BF),
        [once],
        [pltpu.SemaphoreType.DMA((NZ,))],
        1 << 26,
        pltpu.HBM,
    )


def project(parts, x, wt, to_all):
    def body(*refs):
        out_kernel(len(parts), *refs)

    shape = jax.ShapeDtypeStruct((TOK, FEAT), BF)
    copies = pltpu.HBM((NX, TOK, FEAT), BF)
    inside, far = pl.BlockSpec(memory_space=pltpu.VMEM), pl.BlockSpec(memory_space=pltpu.HBM)
    return pl.pallas_call(
        body,
        out_shape=copies if to_all else shape,
        in_specs=[inside] * len(parts) + [far, far],
        out_specs=far if to_all else inside,
        scratch_shapes=[
            pltpu.VMEM((NX, TOK, 128), F32),
            pltpu.VMEM((TOK, 128), F32),
            pltpu.VMEM((NX, TOK, CH), BF),
            pltpu.VMEM((TOK, FEAT), BF),
            pltpu.VMEM(wt.shape, BF),
            pltpu.SemaphoreType.DMA((NX,)),
        ],
        cost_estimate=pl.CostEstimate(
            flops=2 * NX * TOK * CH * FEAT, transcendentals=0, bytes_accessed=1 << 20
        ),
        compiler_params=pltpu.CompilerParams(vmem_limit_bytes=14 << 20),
        interpret=INTERPRET,
    )(*parts, in_hbm(x), in_hbm(wt))


def shards(stream, norm_gain, w_value, w_gate, conv_taps, channel_gain, w_out):
    gain = norm_gain.reshape(LAYERS * NX, 1, FEAT)
    out_t = to_column_owner(jnp.swapaxes(w_out, 1, 2))
    blocks = jnp.concatenate([w_value, w_gate, out_t], axis=1)

    x = stream
    count = lax.axis_size("sp")
    chain = [(i, i + 1) for i in range(count - 1)]
    extended = jnp.concatenate([lax.ppermute(x[TOK - TAPS :], "sp", chain), x])
    once = lines(blocks)
    extended = after(extended, blocks)
    parts = [extended, along_x(extended, 1), along_x(extended, 2)]
    parts.append(along_x(extended, 3))
    ready = spread(0, once)
    gathered = plane(ready)
    ready = spread(1, once)
    normed = normalise(0, parts, gain)
    other = swap_cores(gathered)
    following = plane(after(ready, gathered))
    glu = mix(normed, gathered, other)
    packed = conv_whole(0, glu, conv_taps, channel_gain)
    parts = from_all_x(packed)
    wt = arrange(after(gathered, packed), other)
    copies = project(parts, x, wt, True)

    xs = exchange_x(copies)
    other = swap_cores(following)
    normed = normalise(1, xs, gain)
    glu = mix(normed, following, other)
    before = lax.ppermute(glu[TOK - TAPS :], "sp", chain)
    late = conv_late(1, glu, conv_taps)
    copies = convolve(1, before, glu, late, conv_taps, channel_gain)
    parts = exchange_x(copies)
    wt = arrange(after(following, copies), other)
    x = project(parts, xs[0], wt, False)
    return x


def solution(mesh):
    flat = Mesh(mesh.devices, ("sp", "x"))
    in_specs = (
        P("sp", "x"),
        P(),
        P(None, "sp", "x"),
        P(None, "sp", "x"),
        P(None, None, "x"),
        P(None, "x"),
        P(None, "x", "sp"),
    )

    return jax.shard_map(shards, mesh=flat, in_specs=in_specs, out_specs=P("sp", "x"), check_vma=False)
```

```python
import jax
import jax.numpy as jnp
from jax import lax
from jax.experimental import pallas as pl
from jax.experimental.pallas import tpu as pltpu
from jax.sharding import Mesh
from jax.sharding import PartitionSpec as P


C = 1024
LAYERS = 2
NZ, NY, NX = 8, 8, 4
TOK, CH, TAPS, FEAT = 256, 256, 128, 512
PACK = TOK + 16
HALF = TOK // 2
SPAN = HALF + TAPS - 8
BF = jnp.bfloat16
F32 = jnp.float32
INTERPRET = False


def at(z, y, c):
    return (z * NY + y) * 2 + c


ALONG_Y = [[at(z, y, 0) for y in range(NY)] for z in range(NZ)]
ALONG_Z = [[at(z, y, 1) for z in range(NZ)] for y in range(NY)]
ALONG_Y1 = [[at(z, y, 1) for y in range(NY)] for z in range(NZ)]
ALONG_Z0 = [[at(z, y, 0) for z in range(NZ)] for y in range(NY)]


def to_group(block, groups):
    n = len(groups[0])
    copies = jnp.broadcast_to(block, (n, *block.shape))
    return lax.all_to_all(
        copies, "sp", split_axis=0, concat_axis=0, tiled=True, axis_index_groups=groups
    )


def lines(block):
    return to_group(block, ALONG_Y + ALONG_Z)


def plane(copies):
    return lax.all_to_all(
        copies, "sp", split_axis=0, concat_axis=0, tiled=True,
        axis_index_groups=ALONG_Z0 + ALONG_Y1,
    )


def after(v, earlier):
    return lax.optimization_barrier((v, earlier))[0]


def swap_cores(v):
    count = lax.axis_size("sp")
    return lax.ppermute(v, "sp", [(i, i ^ 1) for i in range(count)])


def to_column_owner(v):
    nb = NZ // NX
    pairs = []
    for z in range(NZ):
        a, b = divmod(z, nb)
        for y in range(NY):
            for c in range(2):
                for x in range(NX):
                    place = (x * nb + b, y) if c == 0 else (y, x * nb + b)
                    pairs.append((at(z, y, c) * NX + x, at(*place, c) * NX + a))
    return lax.ppermute(v, ("sp", "x"), pairs)


def along_x(v, step):
    return lax.ppermute(v, "x", [(i, (i + step) % NX) for i in range(NX)])


def from_all_x(v):
    return [v] + [along_x(v, step) for step in range(1, NX)]


def exchange_x(copies):
    return [lax.all_to_all(copies, "x", split_axis=0, concat_axis=0, tiled=True)]


def part_of(refs, k):
    if len(refs) == 1:
        return refs[0].at[k], k
    return refs[k], (lax.axis_index("x") + NX - k) % NX


def core_here():
    return lax.axis_index("sp") % 2


def norm_kernel(layer, n, *refs):
    parts, (gain, xs, scale) = refs[:n], refs[n:]

    def squares(i, _):
        rows = pl.ds(pl.multiple_of(i * 16, 16), 16)
        total = jnp.zeros((16, 128), F32)
        for k in range(NX):
            v = part_of(parts, k)[0][rows, :].astype(F32)
            sq = v * v
            for q in range(FEAT // 128):
                total += sq[:, q * 128 : (q + 1) * 128]
        scale[rows, :] = total
        return 0

    steps = scale.shape[0] // 16
    lax.fori_loop(0, steps, squares, 0, unroll=2)
    mean = jnp.sum(scale[...], axis=1, keepdims=True) / (NX * FEAT)
    scale[...] = jnp.broadcast_to(lax.rsqrt(mean + 1e-06), scale.shape)

    def apply(i, _):
        rows = pl.ds(pl.multiple_of(i * 16, 16), 16)
        factor = jnp.concatenate([scale[rows, :]] * (FEAT // 128), axis=1)
        for k in range(NX):
            ref, owner = part_of(parts, k)
            xs[owner, rows, :] = (ref[rows, :].astype(F32) * factor * gain[layer * NX + owner]).astype(BF)
        return 0

    lax.fori_loop(0, steps, apply, 0, unroll=2)


def mix_kernel(xs, mine, other, glu, vs, gs):
    def fill(zy, yz):
        for z in range(NZ):
            for c, w in enumerate((zy.at[z], yz.at[:, z])):
                vs[z, :, c] = w[:, :16, :]
                gs[z, :, c] = w[:, 16:32, :]

    @pl.when(core_here() == 0)
    def _():
        fill(mine, other)

    @pl.when(core_here() == 1)
    def _():
        fill(other, mine)

    value = jnp.zeros(glu.shape, F32)
    gate = jnp.zeros(glu.shape, F32)
    for k in range(NX):
        planes = slice(2 * k, 2 * k + 2)
        value += jnp.dot(xs[k], vs[planes].reshape(FEAT, CH), preferred_element_type=F32)
        gate += jnp.dot(xs[k], gs[planes].reshape(FEAT, CH), preferred_element_type=F32)
    glu[...] = (value * jax.nn.sigmoid(gate)).astype(BF)


def split_three(v):
    hi = v.astype(BF).astype(F32)
    mid = (v - hi).astype(BF).astype(F32)
    return [hi, mid, v - hi - mid]


def send_all(src, out, sems):
    copies = [pltpu.make_async_copy(src, out.at[k], sems.at[k]) for k in range(out.shape[0])]
    for c in copies:
        c.start()
    for c in copies:
        c.wait()


def spread_kernel(layer, once, out, sems):
    send_all(once.at[:, layer], out, sems)


def taps_over(layer, ext, taps, conv, shifted):
    rows = conv.shape[0]
    for b in range(8):
        shifted[b] = ext[1 + b : 1 + b + rows + TAPS - 8, :]
    for lane in range(0, CH, 128):
        for base in range(0, rows, HALF):

            def step(a, acc):
                start = pl.multiple_of(a * 8, 8)
                tap = taps[layer, pl.ds(start, 8), lane : lane + 128]
                for b in range(8):
                    window = shifted[b, pl.ds(start + base, HALF), lane : lane + 128]
                    acc += window * tap[b : b + 1]
                return acc

            acc = lax.fori_loop(0, TAPS // 8, step, jnp.zeros((HALF, 128), F32))
            conv[base : base + HALF, lane : lane + 128] = acc


def pack(layer, conv, gain, out):
    ones = jnp.full((8, CH), 1.0 / CH, F32)
    means = lax.dot_general(
        ones, conv[...], (((1,), (1,)), ((), ())), precision=lax.Precision.HIGHEST,
        preferred_element_type=F32,
    )[:1]
    extra = split_three(means) + split_three(gain[layer : layer + 1, :])
    out[TOK:, :] = jnp.concatenate(extra + [jnp.zeros((10, CH), F32)], axis=0).astype(BF)
    v = conv[...]
    out[:TOK, :] = (v - jnp.mean(v, axis=1, keepdims=True)).astype(BF)


def whole_kernel(layer, glu, taps, gain, out, ext, shifted, conv):
    ext[...] = glu[...].astype(F32)
    taps_over(layer, ext, taps, conv, shifted)
    pack(layer, conv, gain, out)


def late_kernel(layer, glu, taps, conv, ext, shifted):
    ext[...] = glu[...].astype(F32)
    taps_over(layer, ext, taps, conv, shifted)


def conv_kernel(layer, before, glu, late, taps, gain, out, ext, shifted, conv, packed, sems):
    ext[:TAPS, :] = before[...].astype(F32)
    ext[TAPS:, :] = glu[:HALF, :].astype(F32)
    taps_over(layer, ext, taps, conv.at[:HALF], shifted)
    conv[HALF:, :] = late[...]
    pack(layer, conv, gain, packed)
    send_all(packed, out, sems)


def out_kernel(n, *refs):
    parts, rest = refs[:n], refs[n:]
    x, source, out, means, scale, acts, held, wt, sems = rest
    weights = pltpu.make_async_copy(source, wt, sems.at[1])
    weights.start()
    mine = x if len(x.shape) == 2 else x.at[lax.axis_index("x")]
    fetch = pltpu.make_async_copy(mine, held, sems.at[0])
    fetch.start()
    pick = (lax.broadcasted_iota(jnp.int32, (16, 128), 0) < 3).astype(BF)
    total = jnp.zeros((TOK, 128), F32)
    for k in range(NX):
        m = lax.dot_general(
            part_of(parts, k)[0][TOK:, :], pick, (((0,), (0,)), ((), ())),
            preferred_element_type=F32,
        )
        means[k] = m
        total += m
    for k in range(NX):
        means[k] = means[k] - total / NX

    def shifted_part(k, rows):
        ref, owner = part_of(parts, k)
        v = ref[rows, :].astype(F32)
        shift = means[k, rows, :]
        return jnp.concatenate([v[:, :128] + shift, v[:, 128:] + shift], axis=1), owner

    def squares(i, _):
        rows = pl.ds(pl.multiple_of(i * 16, 16), 16)
        square = jnp.zeros((16, 128), F32)
        for k in range(NX):
            v, _ = shifted_part(k, rows)
            sq = v * v
            square += sq[:, :128] + sq[:, 128:]
        scale[rows, :] = square
        return 0

    lax.fori_loop(0, TOK // 16, squares, 0, unroll=2)
    spread = jnp.sum(scale[...], axis=1, keepdims=True) / C
    scale[...] = jnp.broadcast_to(lax.rsqrt(spread + 1e-05), (TOK, 128))
    gains = []
    for k in range(NX):
        tail = part_of(parts, k)[0][TOK:, :].astype(F32)
        gains.append(tail[3:4] + tail[4:5] + tail[5:6])

    def activate(i, _):
        rows = pl.ds(pl.multiple_of(i * 16, 16), 16)
        factor = jnp.concatenate([scale[rows, :]] * 2, axis=1)
        for k in range(NX):
            v, owner = shifted_part(k, rows)
            u = v * factor * gains[k]
            acts[owner, rows, :] = (u / (1.0 + jnp.exp(-u))).astype(BF)
        return 0

    lax.fori_loop(0, TOK // 16, activate, 0, unroll=2)
    weights.wait()
    branch = jnp.zeros((TOK, FEAT), F32)
    for k in range(NX):
        branch += lax.dot_general(
            acts[k], wt[k].reshape(FEAT, CH), (((1,), (1,)), ((), ())),
            preferred_element_type=F32,
        )
    fetch.wait()
    new = (held[...].astype(F32) + branch).astype(BF)
    if len(out.shape) == 2:
        out[...] = new
    else:
        held[...] = new
        send_all(held, out, sems)


def in_hbm(v):
    return v if INTERPRET else pltpu.with_memory_space_constraint(v, pltpu.HBM)


def call(body, out, ins, scratch, flops, place=pltpu.VMEM):
    spec = pl.BlockSpec(memory_space=place)
    return pl.pallas_call(
        body,
        out_shape=out,
        in_specs=[pl.BlockSpec(memory_space=pltpu.VMEM)] * len(ins),
        out_specs=spec,
        scratch_shapes=scratch,
        cost_estimate=pl.CostEstimate(flops=flops, transcendentals=0, bytes_accessed=1 << 20),
        compiler_params=pltpu.CompilerParams(vmem_limit_bytes=14 << 20),
        interpret=INTERPRET,
    )(*ins)


def normalise(layer, parts, gain):
    def body(*refs):
        norm_kernel(layer, len(parts), *refs)

    return call(
        body,
        jax.ShapeDtypeStruct((NX, parts[0].shape[-2], FEAT), BF),
        [*parts, gain],
        [pltpu.VMEM((parts[0].shape[-2], 128), F32)],
        8 * NX * TOK * FEAT,
    )


def mix(xs, mine, other):
    weights = pltpu.VMEM((NZ, NY, 2, 16, CH), BF)
    return call(
        mix_kernel,
        jax.ShapeDtypeStruct((xs.shape[1], CH), BF),
        [xs, mine, other],
        [weights, weights],
        4 * NX * TOK * FEAT * CH,
    )


def arrange_kernel(mine, other, out, wt, sem):
    def fill(halves):
        for k in range(NX):
            for c, w in enumerate(halves):
                wt[k, :, :, c] = w[2 * k : 2 * k + 2, :, 32:, :]

    @pl.when(core_here() == 0)
    def _():
        fill((mine, other))

    @pl.when(core_here() == 1)
    def _():
        fill((other, mine))

    done = pltpu.make_async_copy(wt, out, sem)
    done.start()
    done.wait()


def arrange(mine, other):
    shape = (NX, 2, NY, 2, 16, CH)
    return call(
        arrange_kernel,
        pltpu.HBM(shape, BF),
        [mine, other],
        [pltpu.VMEM(shape, BF), pltpu.SemaphoreType.DMA(())],
        1 << 26,
        pltpu.HBM,
    )


def conv_late(layer, glu, taps):
    def body(*refs):
        late_kernel(layer, *refs)

    return call(
        body,
        jax.ShapeDtypeStruct((HALF, CH), F32),
        [glu, taps],
        [pltpu.VMEM((TOK, CH), F32), pltpu.VMEM((8, SPAN, CH), F32)],
        2 * HALF * CH * TAPS,
    )


def conv_whole(layer, glu, taps, gain):
    def body(*refs):
        whole_kernel(layer, *refs)

    return call(
        body,
        jax.ShapeDtypeStruct((PACK, CH), BF),
        [glu, taps, gain],
        [
            pltpu.VMEM((TAPS + TOK, CH), F32),
            pltpu.VMEM((8, TOK + TAPS - 8, CH), F32),
            pltpu.VMEM((TOK, CH), F32),
        ],
        2 * TOK * CH * TAPS,
    )


def convolve(layer, before, glu, late, taps, gain):
    def body(*refs):
        conv_kernel(layer, *refs)

    return call(
        body,
        pltpu.HBM((NX, PACK, CH), BF),
        [before, glu, late, taps, gain],
        [
            pltpu.VMEM((TAPS + HALF, CH), F32),
            pltpu.VMEM((8, SPAN, CH), F32),
            pltpu.VMEM((TOK, CH), F32),
            pltpu.VMEM((PACK, CH), BF),
            pltpu.SemaphoreType.DMA((NX,)),
        ],
        2 * HALF * CH * TAPS,
        pltpu.HBM,
    )


def spread(layer, once):
    def body(*refs):
        spread_kernel(layer, *refs)

    return call(
        body,
        jax.ShapeDtypeStruct((NZ, NZ, 48, CH), BF),
        [once],
        [pltpu.SemaphoreType.DMA((NZ,))],
        1 << 26,
        pltpu.HBM,
    )


def project(parts, x, wt, to_all):
    def body(*refs):
        out_kernel(len(parts), *refs)

    shape = jax.ShapeDtypeStruct((TOK, FEAT), BF)
    copies = pltpu.HBM((NX, TOK, FEAT), BF)
    inside, far = pl.BlockSpec(memory_space=pltpu.VMEM), pl.BlockSpec(memory_space=pltpu.HBM)
    return pl.pallas_call(
        body,
        out_shape=copies if to_all else shape,
        in_specs=[inside] * len(parts) + [far, far],
        out_specs=far if to_all else inside,
        scratch_shapes=[
            pltpu.VMEM((NX, TOK, 128), F32),
            pltpu.VMEM((TOK, 128), F32),
            pltpu.VMEM((NX, TOK, CH), BF),
            pltpu.VMEM((TOK, FEAT), BF),
            pltpu.VMEM(wt.shape, BF),
            pltpu.SemaphoreType.DMA((NX,)),
        ],
        cost_estimate=pl.CostEstimate(
            flops=2 * NX * TOK * CH * FEAT, transcendentals=0, bytes_accessed=1 << 20
        ),
        compiler_params=pltpu.CompilerParams(vmem_limit_bytes=14 << 20),
        interpret=INTERPRET,
    )(*parts, in_hbm(x), in_hbm(wt))


def shards(stream, norm_gain, w_value, w_gate, conv_taps, channel_gain, w_out):
    gain = norm_gain.reshape(LAYERS * NX, 1, FEAT)
    out_t = to_column_owner(jnp.swapaxes(w_out, 1, 2))
    blocks = jnp.concatenate([w_value, w_gate, out_t], axis=1)

    x = stream
    count = lax.axis_size("sp")
    chain = [(i, i + 1) for i in range(count - 1)]
    extended = jnp.concatenate([lax.ppermute(x[TOK - TAPS :], "sp", chain), x])
    once = lines(blocks)
    extended = after(extended, blocks)
    parts = [extended, along_x(extended, 1), along_x(extended, 2)]
    parts.append(along_x(extended, 3))
    ready = spread(0, once)
    gathered = plane(ready)
    ready = spread(1, once)
    normed = normalise(0, parts, gain)
    other = swap_cores(gathered)
    following = plane(after(ready, gathered))
    glu = mix(normed, gathered, other)
    packed = conv_whole(0, glu, conv_taps, channel_gain)
    parts = from_all_x(packed)
    wt = arrange(after(gathered, packed), other)
    copies = project(parts, x, wt, True)

    xs = exchange_x(copies)
    other = swap_cores(following)
    normed = normalise(1, xs, gain)
    glu = mix(normed, following, other)
    before = lax.ppermute(glu[TOK - TAPS :], "sp", chain)
    late = conv_late(1, glu, conv_taps)
    copies = convolve(1, before, glu, late, conv_taps, channel_gain)
    parts = exchange_x(copies)
    wt = arrange(after(following, copies), other)
    x = project(parts, xs[0], wt, False)
    return x


def solution(mesh):
    flat = Mesh(mesh.devices, ("sp", "x"))
    in_specs = (
        P("sp", "x"),
        P(),
        P(None, "sp", "x"),
        P(None, "sp", "x"),
        P(None, None, "x"),
        P(None, "x"),
        P(None, "x", "sp"),
    )

    return jax.shard_map(shards, mesh=flat, in_specs=in_specs, out_specs=P("sp", "x"), check_vma=False)
```

```python
import jax
import jax.numpy as jnp
from jax import lax
from jax.experimental import pallas as pl
from jax.experimental.pallas import tpu as pltpu
from jax.sharding import Mesh
from jax.sharding import PartitionSpec as P


C = 1024
LAYERS = 2
NZ, NY, NX = 8, 8, 4
TOK, CH, TAPS, FEAT = 256, 256, 128, 512
PACK = TOK + 16
HALF = TOK // 2
SPAN = HALF + TAPS - 8
BF = jnp.bfloat16
F32 = jnp.float32
INTERPRET = False


def at(z, y, c):
    return (z * NY + y) * 2 + c


ALONG_Y = [[at(z, y, 0) for y in range(NY)] for z in range(NZ)]
ALONG_Z = [[at(z, y, 1) for z in range(NZ)] for y in range(NY)]
ALONG_Y1 = [[at(z, y, 1) for y in range(NY)] for z in range(NZ)]
ALONG_Z0 = [[at(z, y, 0) for z in range(NZ)] for y in range(NY)]


def to_group(block, groups):
    n = len(groups[0])
    copies = jnp.broadcast_to(block, (n, *block.shape))
    return lax.all_to_all(
        copies, "sp", split_axis=0, concat_axis=0, tiled=True, axis_index_groups=groups
    )


def lines(block):
    return to_group(block, ALONG_Y + ALONG_Z)


def plane(copies):
    return lax.all_to_all(
        copies, "sp", split_axis=0, concat_axis=0, tiled=True,
        axis_index_groups=ALONG_Z0 + ALONG_Y1,
    )


def after(v, earlier):
    return lax.optimization_barrier((v, earlier))[0]


def swap_cores(v):
    count = lax.axis_size("sp")
    return lax.ppermute(v, "sp", [(i, i ^ 1) for i in range(count)])


def to_column_owner(v):
    nb = NZ // NX
    pairs = []
    for z in range(NZ):
        a, b = divmod(z, nb)
        for y in range(NY):
            for c in range(2):
                for x in range(NX):
                    place = (x * nb + b, y) if c == 0 else (y, x * nb + b)
                    pairs.append((at(z, y, c) * NX + x, at(*place, c) * NX + a))
    return lax.ppermute(v, ("sp", "x"), pairs)


def along_x(v, step):
    return lax.ppermute(v, "x", [(i, (i + step) % NX) for i in range(NX)])


def from_all_x(v):
    return [v] + [along_x(v, step) for step in range(1, NX)]


def exchange_x(copies):
    return [lax.all_to_all(copies, "x", split_axis=0, concat_axis=0, tiled=True)]


def part_of(refs, k):
    if len(refs) == 1:
        return refs[0].at[k], k
    return refs[k], (lax.axis_index("x") + NX - k) % NX


def core_here():
    return lax.axis_index("sp") % 2


def norm_kernel(layer, n, *refs):
    parts, (gain, xs, scale, *spare) = refs[:n], refs[n:]
    out = xs
    if spare:
        xs = spare[0]

    def squares(i, _):
        rows = pl.ds(pl.multiple_of(i * 16, 16), 16)
        total = jnp.zeros((16, 128), F32)
        for k in range(NX):
            v = part_of(parts, k)[0][rows, :].astype(F32)
            sq = v * v
            for q in range(FEAT // 128):
                total += sq[:, q * 128 : (q + 1) * 128]
        scale[rows, :] = total
        return 0

    steps = scale.shape[0] // 16
    lax.fori_loop(0, steps, squares, 0, unroll=2)
    mean = jnp.sum(scale[...], axis=1, keepdims=True) / (NX * FEAT)
    scale[...] = jnp.broadcast_to(lax.rsqrt(mean + 1e-06), scale.shape)

    def apply(i, _):
        rows = pl.ds(pl.multiple_of(i * 16, 16), 16)
        factor = jnp.concatenate([scale[rows, :]] * (FEAT // 128), axis=1)
        for k in range(NX):
            ref, owner = part_of(parts, k)
            xs[owner, rows, :] = (ref[rows, :].astype(F32) * factor * gain[layer * NX + owner]).astype(BF)
        return 0

    lax.fori_loop(0, steps, apply, 0, unroll=2)
    if spare:
        done = pltpu.make_async_copy(xs, out, spare[1])
        done.start()
        done.wait()


def mix_kernel(xs, mine, source, glu, vs, gs, other, sems, *spare):
    copies = [pltpu.make_async_copy(source, other, sems.at[0])]
    if spare:
        copies.append(pltpu.make_async_copy(xs, spare[0], sems.at[1]))
        xs = spare[0]
    for one in copies:
        one.start()

    def from_even(w):
        for z in range(NZ):
            vs[z, :, 0] = w[z, :, :16, :]
            gs[z, :, 0] = w[z, :, 16:32, :]

    def from_odd(w):
        for z in range(NZ):
            vs[z, :, 1] = w[:, z, :16, :]
            gs[z, :, 1] = w[:, z, 16:32, :]

    even = core_here() == 0
    pl.when(even)(lambda: from_even(mine))
    pl.when(jnp.logical_not(even))(lambda: from_odd(mine))
    for one in copies:
        one.wait()
    pl.when(even)(lambda: from_odd(other))
    pl.when(jnp.logical_not(even))(lambda: from_even(other))

    value = jnp.zeros(glu.shape, F32)
    gate = jnp.zeros(glu.shape, F32)
    for k in range(NX):
        planes = slice(2 * k, 2 * k + 2)
        value += jnp.dot(xs[k], vs[planes].reshape(FEAT, CH), preferred_element_type=F32)
        gate += jnp.dot(xs[k], gs[planes].reshape(FEAT, CH), preferred_element_type=F32)
    glu[...] = (value * jax.nn.sigmoid(gate)).astype(BF)


def split_three(v):
    hi = v.astype(BF).astype(F32)
    mid = (v - hi).astype(BF).astype(F32)
    return [hi, mid, v - hi - mid]


def send_all(src, out, sems):
    copies = [pltpu.make_async_copy(src, out.at[k], sems.at[k]) for k in range(out.shape[0])]
    for c in copies:
        c.start()
    for c in copies:
        c.wait()


def spread_kernel(layer, once, out, sems):
    send_all(once.at[:, layer], out, sems)


def taps_over(layer, ext, taps, conv, shifted):
    rows = conv.shape[0]
    for b in range(8):
        shifted[b] = ext[1 + b : 1 + b + rows + TAPS - 8, :]
    for lane in range(0, CH, 128):
        for base in range(0, rows, HALF):

            def step(a, acc):
                start = pl.multiple_of(a * 8, 8)
                tap = taps[layer, pl.ds(start, 8), lane : lane + 128]
                for b in range(8):
                    window = shifted[b, pl.ds(start + base, HALF), lane : lane + 128]
                    acc += window * tap[b : b + 1]
                return acc

            acc = lax.fori_loop(0, TAPS // 8, step, jnp.zeros((HALF, 128), F32))
            conv[base : base + HALF, lane : lane + 128] = acc


def pack(layer, conv, gain, out):
    ones = jnp.full((8, CH), 1.0 / CH, F32)
    means = lax.dot_general(
        ones, conv[...], (((1,), (1,)), ((), ())), precision=lax.Precision.HIGHEST,
        preferred_element_type=F32,
    )[:1]
    extra = split_three(means) + split_three(gain[layer : layer + 1, :])
    out[TOK:, :] = jnp.concatenate(extra + [jnp.zeros((10, CH), F32)], axis=0).astype(BF)
    v = conv[...]
    out[:TOK, :] = (v - jnp.mean(v, axis=1, keepdims=True)).astype(BF)


def whole_kernel(layer, glu, taps, gain, out, ext, shifted, conv):
    ext[...] = glu[...].astype(F32)
    taps_over(layer, ext, taps, conv, shifted)
    pack(layer, conv, gain, out)


def late_kernel(layer, glu, taps, conv, ext, shifted):
    ext[...] = glu[...].astype(F32)
    taps_over(layer, ext, taps, conv, shifted)


def conv_kernel(layer, before, glu, late, taps, gain, out, ext, shifted, conv, packed, sems):
    ext[:TAPS, :] = before[...].astype(F32)
    ext[TAPS:, :] = glu[:HALF, :].astype(F32)
    taps_over(layer, ext, taps, conv.at[:HALF], shifted)
    conv[HALF:, :] = late[...]
    pack(layer, conv, gain, packed)
    send_all(packed, out, sems)


def out_kernel(n, *refs):
    parts, rest = refs[:n], refs[n:]
    x, source, out, means, scale, acts, held, wt, sems = rest
    weights = pltpu.make_async_copy(source, wt, sems.at[1])
    weights.start()
    mine = x if len(x.shape) == 2 else x.at[lax.axis_index("x")]
    fetch = pltpu.make_async_copy(mine, held, sems.at[0])
    fetch.start()
    pick = (lax.broadcasted_iota(jnp.int32, (16, 128), 0) < 3).astype(BF)
    total = jnp.zeros((TOK, 128), F32)
    for k in range(NX):
        m = lax.dot_general(
            part_of(parts, k)[0][TOK:, :], pick, (((0,), (0,)), ((), ())),
            preferred_element_type=F32,
        )
        means[k] = m
        total += m
    for k in range(NX):
        means[k] = means[k] - total / NX

    def shifted_part(k, rows):
        ref, owner = part_of(parts, k)
        v = ref[rows, :].astype(F32)
        shift = means[k, rows, :]
        return jnp.concatenate([v[:, :128] + shift, v[:, 128:] + shift], axis=1), owner

    def squares(i, _):
        rows = pl.ds(pl.multiple_of(i * 16, 16), 16)
        square = jnp.zeros((16, 128), F32)
        for k in range(NX):
            v, _ = shifted_part(k, rows)
            sq = v * v
            square += sq[:, :128] + sq[:, 128:]
        scale[rows, :] = square
        return 0

    lax.fori_loop(0, TOK // 16, squares, 0, unroll=2)
    spread = jnp.sum(scale[...], axis=1, keepdims=True) / C
    scale[...] = jnp.broadcast_to(lax.rsqrt(spread + 1e-05), (TOK, 128))
    gains = []
    for k in range(NX):
        tail = part_of(parts, k)[0][TOK:, :].astype(F32)
        gains.append(tail[3:4] + tail[4:5] + tail[5:6])

    def activate(i, _):
        rows = pl.ds(pl.multiple_of(i * 16, 16), 16)
        factor = jnp.concatenate([scale[rows, :]] * 2, axis=1)
        for k in range(NX):
            v, owner = shifted_part(k, rows)
            u = v * factor * gains[k]
            acts[owner, rows, :] = (u / (1.0 + jnp.exp(-u))).astype(BF)
        return 0

    lax.fori_loop(0, TOK // 16, activate, 0, unroll=2)
    weights.wait()
    branch = jnp.zeros((TOK, FEAT), F32)
    for k in range(NX):
        branch += lax.dot_general(
            acts[k], wt[k].reshape(FEAT, CH), (((1,), (1,)), ((), ())),
            preferred_element_type=F32,
        )
    fetch.wait()
    new = (held[...].astype(F32) + branch).astype(BF)
    if len(out.shape) == 2:
        out[...] = new
    else:
        held[...] = new
        send_all(held, out, sems)


def in_hbm(v):
    return v if INTERPRET else pltpu.with_memory_space_constraint(v, pltpu.HBM)


def call(body, out, ins, scratch, flops, place=pltpu.VMEM):
    spec = pl.BlockSpec(memory_space=place)
    return pl.pallas_call(
        body,
        out_shape=out,
        in_specs=[pl.BlockSpec(memory_space=pltpu.VMEM)] * len(ins),
        out_specs=spec,
        scratch_shapes=scratch,
        cost_estimate=pl.CostEstimate(flops=flops, transcendentals=0, bytes_accessed=1 << 20),
        compiler_params=pltpu.CompilerParams(vmem_limit_bytes=14 << 20),
        interpret=INTERPRET,
    )(*ins)


def normalise(layer, parts, gain, far):
    def body(*refs):
        norm_kernel(layer, len(parts), *refs)

    shape = (NX, parts[0].shape[-2], FEAT)
    scratch = [pltpu.VMEM((shape[1], 128), F32)]
    if far:
        scratch += [pltpu.VMEM(shape, BF), pltpu.SemaphoreType.DMA(())]
    return call(
        body,
        pltpu.HBM(shape, BF) if far else jax.ShapeDtypeStruct(shape, BF),
        [*parts, gain],
        scratch,
        8 * NX * TOK * FEAT,
        pltpu.HBM if far else pltpu.VMEM,
    )


def mix(xs, mine, other, far):
    weights = pltpu.VMEM((NZ, NY, 2, 16, CH), BF)
    scratch = [weights, weights, pltpu.VMEM(other.shape, BF), pltpu.SemaphoreType.DMA((2,))]
    spots = [pltpu.HBM if far else pltpu.VMEM, pltpu.VMEM, pltpu.HBM]
    return pl.pallas_call(
        mix_kernel,
        out_shape=jax.ShapeDtypeStruct((xs.shape[1], CH), BF),
        in_specs=[pl.BlockSpec(memory_space=spot) for spot in spots],
        out_specs=pl.BlockSpec(memory_space=pltpu.VMEM),
        scratch_shapes=scratch + ([pltpu.VMEM(xs.shape, BF)] if far else []),
        cost_estimate=pl.CostEstimate(
            flops=4 * NX * TOK * FEAT * CH, transcendentals=0, bytes_accessed=1 << 20
        ),
        compiler_params=pltpu.CompilerParams(vmem_limit_bytes=14 << 20),
        interpret=INTERPRET,
    )(in_hbm(xs) if far else xs, mine, in_hbm(other))


def arrange_kernel(mine, other, out, wt, sem):
    def fill(halves):
        for k in range(NX):
            for c, w in enumerate(halves):
                wt[k, :, :, c] = w[2 * k : 2 * k + 2, :, 32:, :]

    @pl.when(core_here() == 0)
    def _():
        fill((mine, other))

    @pl.when(core_here() == 1)
    def _():
        fill((other, mine))

    done = pltpu.make_async_copy(wt, out, sem)
    done.start()
    done.wait()


def arrange(mine, other):
    shape = (NX, 2, NY, 2, 16, CH)
    return call(
        arrange_kernel,
        pltpu.HBM(shape, BF),
        [mine, other],
        [pltpu.VMEM(shape, BF), pltpu.SemaphoreType.DMA(())],
        1 << 26,
        pltpu.HBM,
    )


def conv_late(layer, glu, taps):
    def body(*refs):
        late_kernel(layer, *refs)

    return call(
        body,
        jax.ShapeDtypeStruct((HALF, CH), F32),
        [glu, taps],
        [pltpu.VMEM((TOK, CH), F32), pltpu.VMEM((8, SPAN, CH), F32)],
        2 * HALF * CH * TAPS,
    )


def conv_whole(layer, glu, taps, gain):
    def body(*refs):
        whole_kernel(layer, *refs)

    return call(
        body,
        jax.ShapeDtypeStruct((PACK, CH), BF),
        [glu, taps, gain],
        [
            pltpu.VMEM((TAPS + TOK, CH), F32),
            pltpu.VMEM((8, TOK + TAPS - 8, CH), F32),
            pltpu.VMEM((TOK, CH), F32),
        ],
        2 * TOK * CH * TAPS,
    )


def convolve(layer, before, glu, late, taps, gain):
    def body(*refs):
        conv_kernel(layer, *refs)

    return call(
        body,
        pltpu.HBM((NX, PACK, CH), BF),
        [before, glu, late, taps, gain],
        [
            pltpu.VMEM((TAPS + HALF, CH), F32),
            pltpu.VMEM((8, SPAN, CH), F32),
            pltpu.VMEM((TOK, CH), F32),
            pltpu.VMEM((PACK, CH), BF),
            pltpu.SemaphoreType.DMA((NX,)),
        ],
        2 * HALF * CH * TAPS,
        pltpu.HBM,
    )


def spread(layer, once):
    def body(*refs):
        spread_kernel(layer, *refs)

    return call(
        body,
        pltpu.HBM((NZ, NZ, 48, CH), BF),
        [once],
        [pltpu.SemaphoreType.DMA((NZ,))],
        1 << 26,
        pltpu.HBM,
    )


def project(parts, x, wt, to_all):
    def body(*refs):
        out_kernel(len(parts), *refs)

    shape = jax.ShapeDtypeStruct((TOK, FEAT), BF)
    copies = pltpu.HBM((NX, TOK, FEAT), BF)
    inside, far = pl.BlockSpec(memory_space=pltpu.VMEM), pl.BlockSpec(memory_space=pltpu.HBM)
    return pl.pallas_call(
        body,
        out_shape=copies if to_all else shape,
        in_specs=[inside] * len(parts) + [far, far],
        out_specs=far if to_all else inside,
        scratch_shapes=[
            pltpu.VMEM((NX, TOK, 128), F32),
            pltpu.VMEM((TOK, 128), F32),
            pltpu.VMEM((NX, TOK, CH), BF),
            pltpu.VMEM((TOK, FEAT), BF),
            pltpu.VMEM(wt.shape, BF),
            pltpu.SemaphoreType.DMA((NX,)),
        ],
        cost_estimate=pl.CostEstimate(
            flops=2 * NX * TOK * CH * FEAT, transcendentals=0, bytes_accessed=1 << 20
        ),
        compiler_params=pltpu.CompilerParams(vmem_limit_bytes=14 << 20),
        interpret=INTERPRET,
    )(*parts, in_hbm(x), in_hbm(wt))


def shards(stream, norm_gain, w_value, w_gate, conv_taps, channel_gain, w_out):
    gain = norm_gain.reshape(LAYERS * NX, 1, FEAT)
    out_t = to_column_owner(jnp.swapaxes(w_out, 1, 2))
    blocks = jnp.concatenate([w_value, w_gate, out_t], axis=1)

    x = stream
    count = lax.axis_size("sp")
    chain = [(i, i + 1) for i in range(count - 1)]
    extended = jnp.concatenate([lax.ppermute(x, "sp", chain)[TOK - TAPS :], x])
    once = lines(blocks)
    extended = after(extended, blocks)
    parts = [extended, along_x(extended, 2)]
    parts[1:1] = [along_x(extended, 1)]
    parts.append(along_x(extended, 3))
    ready = spread(0, once)
    gathered = plane(ready)
    ready = spread(1, once)
    normed = normalise(0, parts, gain, True)
    other = swap_cores(gathered)
    following = plane(after(ready, gathered))
    glu = mix(normed, gathered, other, True)
    packed = conv_whole(0, glu, conv_taps, channel_gain)
    parts = from_all_x(packed)
    wt = arrange(after(gathered, packed), other)
    copies = project(parts, x, wt, True)

    xs = exchange_x(copies)
    other = swap_cores(following)
    normed = normalise(1, xs, gain, False)
    glu = mix(normed, following, other, False)
    before = lax.ppermute(glu[TOK - TAPS :], "sp", chain)
    late = conv_late(1, glu, conv_taps)
    copies = convolve(1, before, glu, late, conv_taps, channel_gain)
    parts = exchange_x(copies)
    wt = arrange(after(following, copies), other)
    x = project(parts, xs[0], wt, False)
    return x


def solution(mesh):
    flat = Mesh(mesh.devices, ("sp", "x"))
    in_specs = (
        P("sp", "x"),
        P(),
        P(None, "sp", "x"),
        P(None, "sp", "x"),
        P(None, None, "x"),
        P(None, "x"),
        P(None, "x", "sp"),
    )

    return jax.shard_map(shards, mesh=flat, in_specs=in_specs, out_specs=P("sp", "x"), check_vma=False)
```

```python
import jax
import jax.numpy as jnp
from jax import lax
from jax.experimental import pallas as pl
from jax.experimental.pallas import tpu as pltpu
from jax.sharding import Mesh
from jax.sharding import PartitionSpec as P


C = 1024
LAYERS = 2
NZ, NY, NX = 8, 8, 4
TOK, CH, TAPS, FEAT = 256, 256, 128, 512
PACK = TOK + 16
HALF = TOK // 2
SPAN = HALF + TAPS - 8
BF = jnp.bfloat16
F32 = jnp.float32
INTERPRET = False


def at(z, y, c):
    return (z * NY + y) * 2 + c


ALONG_Y = [[at(z, y, 0) for y in range(NY)] for z in range(NZ)]
ALONG_Z = [[at(z, y, 1) for z in range(NZ)] for y in range(NY)]
ALONG_Y1 = [[at(z, y, 1) for y in range(NY)] for z in range(NZ)]
ALONG_Z0 = [[at(z, y, 0) for z in range(NZ)] for y in range(NY)]


def to_group(block, groups):
    n = len(groups[0])
    copies = jnp.broadcast_to(block, (n, *block.shape))
    return lax.all_to_all(
        copies, "sp", split_axis=0, concat_axis=0, tiled=True, axis_index_groups=groups
    )


def lines(block):
    return to_group(block, ALONG_Y + ALONG_Z)


def plane(copies):
    return lax.all_to_all(
        copies, "sp", split_axis=0, concat_axis=0, tiled=True,
        axis_index_groups=ALONG_Z0 + ALONG_Y1,
    )


def after(v, earlier):
    return lax.optimization_barrier((v, earlier))[0]


def swap_cores(v):
    count = lax.axis_size("sp")
    return lax.ppermute(v, "sp", [(i, i ^ 1) for i in range(count)])


def to_column_owner(v):
    nb = NZ // NX
    pairs = []
    for z in range(NZ):
        a, b = divmod(z, nb)
        for y in range(NY):
            for c in range(2):
                for x in range(NX):
                    place = (x * nb + b, y) if c == 0 else (y, x * nb + b)
                    pairs.append((at(z, y, c) * NX + x, at(*place, c) * NX + a))
    return lax.ppermute(v, ("sp", "x"), pairs)


def along_x(v, step):
    return lax.ppermute(v, "x", [(i, (i + step) % NX) for i in range(NX)])


def from_all_x(v):
    two = along_x(v, 2)
    return [v, along_x(v, 1), two, along_x(v, 3)]


def exchange_x(copies):
    return [lax.all_to_all(copies, "x", split_axis=0, concat_axis=0, tiled=True)]


def part_of(refs, k):
    if len(refs) == 1:
        return refs[0].at[k], k
    return refs[k], (lax.axis_index("x") + NX - k) % NX


def core_here():
    return lax.axis_index("sp") % 2


def norm_kernel(layer, n, *refs):
    parts, (gain, xs, scale, *spare) = refs[:n], refs[n:]
    out = xs
    if spare:
        xs = spare[0]

    def squares(i, _):
        rows = pl.ds(pl.multiple_of(i * 16, 16), 16)
        total = jnp.zeros((16, 128), F32)
        for k in range(NX):
            v = part_of(parts, k)[0][rows, :].astype(F32)
            sq = v * v
            for q in range(FEAT // 128):
                total += sq[:, q * 128 : (q + 1) * 128]
        scale[rows, :] = total
        return 0

    steps = scale.shape[0] // 16
    lax.fori_loop(0, steps, squares, 0, unroll=2)
    mean = jnp.sum(scale[...], axis=1, keepdims=True) / (NX * FEAT)
    scale[...] = jnp.broadcast_to(lax.rsqrt(mean + 1e-06), scale.shape)

    def apply(i, _):
        rows = pl.ds(pl.multiple_of(i * 16, 16), 16)
        factor = jnp.concatenate([scale[rows, :]] * (FEAT // 128), axis=1)
        for k in range(NX):
            ref, owner = part_of(parts, k)
            xs[owner, rows, :] = (ref[rows, :].astype(F32) * factor * gain[layer * NX + owner]).astype(BF)
        return 0

    lax.fori_loop(0, steps, apply, 0, unroll=2)
    if spare:
        done = pltpu.make_async_copy(xs, out, spare[1])
        done.start()
        done.wait()


def mix_kernel(held, gain, mine, source, glu, vs, gs, other, sems, xs, *spare):
    copies = [pltpu.make_async_copy(source, other, sems.at[0])]
    if not spare:
        copies.append(pltpu.make_async_copy(held, xs, sems.at[1]))
    for one in copies:
        one.start()
    if spare:
        norm_kernel(1, 1, held, gain, xs, spare[0])

    def from_even(w):
        for z in range(NZ):
            vs[z, :, 0] = w[z, :, :16, :]
            gs[z, :, 0] = w[z, :, 16:32, :]

    def from_odd(w):
        for z in range(NZ):
            vs[z, :, 1] = w[:, z, :16, :]
            gs[z, :, 1] = w[:, z, 16:32, :]

    even = core_here() == 0
    pl.when(even)(lambda: from_even(mine))
    pl.when(jnp.logical_not(even))(lambda: from_odd(mine))
    for one in copies:
        one.wait()
    pl.when(even)(lambda: from_odd(other))
    pl.when(jnp.logical_not(even))(lambda: from_even(other))

    value = jnp.zeros(glu.shape, F32)
    gate = jnp.zeros(glu.shape, F32)
    for k in range(NX):
        planes = slice(2 * k, 2 * k + 2)
        value += jnp.dot(xs[k], vs[planes].reshape(FEAT, CH), preferred_element_type=F32)
        gate += jnp.dot(xs[k], gs[planes].reshape(FEAT, CH), preferred_element_type=F32)
    glu[...] = (value * jax.nn.sigmoid(gate)).astype(BF)


def split_three(v):
    hi = v.astype(BF).astype(F32)
    mid = (v - hi).astype(BF).astype(F32)
    return [hi, mid, v - hi - mid]


def send_all(src, out, sems):
    copies = [pltpu.make_async_copy(src, out.at[k], sems.at[k]) for k in range(out.shape[0])]
    for c in copies:
        c.start()
    for c in copies:
        c.wait()


def spread_kernel(layer, once, out, sems):
    send_all(once.at[:, layer], out, sems)


def taps_over(layer, ext, taps, conv, shifted):
    rows = conv.shape[0]
    for b in range(8):
        shifted[b] = ext[1 + b : 1 + b + rows + TAPS - 8, :]
    for lane in range(0, CH, 128):
        for base in range(0, rows, HALF):

            def step(a, acc):
                start = pl.multiple_of(a * 8, 8)
                tap = taps[layer, pl.ds(start, 8), lane : lane + 128]
                for b in range(8):
                    window = shifted[b, pl.ds(start + base, HALF), lane : lane + 128]
                    acc += window * tap[b : b + 1]
                return acc

            acc = lax.fori_loop(0, TAPS // 8, step, jnp.zeros((HALF, 128), F32))
            conv[base : base + HALF, lane : lane + 128] = acc


def pack(layer, conv, gain, out):
    ones = jnp.full((8, CH), 1.0 / CH, F32)
    means = lax.dot_general(
        ones, conv[...], (((1,), (1,)), ((), ())), precision=lax.Precision.HIGHEST,
        preferred_element_type=F32,
    )[:1]
    extra = split_three(means) + split_three(gain[layer : layer + 1, :])
    out[TOK:, :] = jnp.concatenate(extra + [jnp.zeros((10, CH), F32)], axis=0).astype(BF)
    v = conv[...]
    out[:TOK, :] = (v - jnp.mean(v, axis=1, keepdims=True)).astype(BF)


def whole_kernel(layer, glu, taps, gain, out, ext, shifted, conv):
    ext[...] = glu[...].astype(F32)
    taps_over(layer, ext, taps, conv, shifted)
    pack(layer, conv, gain, out)


def late_kernel(layer, glu, taps, conv, ext, shifted):
    ext[...] = glu[...].astype(F32)
    taps_over(layer, ext, taps, conv, shifted)


def conv_kernel(layer, before, glu, late, taps, gain, out, ext, shifted, conv, packed, sems):
    ext[:TAPS, :] = before[...].astype(F32)
    ext[TAPS:, :] = glu[:HALF, :].astype(F32)
    taps_over(layer, ext, taps, conv.at[:HALF], shifted)
    conv[HALF:, :] = late[...]
    pack(layer, conv, gain, packed)
    send_all(packed, out, sems)


def out_kernel(n, *refs):
    parts, rest = refs[:n], refs[n:]
    x, source, out, means, scale, acts, held, wt, sems = rest
    weights = pltpu.make_async_copy(source, wt, sems.at[1])
    weights.start()
    mine = x if len(x.shape) == 2 else x.at[lax.axis_index("x")]
    fetch = pltpu.make_async_copy(mine, held, sems.at[0])
    fetch.start()
    pick = (lax.broadcasted_iota(jnp.int32, (16, 128), 0) < 3).astype(BF)
    total = jnp.zeros((TOK, 128), F32)
    for k in range(NX):
        m = lax.dot_general(
            part_of(parts, k)[0][TOK:, :], pick, (((0,), (0,)), ((), ())),
            preferred_element_type=F32,
        )
        means[k] = m
        total += m
    for k in range(NX):
        means[k] = means[k] - total / NX

    def shifted_part(k, rows):
        ref, owner = part_of(parts, k)
        v = ref[rows, :].astype(F32)
        shift = means[k, rows, :]
        return jnp.concatenate([v[:, :128] + shift, v[:, 128:] + shift], axis=1), owner

    def squares(i, _):
        rows = pl.ds(pl.multiple_of(i * 16, 16), 16)
        square = jnp.zeros((16, 128), F32)
        for k in range(NX):
            v, _ = shifted_part(k, rows)
            sq = v * v
            square += sq[:, :128] + sq[:, 128:]
        scale[rows, :] = square
        return 0

    lax.fori_loop(0, TOK // 16, squares, 0, unroll=2)
    spread = jnp.sum(scale[...], axis=1, keepdims=True) / C
    scale[...] = jnp.broadcast_to(lax.rsqrt(spread + 1e-05), (TOK, 128))
    gains = []
    for k in range(NX):
        tail = part_of(parts, k)[0][TOK:, :].astype(F32)
        gains.append(tail[3:4] + tail[4:5] + tail[5:6])

    def activate(i, _):
        rows = pl.ds(pl.multiple_of(i * 16, 16), 16)
        factor = jnp.concatenate([scale[rows, :]] * 2, axis=1)
        for k in range(NX):
            v, owner = shifted_part(k, rows)
            u = v * factor * gains[k]
            acts[owner, rows, :] = (u / (1.0 + jnp.exp(-u))).astype(BF)
        return 0

    lax.fori_loop(0, TOK // 16, activate, 0, unroll=2)
    weights.wait()
    branch = jnp.zeros((TOK, FEAT), F32)
    for k in range(NX):
        branch += lax.dot_general(
            acts[k], wt[k].reshape(FEAT, CH), (((1,), (1,)), ((), ())),
            preferred_element_type=F32,
        )
    fetch.wait()
    new = (held[...].astype(F32) + branch).astype(BF)
    if len(out.shape) == 2:
        out[...] = new
    else:
        held[...] = new
        send_all(held, out, sems)


def in_hbm(v):
    return v if INTERPRET else pltpu.with_memory_space_constraint(v, pltpu.HBM)


def call(body, out, ins, scratch, flops, place=pltpu.VMEM):
    spec = pl.BlockSpec(memory_space=place)
    return pl.pallas_call(
        body,
        out_shape=out,
        in_specs=[pl.BlockSpec(memory_space=pltpu.VMEM)] * len(ins),
        out_specs=spec,
        scratch_shapes=scratch,
        cost_estimate=pl.CostEstimate(flops=flops, transcendentals=0, bytes_accessed=1 << 20),
        compiler_params=pltpu.CompilerParams(vmem_limit_bytes=14 << 20),
        interpret=INTERPRET,
    )(*ins)


def normalise(layer, parts, gain):
    def body(*refs):
        norm_kernel(layer, len(parts), *refs)

    shape = (NX, parts[0].shape[-2], FEAT)
    return call(
        body,
        pltpu.HBM(shape, BF),
        [*parts, gain],
        [pltpu.VMEM((shape[1], 128), F32), pltpu.VMEM(shape, BF), pltpu.SemaphoreType.DMA(())],
        8 * NX * TOK * FEAT,
        pltpu.HBM,
    )


def mix(xs, gain, mine, other, far):
    weights = pltpu.VMEM((NZ, NY, 2, 16, CH), BF)
    scratch = [weights, weights, pltpu.VMEM(other.shape, BF), pltpu.SemaphoreType.DMA((2,))]
    scratch.append(pltpu.VMEM(xs.shape, BF))
    if not far:
        scratch.append(pltpu.VMEM((TOK, 128), F32))
    spots = [pltpu.HBM if far else pltpu.VMEM, pltpu.VMEM, pltpu.VMEM, pltpu.HBM]
    return pl.pallas_call(
        mix_kernel,
        out_shape=jax.ShapeDtypeStruct((xs.shape[1], CH), BF),
        in_specs=[pl.BlockSpec(memory_space=spot) for spot in spots],
        out_specs=pl.BlockSpec(memory_space=pltpu.VMEM),
        scratch_shapes=scratch,
        cost_estimate=pl.CostEstimate(
            flops=4 * NX * TOK * FEAT * CH, transcendentals=0, bytes_accessed=1 << 20
        ),
        compiler_params=pltpu.CompilerParams(vmem_limit_bytes=14 << 20),
        interpret=INTERPRET,
    )(in_hbm(xs) if far else xs, gain, mine, in_hbm(other))


def arrange_kernel(mine, other, out, wt, sem):
    def fill(halves):
        for k in range(NX):
            for c, w in enumerate(halves):
                wt[k, :, :, c] = w[2 * k : 2 * k + 2, :, 32:, :]

    @pl.when(core_here() == 0)
    def _():
        fill((mine, other))

    @pl.when(core_here() == 1)
    def _():
        fill((other, mine))

    done = pltpu.make_async_copy(wt, out, sem)
    done.start()
    done.wait()


def arrange(mine, other):
    shape = (NX, 2, NY, 2, 16, CH)
    return call(
        arrange_kernel,
        pltpu.HBM(shape, BF),
        [mine, other],
        [pltpu.VMEM(shape, BF), pltpu.SemaphoreType.DMA(())],
        1 << 26,
        pltpu.HBM,
    )


def conv_late(layer, glu, taps):
    def body(*refs):
        late_kernel(layer, *refs)

    return call(
        body,
        jax.ShapeDtypeStruct((HALF, CH), F32),
        [glu, taps],
        [pltpu.VMEM((TOK, CH), F32), pltpu.VMEM((8, SPAN, CH), F32)],
        2 * HALF * CH * TAPS,
    )


def conv_whole(layer, glu, taps, gain):
    def body(*refs):
        whole_kernel(layer, *refs)

    return call(
        body,
        jax.ShapeDtypeStruct((PACK, CH), BF),
        [glu, taps, gain],
        [
            pltpu.VMEM((TAPS + TOK, CH), F32),
            pltpu.VMEM((8, TOK + TAPS - 8, CH), F32),
            pltpu.VMEM((TOK, CH), F32),
        ],
        2 * TOK * CH * TAPS,
    )


def convolve(layer, before, glu, late, taps, gain):
    def body(*refs):
        conv_kernel(layer, *refs)

    return call(
        body,
        pltpu.HBM((NX, PACK, CH), BF),
        [before, glu, late, taps, gain],
        [
            pltpu.VMEM((TAPS + HALF, CH), F32),
            pltpu.VMEM((8, SPAN, CH), F32),
            pltpu.VMEM((TOK, CH), F32),
            pltpu.VMEM((PACK, CH), BF),
            pltpu.SemaphoreType.DMA((NX,)),
        ],
        2 * HALF * CH * TAPS,
        pltpu.HBM,
    )


def spread(layer, once):
    def body(*refs):
        spread_kernel(layer, *refs)

    return call(
        body,
        pltpu.HBM((NZ, NZ, 48, CH), BF),
        [once],
        [pltpu.SemaphoreType.DMA((NZ,))],
        1 << 26,
        pltpu.HBM,
    )


def project(parts, x, wt, to_all):
    def body(*refs):
        out_kernel(len(parts), *refs)

    shape = jax.ShapeDtypeStruct((TOK, FEAT), BF)
    copies = pltpu.HBM((NX, TOK, FEAT), BF)
    inside, far = pl.BlockSpec(memory_space=pltpu.VMEM), pl.BlockSpec(memory_space=pltpu.HBM)
    return pl.pallas_call(
        body,
        out_shape=copies if to_all else shape,
        in_specs=[inside] * len(parts) + [far, far],
        out_specs=far if to_all else inside,
        scratch_shapes=[
            pltpu.VMEM((NX, TOK, 128), F32),
            pltpu.VMEM((TOK, 128), F32),
            pltpu.VMEM((NX, TOK, CH), BF),
            pltpu.VMEM((TOK, FEAT), BF),
            pltpu.VMEM(wt.shape, BF),
            pltpu.SemaphoreType.DMA((NX,)),
        ],
        cost_estimate=pl.CostEstimate(
            flops=2 * NX * TOK * CH * FEAT, transcendentals=0, bytes_accessed=1 << 20
        ),
        compiler_params=pltpu.CompilerParams(vmem_limit_bytes=14 << 20),
        interpret=INTERPRET,
    )(*parts, in_hbm(x), in_hbm(wt))


def shards(stream, norm_gain, w_value, w_gate, conv_taps, channel_gain, w_out):
    gain = norm_gain.reshape(LAYERS * NX, 1, FEAT)
    out_t = to_column_owner(jnp.swapaxes(w_out, 1, 2))
    blocks = jnp.concatenate([w_value, w_gate, out_t], axis=1)

    x = stream
    count = lax.axis_size("sp")
    chain = [(i, i + 1) for i in range(count - 1)]
    extended = jnp.concatenate([lax.ppermute(x, "sp", chain)[TOK - TAPS :], x])
    once = lines(blocks)
    extended = after(extended, blocks)
    parts = [extended, along_x(extended, 2)]
    parts[1:1] = [along_x(extended, 1)]
    parts.append(along_x(extended, 3))
    ready = spread(0, once)
    gathered = plane(ready)
    ready = spread(1, once)
    normed = normalise(0, parts, gain)
    other = swap_cores(gathered)
    following = plane(after(ready, gathered))
    glu = mix(normed, gain, gathered, other, True)
    packed = conv_whole(0, glu, conv_taps, channel_gain)
    parts = from_all_x(packed)
    wt = arrange(after(gathered, packed), other)
    copies = project(parts, x, wt, True)

    xs = exchange_x(copies)
    other = swap_cores(following)
    glu = mix(xs[0], gain, following, other, False)
    before = lax.ppermute(glu[TOK - TAPS :], "sp", chain)
    late = conv_late(1, glu, conv_taps)
    copies = convolve(1, before, glu, late, conv_taps, channel_gain)
    parts = exchange_x(copies)
    wt = arrange(after(following, copies), other)
    x = project(parts, xs[0], wt, False)
    return x


def solution(mesh):
    flat = Mesh(mesh.devices, ("sp", "x"))
    in_specs = (
        P("sp", "x"),
        P(),
        P(None, "sp", "x"),
        P(None, "sp", "x"),
        P(None, None, "x"),
        P(None, "x"),
        P(None, "x", "sp"),
    )

    return jax.shard_map(shards, mesh=flat, in_specs=in_specs, out_specs=P("sp", "x"), check_vma=False)
```

```python
import jax
import jax.numpy as jnp
from jax import lax
from jax.experimental import pallas as pl
from jax.experimental.pallas import tpu as pltpu
from jax.sharding import Mesh
from jax.sharding import PartitionSpec as P


C = 1024
LAYERS = 2
NZ, NY, NX = 8, 8, 4
TOK, CH, TAPS, FEAT = 256, 256, 128, 512
PACK = TOK + 16
HALF = TOK // 2
SPAN = HALF + TAPS - 8
BF = jnp.bfloat16
F32 = jnp.float32
INTERPRET = False


def at(z, y, c):
    return (z * NY + y) * 2 + c


ALONG_Y = [[at(z, y, 0) for y in range(NY)] for z in range(NZ)]
ALONG_Z = [[at(z, y, 1) for z in range(NZ)] for y in range(NY)]
ALONG_Y1 = [[at(z, y, 1) for y in range(NY)] for z in range(NZ)]
ALONG_Z0 = [[at(z, y, 0) for z in range(NZ)] for y in range(NY)]


def to_group(block, groups):
    n = len(groups[0])
    copies = jnp.broadcast_to(block, (n, *block.shape))
    return lax.all_to_all(
        copies, "sp", split_axis=0, concat_axis=0, tiled=True, axis_index_groups=groups
    )


def lines(block):
    return to_group(block, ALONG_Y + ALONG_Z)


def plane(copies):
    return lax.all_to_all(
        copies, "sp", split_axis=0, concat_axis=0, tiled=True,
        axis_index_groups=ALONG_Z0 + ALONG_Y1,
    )


def after(v, earlier):
    return lax.optimization_barrier((v, earlier))[0]


def swap_cores(v):
    count = lax.axis_size("sp")
    return lax.ppermute(v, "sp", [(i, i ^ 1) for i in range(count)])


def to_column_owner(v):
    nb = NZ // NX
    pairs = []
    for z in range(NZ):
        a, b = divmod(z, nb)
        for y in range(NY):
            for c in range(2):
                for x in range(NX):
                    pairs.append((at(z, y, c) * NX + x, at(x * nb + b, y, c) * NX + a))
    return lax.ppermute(v, ("sp", "x"), pairs)


def along_x(v, step):
    return lax.ppermute(v, "x", [(i, (i + step) % NX) for i in range(NX)])


def from_all_x(v):
    two = along_x(v, 2)
    return [v, along_x(v, 1), two, along_x(v, 3)]


def exchange_x(copies):
    return [lax.all_to_all(copies, "x", split_axis=0, concat_axis=0, tiled=True)]


def part_of(refs, k):
    if len(refs) == 1:
        return refs[0].at[k], k
    return refs[k], (lax.axis_index("x") + NX - k) % NX


def core_here():
    return lax.axis_index("sp") % 2


def norm_kernel(layer, n, *refs):
    parts, (gain, xs, scale, *spare) = refs[:n], refs[n:]
    out = xs
    if spare:
        xs = spare[0]

    def squares(i, _):
        rows = pl.ds(pl.multiple_of(i * 16, 16), 16)
        total = jnp.zeros((16, 128), F32)
        for k in range(NX):
            v = part_of(parts, k)[0][rows, :].astype(F32)
            sq = v * v
            for q in range(FEAT // 128):
                total += sq[:, q * 128 : (q + 1) * 128]
        scale[rows, :] = total
        return 0

    steps = scale.shape[0] // 16
    lax.fori_loop(0, steps, squares, 0, unroll=2)
    mean = jnp.sum(scale[...], axis=1, keepdims=True) / (NX * FEAT)
    scale[...] = jnp.broadcast_to(lax.rsqrt(mean + 1e-06), scale.shape)

    def apply(i, _):
        rows = pl.ds(pl.multiple_of(i * 16, 16), 16)
        factor = jnp.concatenate([scale[rows, :]] * (FEAT // 128), axis=1)
        for k in range(NX):
            ref, owner = part_of(parts, k)
            xs[owner, rows, :] = (ref[rows, :].astype(F32) * factor * gain[layer * NX + owner]).astype(BF)
        return 0

    lax.fori_loop(0, steps, apply, 0, unroll=2)
    if spare:
        done = pltpu.make_async_copy(xs, out, spare[1])
        done.start()
        done.wait()


def mix_kernel(held, gain, mine, source, glu, vs, gs, other, sems, xs, *spare):
    copies = [pltpu.make_async_copy(source, other, sems.at[0])]
    if not spare:
        copies.append(pltpu.make_async_copy(held, xs, sems.at[1]))
    for one in copies:
        one.start()
    if spare:
        norm_kernel(1, 1, held, gain, xs, spare[0])

    def from_even(w):
        for z in range(NZ):
            vs[z, :, 0] = w[z, :, :16, :]
            gs[z, :, 0] = w[z, :, 16:32, :]

    def from_odd(w):
        for z in range(NZ):
            vs[z, :, 1] = w[:, z, :16, :]
            gs[z, :, 1] = w[:, z, 16:32, :]

    even = core_here() == 0
    pl.when(even)(lambda: from_even(mine))
    pl.when(jnp.logical_not(even))(lambda: from_odd(mine))
    for one in copies:
        one.wait()
    pl.when(even)(lambda: from_odd(other))
    pl.when(jnp.logical_not(even))(lambda: from_even(other))

    value = jnp.zeros(glu.shape, F32)
    gate = jnp.zeros(glu.shape, F32)
    for k in range(NX):
        planes = slice(2 * k, 2 * k + 2)
        value += jnp.dot(xs[k], vs[planes].reshape(FEAT, CH), preferred_element_type=F32)
        gate += jnp.dot(xs[k], gs[planes].reshape(FEAT, CH), preferred_element_type=F32)
    glu[...] = (value * jax.nn.sigmoid(gate)).astype(BF)


def split_three(v):
    hi = v.astype(BF).astype(F32)
    mid = (v - hi).astype(BF).astype(F32)
    return [hi, mid, v - hi - mid]


def send_all(src, out, sems):
    copies = [pltpu.make_async_copy(src, out.at[k], sems.at[k]) for k in range(out.shape[0])]
    for c in copies:
        c.start()
    for c in copies:
        c.wait()


def spread_kernel(layer, once, out, sems):
    send_all(once.at[:, layer], out, sems)


def taps_over(layer, ext, taps, conv, shifted):
    rows = conv.shape[0]
    for b in range(8):
        shifted[b] = ext[1 + b : 1 + b + rows + TAPS - 8, :]
    for lane in range(0, CH, 128):
        for base in range(0, rows, HALF):

            def step(a, acc):
                start = pl.multiple_of(a * 8, 8)
                tap = taps[layer, pl.ds(start, 8), lane : lane + 128]
                for b in range(8):
                    window = shifted[b, pl.ds(start + base, HALF), lane : lane + 128]
                    acc += window * tap[b : b + 1]
                return acc

            acc = lax.fori_loop(0, TAPS // 8, step, jnp.zeros((HALF, 128), F32))
            conv[base : base + HALF, lane : lane + 128] = acc


def pack(layer, conv, gain, out):
    ones = jnp.full((8, CH), 1.0 / CH, F32)
    means = lax.dot_general(
        ones, conv[...], (((1,), (1,)), ((), ())), precision=lax.Precision.HIGHEST,
        preferred_element_type=F32,
    )[:1]
    extra = split_three(means) + split_three(gain[layer : layer + 1, :])
    out[TOK:, :] = jnp.concatenate(extra + [jnp.zeros((10, CH), F32)], axis=0).astype(BF)
    v = conv[...]
    out[:TOK, :] = (v - jnp.mean(v, axis=1, keepdims=True)).astype(BF)


def whole_kernel(layer, glu, taps, gain, out, ext, shifted, conv):
    ext[...] = glu[...].astype(F32)
    taps_over(layer, ext, taps, conv, shifted)
    pack(layer, conv, gain, out)


def late_kernel(layer, glu, taps, conv, ext, shifted):
    ext[...] = glu[...].astype(F32)
    taps_over(layer, ext, taps, conv, shifted)


def conv_kernel(layer, before, glu, late, taps, gain, out, ext, shifted, conv, packed, sems):
    ext[:TAPS, :] = before[...].astype(F32)
    ext[TAPS:, :] = glu[:HALF, :].astype(F32)
    taps_over(layer, ext, taps, conv.at[:HALF], shifted)
    conv[HALF:, :] = late[...]
    pack(layer, conv, gain, packed)
    send_all(packed, out, sems)


def out_kernel(n, *refs):
    parts, rest = refs[:n], refs[n:]
    x, source, out, means, scale, acts, held, wt, sems = rest
    weights = pltpu.make_async_copy(source, wt, sems.at[1])
    weights.start()
    mine = x if len(x.shape) == 2 else x.at[lax.axis_index("x")]
    fetch = pltpu.make_async_copy(mine, held, sems.at[0])
    fetch.start()
    pick = (lax.broadcasted_iota(jnp.int32, (16, 128), 0) < 3).astype(BF)
    total = jnp.zeros((TOK, 128), F32)
    for k in range(NX):
        m = lax.dot_general(
            part_of(parts, k)[0][TOK:, :], pick, (((0,), (0,)), ((), ())),
            preferred_element_type=F32,
        )
        means[k] = m
        total += m
    for k in range(NX):
        means[k] = means[k] - total / NX

    def shifted_part(k, rows):
        ref, owner = part_of(parts, k)
        v = ref[rows, :].astype(F32)
        shift = means[k, rows, :]
        return jnp.concatenate([v[:, :128] + shift, v[:, 128:] + shift], axis=1), owner

    def squares(i, _):
        rows = pl.ds(pl.multiple_of(i * 16, 16), 16)
        square = jnp.zeros((16, 128), F32)
        for k in range(NX):
            v, _ = shifted_part(k, rows)
            sq = v * v
            square += sq[:, :128] + sq[:, 128:]
        scale[rows, :] = square
        return 0

    lax.fori_loop(0, TOK // 16, squares, 0, unroll=2)
    spread = jnp.sum(scale[...], axis=1, keepdims=True) / C
    scale[...] = jnp.broadcast_to(lax.rsqrt(spread + 1e-05), (TOK, 128))
    gains = []
    for k in range(NX):
        tail = part_of(parts, k)[0][TOK:, :].astype(F32)
        gains.append(tail[3:4] + tail[4:5] + tail[5:6])

    def activate(i, _):
        rows = pl.ds(pl.multiple_of(i * 16, 16), 16)
        factor = jnp.concatenate([scale[rows, :]] * 2, axis=1)
        for k in range(NX):
            v, owner = shifted_part(k, rows)
            u = v * factor * gains[k]
            acts[owner, rows, :] = (u / (1.0 + jnp.exp(-u))).astype(BF)
        return 0

    lax.fori_loop(0, TOK // 16, activate, 0, unroll=2)
    weights.wait()
    branch = jnp.zeros((TOK, FEAT), F32)
    for k in range(NX):
        branch += lax.dot_general(
            acts[k], wt[k].reshape(FEAT, CH), (((1,), (1,)), ((), ())),
            preferred_element_type=F32,
        )
    fetch.wait()
    new = (held[...].astype(F32) + branch).astype(BF)
    if len(out.shape) == 2:
        out[...] = new
    else:
        held[...] = new
        send_all(held, out, sems)


def in_hbm(v):
    return v if INTERPRET else pltpu.with_memory_space_constraint(v, pltpu.HBM)


def call(body, out, ins, scratch, flops, place=pltpu.VMEM):
    spec = pl.BlockSpec(memory_space=place)
    return pl.pallas_call(
        body,
        out_shape=out,
        in_specs=[pl.BlockSpec(memory_space=pltpu.VMEM)] * len(ins),
        out_specs=spec,
        scratch_shapes=scratch,
        cost_estimate=pl.CostEstimate(flops=flops, transcendentals=0, bytes_accessed=1 << 20),
        compiler_params=pltpu.CompilerParams(vmem_limit_bytes=14 << 20),
        interpret=INTERPRET,
    )(*ins)


def normalise(layer, parts, gain):
    def body(*refs):
        norm_kernel(layer, len(parts), *refs)

    shape = (NX, parts[0].shape[-2], FEAT)
    return call(
        body,
        pltpu.HBM(shape, BF),
        [*parts, gain],
        [pltpu.VMEM((shape[1], 128), F32), pltpu.VMEM(shape, BF), pltpu.SemaphoreType.DMA(())],
        8 * NX * TOK * FEAT,
        pltpu.HBM,
    )


def mix(xs, gain, mine, other, far):
    weights = pltpu.VMEM((NZ, NY, 2, 16, CH), BF)
    scratch = [weights, weights, pltpu.VMEM(other.shape, BF), pltpu.SemaphoreType.DMA((2,))]
    scratch.append(pltpu.VMEM(xs.shape, BF))
    if not far:
        scratch.append(pltpu.VMEM((TOK, 128), F32))
    spots = [pltpu.HBM if far else pltpu.VMEM, pltpu.VMEM, pltpu.VMEM, pltpu.HBM]
    return pl.pallas_call(
        mix_kernel,
        out_shape=jax.ShapeDtypeStruct((xs.shape[1], CH), BF),
        in_specs=[pl.BlockSpec(memory_space=spot) for spot in spots],
        out_specs=pl.BlockSpec(memory_space=pltpu.VMEM),
        scratch_shapes=scratch,
        cost_estimate=pl.CostEstimate(
            flops=4 * NX * TOK * FEAT * CH, transcendentals=0, bytes_accessed=1 << 20
        ),
        compiler_params=pltpu.CompilerParams(vmem_limit_bytes=14 << 20),
        interpret=INTERPRET,
    )(in_hbm(xs) if far else xs, gain, mine, in_hbm(other))


def arrange_kernel(mine, other, out, wt, sem):
    def fill(zy, yz):
        for z in range(NZ):
            k, i = divmod(z, NZ // NX)
            wt[k, i, :, 0] = zy[z, :, 32:, :]
            wt[k, i, :, 1] = yz[:, z, 32:, :]

    @pl.when(core_here() == 0)
    def _():
        fill(mine, other)

    @pl.when(core_here() == 1)
    def _():
        fill(other, mine)

    done = pltpu.make_async_copy(wt, out, sem)
    done.start()
    done.wait()


def arrange(mine, other):
    shape = (NX, 2, NY, 2, 16, CH)
    return call(
        arrange_kernel,
        pltpu.HBM(shape, BF),
        [mine, other],
        [pltpu.VMEM(shape, BF), pltpu.SemaphoreType.DMA(())],
        1 << 26,
        pltpu.HBM,
    )


def conv_late(layer, glu, taps):
    def body(*refs):
        late_kernel(layer, *refs)

    return call(
        body,
        jax.ShapeDtypeStruct((HALF, CH), F32),
        [glu, taps],
        [pltpu.VMEM((TOK, CH), F32), pltpu.VMEM((8, SPAN, CH), F32)],
        2 * HALF * CH * TAPS,
    )


def conv_whole(layer, glu, taps, gain):
    def body(*refs):
        whole_kernel(layer, *refs)

    return call(
        body,
        jax.ShapeDtypeStruct((PACK, CH), BF),
        [glu, taps, gain],
        [
            pltpu.VMEM((TAPS + TOK, CH), F32),
            pltpu.VMEM((8, TOK + TAPS - 8, CH), F32),
            pltpu.VMEM((TOK, CH), F32),
        ],
        2 * TOK * CH * TAPS,
    )


def convolve(layer, before, glu, late, taps, gain):
    def body(*refs):
        conv_kernel(layer, *refs)

    return call(
        body,
        pltpu.HBM((NX, PACK, CH), BF),
        [before, glu, late, taps, gain],
        [
            pltpu.VMEM((TAPS + HALF, CH), F32),
            pltpu.VMEM((8, SPAN, CH), F32),
            pltpu.VMEM((TOK, CH), F32),
            pltpu.VMEM((PACK, CH), BF),
            pltpu.SemaphoreType.DMA((NX,)),
        ],
        2 * HALF * CH * TAPS,
        pltpu.HBM,
    )


def spread(layer, once):
    def body(*refs):
        spread_kernel(layer, *refs)

    return call(
        body,
        pltpu.HBM((NZ, NZ, 48, CH), BF),
        [once],
        [pltpu.SemaphoreType.DMA((NZ,))],
        1 << 26,
        pltpu.HBM,
    )


def project(parts, x, wt, to_all):
    def body(*refs):
        out_kernel(len(parts), *refs)

    shape = jax.ShapeDtypeStruct((TOK, FEAT), BF)
    copies = pltpu.HBM((NX, TOK, FEAT), BF)
    inside, far = pl.BlockSpec(memory_space=pltpu.VMEM), pl.BlockSpec(memory_space=pltpu.HBM)
    return pl.pallas_call(
        body,
        out_shape=copies if to_all else shape,
        in_specs=[inside] * len(parts) + [far, far],
        out_specs=far if to_all else inside,
        scratch_shapes=[
            pltpu.VMEM((NX, TOK, 128), F32),
            pltpu.VMEM((TOK, 128), F32),
            pltpu.VMEM((NX, TOK, CH), BF),
            pltpu.VMEM((TOK, FEAT), BF),
            pltpu.VMEM(wt.shape, BF),
            pltpu.SemaphoreType.DMA((NX,)),
        ],
        cost_estimate=pl.CostEstimate(
            flops=2 * NX * TOK * CH * FEAT, transcendentals=0, bytes_accessed=1 << 20
        ),
        compiler_params=pltpu.CompilerParams(vmem_limit_bytes=14 << 20),
        interpret=INTERPRET,
    )(*parts, in_hbm(x), in_hbm(wt))


def shards(stream, norm_gain, w_value, w_gate, conv_taps, channel_gain, w_out):
    gain = norm_gain.reshape(LAYERS * NX, 1, FEAT)
    out_t = to_column_owner(jnp.swapaxes(w_out, 1, 2))
    blocks = jnp.concatenate([w_value, w_gate, out_t], axis=1)

    x = stream
    count = lax.axis_size("sp")
    chain = [(i, i + 1) for i in range(count - 1)]
    extended = jnp.concatenate([lax.ppermute(x, "sp", chain)[TOK - TAPS :], x])
    once = lines(blocks)
    extended = after(extended, blocks)
    parts = [extended, along_x(extended, 2)]
    parts[1:1] = [along_x(extended, 1)]
    parts.append(along_x(extended, 3))
    ready = spread(0, once)
    gathered = plane(ready)
    ready = spread(1, once)
    normed = normalise(0, parts, gain)
    other = swap_cores(gathered)
    following = plane(after(ready, gathered))
    glu = mix(normed, gain, gathered, other, True)
    packed = conv_whole(0, glu, conv_taps, channel_gain)
    parts = from_all_x(packed)
    wt = arrange(after(gathered, packed), other)
    copies = project(parts, x, wt, True)

    xs = exchange_x(copies)
    other = swap_cores(following)
    glu = mix(xs[0], gain, following, other, False)
    before = lax.ppermute(glu[TOK - TAPS :], "sp", chain)
    late = conv_late(1, glu, conv_taps)
    copies = convolve(1, before, glu, late, conv_taps, channel_gain)
    parts = exchange_x(copies)
    wt = arrange(after(following, copies), other)
    x = project(parts, xs[0], wt, False)
    return x


def solution(mesh):
    flat = Mesh(mesh.devices, ("sp", "x"))
    in_specs = (
        P("sp", "x"),
        P(),
        P(None, "sp", "x"),
        P(None, "sp", "x"),
        P(None, None, "x"),
        P(None, "x"),
        P(None, "x", "sp"),
    )

    return jax.shard_map(shards, mesh=flat, in_specs=in_specs, out_specs=P("sp", "x"), check_vma=False)
```

```python
import jax
import jax.numpy as jnp
from jax import lax
from jax.experimental import pallas as pl
from jax.experimental.pallas import tpu as pltpu
from jax.sharding import Mesh
from jax.sharding import PartitionSpec as P


C = 1024
LAYERS = 2
NZ, NY, NX = 8, 8, 4
TOK, CH, TAPS, FEAT = 256, 256, 128, 512
PACK = TOK + 16
HALF = TOK // 2
SPAN = HALF + TAPS - 8
BF = jnp.bfloat16
F32 = jnp.float32
INTERPRET = False


def at(z, y, c):
    return (z * NY + y) * 2 + c


ALONG_Y = [[at(z, y, 0) for y in range(NY)] for z in range(NZ)]
ALONG_Z = [[at(z, y, 1) for z in range(NZ)] for y in range(NY)]
ALONG_Y1 = [[at(z, y, 1) for y in range(NY)] for z in range(NZ)]
ALONG_Z0 = [[at(z, y, 0) for z in range(NZ)] for y in range(NY)]


def to_group(block, groups):
    n = len(groups[0])
    copies = jnp.broadcast_to(block, (n, *block.shape))
    return lax.all_to_all(
        copies, "sp", split_axis=0, concat_axis=0, tiled=True, axis_index_groups=groups
    )


def lines(block):
    return to_group(block, ALONG_Y + ALONG_Z)


def plane(copies):
    return lax.all_to_all(
        copies, "sp", split_axis=0, concat_axis=0, tiled=True,
        axis_index_groups=ALONG_Z0 + ALONG_Y1,
    )


def after(v, earlier):
    return lax.optimization_barrier((v, earlier))[0]


def swap_cores(v):
    count = lax.axis_size("sp")
    return lax.ppermute(v, "sp", [(i, i ^ 1) for i in range(count)])


def to_column_owner(v):
    nb = NZ // NX
    pairs = []
    for z in range(NZ):
        a, b = divmod(z, nb)
        for y in range(NY):
            for c in range(2):
                for x in range(NX):
                    pairs.append((at(z, y, c) * NX + x, at(x * nb + b, y, c) * NX + a))
    return lax.ppermute(v, ("sp", "x"), pairs)


def along_x(v, step):
    return lax.ppermute(v, "x", [(i, (i + step) % NX) for i in range(NX)])


def from_all_x(v):
    two = along_x(v, 2)
    return [v, along_x(v, 1), two, along_x(v, 3)]


def exchange_x(copies):
    return [lax.all_to_all(copies, "x", split_axis=0, concat_axis=0, tiled=True)]


def part_of(refs, k):
    if len(refs) == 1:
        return refs[0].at[k], k
    return refs[k], (lax.axis_index("x") + NX - k) % NX


def core_here():
    return lax.axis_index("sp") % 2


def norm_kernel(layer, n, *refs):
    parts, (gain, xs, scale, *spare) = refs[:n], refs[n:]
    out = xs
    if spare:
        xs = spare[0]

    def squares(i, _):
        rows = pl.ds(pl.multiple_of(i * 16, 16), 16)
        total = jnp.zeros((16, 128), F32)
        for k in range(NX):
            v = part_of(parts, k)[0][rows, :].astype(F32)
            sq = v * v
            for q in range(FEAT // 128):
                total += sq[:, q * 128 : (q + 1) * 128]
        scale[rows, :] = total
        return 0

    steps = scale.shape[0] // 16
    lax.fori_loop(0, steps, squares, 0, unroll=2)
    mean = jnp.sum(scale[...], axis=1, keepdims=True) / (NX * FEAT)
    scale[...] = jnp.broadcast_to(lax.rsqrt(mean + 1e-06), scale.shape)

    def apply(i, _):
        rows = pl.ds(pl.multiple_of(i * 16, 16), 16)
        factor = jnp.concatenate([scale[rows, :]] * (FEAT // 128), axis=1)
        for k in range(NX):
            ref, owner = part_of(parts, k)
            xs[owner, rows, :] = (ref[rows, :].astype(F32) * factor * gain[layer * NX + owner]).astype(BF)
        return 0

    lax.fori_loop(0, steps, apply, 0, unroll=2)
    if spare:
        done = pltpu.make_async_copy(xs, out, spare[1])
        done.start()
        done.wait()


def mix_kernel(n, *refs):
    parts, rest = refs[:n], refs[n:]
    gain, mine, other, glu, vs, gs, xs, *spare = rest
    copies = []
    if len(spare) == 2:
        far, sems = spare
        copies.append(pltpu.make_async_copy(other, far, sems.at[0]))
        copies.append(pltpu.make_async_copy(parts[0], xs, sems.at[1]))
        other = far
    for one in copies:
        one.start()
    if not copies:
        norm_kernel(1, n, *parts, gain, xs, spare[0])

    def from_even(w):
        for z in range(NZ):
            vs[z, :, 0] = w[z, :, :16, :]
            gs[z, :, 0] = w[z, :, 16:32, :]

    def from_odd(w):
        for z in range(NZ):
            vs[z, :, 1] = w[:, z, :16, :]
            gs[z, :, 1] = w[:, z, 16:32, :]

    even = core_here() == 0
    pl.when(even)(lambda: from_even(mine))
    pl.when(jnp.logical_not(even))(lambda: from_odd(mine))
    for one in copies:
        one.wait()
    pl.when(even)(lambda: from_odd(other))
    pl.when(jnp.logical_not(even))(lambda: from_even(other))

    value = jnp.zeros(glu.shape, F32)
    gate = jnp.zeros(glu.shape, F32)
    for k in range(NX):
        planes = slice(2 * k, 2 * k + 2)
        value += jnp.dot(xs[k], vs[planes].reshape(FEAT, CH), preferred_element_type=F32)
        gate += jnp.dot(xs[k], gs[planes].reshape(FEAT, CH), preferred_element_type=F32)
    glu[...] = (value * jax.nn.sigmoid(gate)).astype(BF)


def split_three(v):
    hi = v.astype(BF).astype(F32)
    mid = (v - hi).astype(BF).astype(F32)
    return [hi, mid, v - hi - mid]


def send_all(src, out, sems):
    copies = [pltpu.make_async_copy(src, out.at[k], sems.at[k]) for k in range(out.shape[0])]
    for c in copies:
        c.start()
    for c in copies:
        c.wait()


def spread_kernel(layer, once, out, sems):
    send_all(once.at[:, layer], out, sems)


def taps_over(layer, ext, taps, conv, shifted):
    rows = conv.shape[0]
    for b in range(8):
        shifted[b] = ext[1 + b : 1 + b + rows + TAPS - 8, :]
    for lane in range(0, CH, 128):
        for base in range(0, rows, HALF):

            def step(a, acc):
                start = pl.multiple_of(a * 8, 8)
                tap = taps[layer, pl.ds(start, 8), lane : lane + 128]
                for b in range(8):
                    window = shifted[b, pl.ds(start + base, HALF), lane : lane + 128]
                    acc += window * tap[b : b + 1]
                return acc

            acc = lax.fori_loop(0, TAPS // 8, step, jnp.zeros((HALF, 128), F32))
            conv[base : base + HALF, lane : lane + 128] = acc


def pack(layer, conv, gain, out):
    ones = jnp.full((8, CH), 1.0 / CH, F32)
    means = lax.dot_general(
        ones, conv[...], (((1,), (1,)), ((), ())), precision=lax.Precision.HIGHEST,
        preferred_element_type=F32,
    )[:1]
    extra = split_three(means) + split_three(gain[layer : layer + 1, :])
    out[TOK:, :] = jnp.concatenate(extra + [jnp.zeros((10, CH), F32)], axis=0).astype(BF)
    v = conv[...]
    out[:TOK, :] = (v - jnp.mean(v, axis=1, keepdims=True)).astype(BF)


def whole_kernel(layer, glu, taps, gain, out, ext, shifted, conv):
    ext[...] = glu[...].astype(F32)
    taps_over(layer, ext, taps, conv, shifted)
    pack(layer, conv, gain, out)


def late_kernel(layer, glu, taps, conv, ext, shifted):
    ext[...] = glu[...].astype(F32)
    taps_over(layer, ext, taps, conv, shifted)


def conv_kernel(layer, before, glu, late, taps, gain, out, ext, shifted, conv, packed, sems):
    ext[:TAPS, :] = before[...].astype(F32)
    ext[TAPS:, :] = glu[:HALF, :].astype(F32)
    taps_over(layer, ext, taps, conv.at[:HALF], shifted)
    conv[HALF:, :] = late[...]
    pack(layer, conv, gain, packed)
    send_all(packed, out, sems)


def out_kernel(n, *refs):
    parts, rest = refs[:n], refs[n:]
    x, source, out, means, scale, acts, held, wt, sems = rest
    weights = pltpu.make_async_copy(source, wt, sems.at[1])
    weights.start()
    mine = x if len(x.shape) == 2 else x.at[lax.axis_index("x")]
    fetch = pltpu.make_async_copy(mine, held, sems.at[0])
    fetch.start()
    pick = (lax.broadcasted_iota(jnp.int32, (16, 128), 0) < 3).astype(BF)
    total = jnp.zeros((TOK, 128), F32)
    for k in range(NX):
        m = lax.dot_general(
            part_of(parts, k)[0][TOK:, :], pick, (((0,), (0,)), ((), ())),
            preferred_element_type=F32,
        )
        means[k] = m
        total += m
    for k in range(NX):
        means[k] = means[k] - total / NX

    def shifted_part(k, rows):
        ref, owner = part_of(parts, k)
        v = ref[rows, :].astype(F32)
        shift = means[k, rows, :]
        return jnp.concatenate([v[:, :128] + shift, v[:, 128:] + shift], axis=1), owner

    def squares(i, _):
        rows = pl.ds(pl.multiple_of(i * 16, 16), 16)
        square = jnp.zeros((16, 128), F32)
        for k in range(NX):
            v, _ = shifted_part(k, rows)
            sq = v * v
            square += sq[:, :128] + sq[:, 128:]
        scale[rows, :] = square
        return 0

    lax.fori_loop(0, TOK // 16, squares, 0, unroll=2)
    spread = jnp.sum(scale[...], axis=1, keepdims=True) / C
    scale[...] = jnp.broadcast_to(lax.rsqrt(spread + 1e-05), (TOK, 128))
    gains = []
    for k in range(NX):
        tail = part_of(parts, k)[0][TOK:, :].astype(F32)
        gains.append(tail[3:4] + tail[4:5] + tail[5:6])

    def activate(i, _):
        rows = pl.ds(pl.multiple_of(i * 16, 16), 16)
        factor = jnp.concatenate([scale[rows, :]] * 2, axis=1)
        for k in range(NX):
            v, owner = shifted_part(k, rows)
            u = v * factor * gains[k]
            acts[owner, rows, :] = (u / (1.0 + jnp.exp(-u))).astype(BF)
        return 0

    lax.fori_loop(0, TOK // 16, activate, 0, unroll=2)
    weights.wait()
    branch = jnp.zeros((TOK, FEAT), F32)
    for k in range(NX):
        branch += lax.dot_general(
            acts[k], wt[k].reshape(FEAT, CH), (((1,), (1,)), ((), ())),
            preferred_element_type=F32,
        )
    fetch.wait()
    new = (held[...].astype(F32) + branch).astype(BF)
    if len(out.shape) == 2:
        out[...] = new
    else:
        held[...] = new
        send_all(held, out, sems)


def in_hbm(v):
    return v if INTERPRET else pltpu.with_memory_space_constraint(v, pltpu.HBM)


def call(body, out, ins, scratch, flops, place=pltpu.VMEM):
    spec = pl.BlockSpec(memory_space=place)
    return pl.pallas_call(
        body,
        out_shape=out,
        in_specs=[pl.BlockSpec(memory_space=pltpu.VMEM)] * len(ins),
        out_specs=spec,
        scratch_shapes=scratch,
        cost_estimate=pl.CostEstimate(flops=flops, transcendentals=0, bytes_accessed=1 << 20),
        compiler_params=pltpu.CompilerParams(vmem_limit_bytes=14 << 20),
        interpret=INTERPRET,
    )(*ins)


def normalise(layer, parts, gain):
    def body(*refs):
        norm_kernel(layer, len(parts), *refs)

    shape = (NX, parts[0].shape[-2], FEAT)
    return call(
        body,
        pltpu.HBM(shape, BF),
        [*parts, gain],
        [pltpu.VMEM((shape[1], 128), F32), pltpu.VMEM(shape, BF), pltpu.SemaphoreType.DMA(())],
        8 * NX * TOK * FEAT,
        pltpu.HBM,
    )


def mix(parts, gain, mine, other, far):
    def body(*refs):
        mix_kernel(len(parts), *refs)

    rows = parts[0].shape[-2]
    weights = pltpu.VMEM((NZ, NY, 2, 16, CH), BF)
    scratch = [weights, weights, pltpu.VMEM((NX, rows, FEAT), BF)]
    if far:
        scratch += [pltpu.VMEM(other.shape, BF), pltpu.SemaphoreType.DMA((2,))]
    else:
        scratch.append(pltpu.VMEM((TOK, 128), F32))
    place = pltpu.HBM if far else pltpu.VMEM
    spots = [place] * len(parts) + [pltpu.VMEM, pltpu.VMEM, place]
    return pl.pallas_call(
        body,
        out_shape=jax.ShapeDtypeStruct((rows, CH), BF),
        in_specs=[pl.BlockSpec(memory_space=spot) for spot in spots],
        out_specs=pl.BlockSpec(memory_space=pltpu.VMEM),
        scratch_shapes=scratch,
        cost_estimate=pl.CostEstimate(
            flops=4 * NX * TOK * FEAT * CH, transcendentals=0, bytes_accessed=1 << 20
        ),
        compiler_params=pltpu.CompilerParams(vmem_limit_bytes=14 << 20),
        interpret=INTERPRET,
    )(*([in_hbm(v) for v in parts] if far else parts), gain, mine, in_hbm(other) if far else other)


def arrange_kernel(mine, other, out, wt, sem):
    def fill(zy, yz):
        for z in range(NZ):
            k, i = divmod(z, NZ // NX)
            wt[k, i, :, 0] = zy[z, :, 32:, :]
            wt[k, i, :, 1] = yz[:, z, 32:, :]

    @pl.when(core_here() == 0)
    def _():
        fill(mine, other)

    @pl.when(core_here() == 1)
    def _():
        fill(other, mine)

    done = pltpu.make_async_copy(wt, out, sem)
    done.start()
    done.wait()


def arrange(mine, other):
    shape = (NX, 2, NY, 2, 16, CH)
    return call(
        arrange_kernel,
        pltpu.HBM(shape, BF),
        [mine, other],
        [pltpu.VMEM(shape, BF), pltpu.SemaphoreType.DMA(())],
        1 << 26,
        pltpu.HBM,
    )


def conv_late(layer, glu, taps):
    def body(*refs):
        late_kernel(layer, *refs)

    return call(
        body,
        jax.ShapeDtypeStruct((HALF, CH), F32),
        [glu, taps],
        [pltpu.VMEM((TOK, CH), F32), pltpu.VMEM((8, SPAN, CH), F32)],
        2 * HALF * CH * TAPS,
    )


def conv_whole(layer, glu, taps, gain):
    def body(*refs):
        whole_kernel(layer, *refs)

    return call(
        body,
        jax.ShapeDtypeStruct((PACK, CH), BF),
        [glu, taps, gain],
        [
            pltpu.VMEM((TAPS + TOK, CH), F32),
            pltpu.VMEM((8, TOK + TAPS - 8, CH), F32),
            pltpu.VMEM((TOK, CH), F32),
        ],
        2 * TOK * CH * TAPS,
    )


def convolve(layer, before, glu, late, taps, gain):
    def body(*refs):
        conv_kernel(layer, *refs)

    return call(
        body,
        pltpu.HBM((NX, PACK, CH), BF),
        [before, glu, late, taps, gain],
        [
            pltpu.VMEM((TAPS + HALF, CH), F32),
            pltpu.VMEM((8, SPAN, CH), F32),
            pltpu.VMEM((TOK, CH), F32),
            pltpu.VMEM((PACK, CH), BF),
            pltpu.SemaphoreType.DMA((NX,)),
        ],
        2 * HALF * CH * TAPS,
        pltpu.HBM,
    )


def spread(layer, once):
    def body(*refs):
        spread_kernel(layer, *refs)

    return call(
        body,
        pltpu.HBM((NZ, NZ, 48, CH), BF),
        [once],
        [pltpu.SemaphoreType.DMA((NZ,))],
        1 << 26,
        pltpu.HBM,
    )


def project(parts, x, wt, to_all):
    def body(*refs):
        out_kernel(len(parts), *refs)

    shape = jax.ShapeDtypeStruct((TOK, FEAT), BF)
    copies = pltpu.HBM((NX, TOK, FEAT), BF)
    inside, far = pl.BlockSpec(memory_space=pltpu.VMEM), pl.BlockSpec(memory_space=pltpu.HBM)
    return pl.pallas_call(
        body,
        out_shape=copies if to_all else shape,
        in_specs=[inside] * len(parts) + [far, far],
        out_specs=far if to_all else inside,
        scratch_shapes=[
            pltpu.VMEM((NX, TOK, 128), F32),
            pltpu.VMEM((TOK, 128), F32),
            pltpu.VMEM((NX, TOK, CH), BF),
            pltpu.VMEM((TOK, FEAT), BF),
            pltpu.VMEM(wt.shape, BF),
            pltpu.SemaphoreType.DMA((NX,)),
        ],
        cost_estimate=pl.CostEstimate(
            flops=2 * NX * TOK * CH * FEAT, transcendentals=0, bytes_accessed=1 << 20
        ),
        compiler_params=pltpu.CompilerParams(vmem_limit_bytes=14 << 20),
        interpret=INTERPRET,
    )(*parts, in_hbm(x), in_hbm(wt))


def shards(stream, norm_gain, w_value, w_gate, conv_taps, channel_gain, w_out):
    gain = norm_gain.reshape(LAYERS * NX, 1, FEAT)
    out_t = to_column_owner(jnp.swapaxes(w_out, 1, 2))
    blocks = jnp.concatenate([w_value, w_gate, out_t], axis=1)

    x = stream
    count = lax.axis_size("sp")
    chain = [(i, i + 1) for i in range(count - 1)]
    extended = jnp.concatenate([lax.ppermute(x, "sp", chain)[TOK - TAPS :], x])
    once = lines(blocks)
    extended = after(extended, blocks)
    parts = [extended, along_x(extended, 2)]
    parts[1:1] = [along_x(extended, 1)]
    parts.append(along_x(extended, 3))
    ready = spread(0, once)
    gathered = plane(ready)
    ready = spread(1, once)
    normed = normalise(0, parts, gain)
    other = swap_cores(gathered)
    following = plane(after(ready, gathered))
    glu = mix([normed], gain, gathered, other, True)
    packed = conv_whole(0, glu, conv_taps, channel_gain)
    parts = from_all_x(packed)
    wt = arrange(after(gathered, packed), other)
    x = project(parts, x, wt, False)

    xs = from_all_x(x)
    other = swap_cores(following)
    glu = mix(xs, gain, following, other, False)
    before = lax.ppermute(glu[TOK - TAPS :], "sp", chain)
    late = conv_late(1, glu, conv_taps)
    wt = arrange(after(following, late), other)
    copies = convolve(1, before, glu, late, conv_taps, channel_gain)
    parts = exchange_x(copies)
    x = project(parts, x, wt, False)
    return x


def solution(mesh):
    flat = Mesh(mesh.devices, ("sp", "x"))
    in_specs = (
        P("sp", "x"),
        P(),
        P(None, "sp", "x"),
        P(None, "sp", "x"),
        P(None, None, "x"),
        P(None, "x"),
        P(None, "x", "sp"),
    )

    return jax.shard_map(shards, mesh=flat, in_specs=in_specs, out_specs=P("sp", "x"), check_vma=False)
```

```python
import jax
import jax.numpy as jnp
from jax import lax
from jax.experimental import pallas as pl
from jax.experimental.pallas import tpu as pltpu
from jax.sharding import Mesh
from jax.sharding import PartitionSpec as P


C = 1024
LAYERS = 2
NZ, NY, NX = 8, 8, 4
TOK, CH, TAPS, FEAT = 256, 256, 128, 512
PACK = TOK + 16
HALF = TOK // 2
SPAN = HALF + TAPS - 8
BF = jnp.bfloat16
F32 = jnp.float32
INTERPRET = False


def at(z, y, c):
    return (z * NY + y) * 2 + c


ALONG_Y = [[at(z, y, 0) for y in range(NY)] for z in range(NZ)]
ALONG_Z = [[at(z, y, 1) for z in range(NZ)] for y in range(NY)]
ALONG_Y1 = [[at(z, y, 1) for y in range(NY)] for z in range(NZ)]
ALONG_Z0 = [[at(z, y, 0) for z in range(NZ)] for y in range(NY)]


def to_group(block, groups):
    n = len(groups[0])
    copies = jnp.broadcast_to(block, (n, *block.shape))
    return lax.all_to_all(
        copies, "sp", split_axis=0, concat_axis=0, tiled=True, axis_index_groups=groups
    )


def lines(block):
    return to_group(block, ALONG_Y + ALONG_Z)


def plane(copies):
    return lax.all_to_all(
        copies, "sp", split_axis=0, concat_axis=0, tiled=True,
        axis_index_groups=ALONG_Z0 + ALONG_Y1,
    )


def after(v, earlier):
    return lax.optimization_barrier((v, earlier))[0]


def swap_cores(v):
    count = lax.axis_size("sp")
    return lax.ppermute(v, "sp", [(i, i ^ 1) for i in range(count)])


def to_column_owner(v):
    nb = NZ // NX
    pairs = []
    for z in range(NZ):
        a, b = divmod(z, nb)
        for y in range(NY):
            for c in range(2):
                for x in range(NX):
                    pairs.append((at(z, y, c) * NX + x, at(x * nb + b, y, c) * NX + a))
    return lax.ppermute(v, ("sp", "x"), pairs)


def along_x(v, step):
    return lax.ppermute(v, "x", [(i, (i + step) % NX) for i in range(NX)])


def from_all_x(v):
    two = along_x(v, 2)
    return [v, along_x(v, 1), two, along_x(v, 3)]


def exchange_x(copies):
    return [lax.all_to_all(copies, "x", split_axis=0, concat_axis=0, tiled=True)]


def part_of(refs, k):
    if len(refs) == 1:
        return refs[0].at[k], k
    return refs[k], (lax.axis_index("x") + NX - k) % NX


def core_here():
    return lax.axis_index("sp") % 2


def norm_kernel(layer, n, *refs):
    parts, (gain, xs, scale, *spare) = refs[:n], refs[n:]
    out = xs
    if spare:
        xs = spare[0]

    def squares(i, _):
        rows = pl.ds(pl.multiple_of(i * 16, 16), 16)
        total = jnp.zeros((16, 128), F32)
        for k in range(NX):
            v = part_of(parts, k)[0][rows, :].astype(F32)
            sq = v * v
            for q in range(FEAT // 128):
                total += sq[:, q * 128 : (q + 1) * 128]
        scale[rows, :] = total
        return 0

    steps = scale.shape[0] // 16
    lax.fori_loop(0, steps, squares, 0, unroll=2)
    mean = jnp.sum(scale[...], axis=1, keepdims=True) / (NX * FEAT)
    scale[...] = jnp.broadcast_to(lax.rsqrt(mean + 1e-06), scale.shape)

    def apply(i, _):
        rows = pl.ds(pl.multiple_of(i * 16, 16), 16)
        factor = jnp.concatenate([scale[rows, :]] * (FEAT // 128), axis=1)
        for k in range(NX):
            ref, owner = part_of(parts, k)
            xs[owner, rows, :] = (ref[rows, :].astype(F32) * factor * gain[layer * NX + owner]).astype(BF)
        return 0

    lax.fori_loop(0, steps, apply, 0, unroll=2)
    if spare:
        done = pltpu.make_async_copy(xs, out, spare[1])
        done.start()
        done.wait()


def mix_kernel(n, *refs):
    parts, rest = refs[:n], refs[n:]
    gain, mine, other, glu, vs, gs, xs, *spare = rest
    copies = []
    if len(spare) == 2:
        far, sems = spare
        copies.append(pltpu.make_async_copy(other, far, sems.at[0]))
        copies.append(pltpu.make_async_copy(parts[0], xs, sems.at[1]))
        other = far
    for one in copies:
        one.start()
    if not copies:
        norm_kernel(1, n, *parts, gain, xs, spare[0])

    def from_even(w):
        for z in range(NZ):
            vs[z, :, 0] = w[z, :, :16, :]
            gs[z, :, 0] = w[z, :, 16:32, :]

    def from_odd(w):
        for z in range(NZ):
            vs[z, :, 1] = w[:, z, :16, :]
            gs[z, :, 1] = w[:, z, 16:32, :]

    even = core_here() == 0
    pl.when(even)(lambda: from_even(mine))
    pl.when(jnp.logical_not(even))(lambda: from_odd(mine))
    for one in copies:
        one.wait()
    pl.when(even)(lambda: from_odd(other))
    pl.when(jnp.logical_not(even))(lambda: from_even(other))

    value = jnp.zeros(glu.shape, F32)
    gate = jnp.zeros(glu.shape, F32)
    for k in range(NX):
        planes = slice(2 * k, 2 * k + 2)
        value += jnp.dot(xs[k], vs[planes].reshape(FEAT, CH), preferred_element_type=F32)
        gate += jnp.dot(xs[k], gs[planes].reshape(FEAT, CH), preferred_element_type=F32)
    glu[...] = (value * jax.nn.sigmoid(gate)).astype(BF)


def split_three(v):
    hi = v.astype(BF).astype(F32)
    mid = (v - hi).astype(BF).astype(F32)
    return [hi, mid, v - hi - mid]


def send_all(src, out, sems):
    copies = [pltpu.make_async_copy(src, out.at[k], sems.at[k]) for k in range(out.shape[0])]
    for c in copies:
        c.start()
    for c in copies:
        c.wait()


def spread_kernel(layer, once, out, sems):
    send_all(once.at[:, layer], out, sems)


def taps_over(layer, ext, taps, conv, shifted):
    rows = conv.shape[0]
    for b in range(8):
        shifted[b] = ext[1 + b : 1 + b + rows + TAPS - 8, :]
    for lane in range(0, CH, 128):
        for base in range(0, rows, HALF):

            def step(a, acc):
                start = pl.multiple_of(a * 8, 8)
                tap = taps[layer, pl.ds(start, 8), lane : lane + 128]
                for b in range(8):
                    window = shifted[b, pl.ds(start + base, HALF), lane : lane + 128]
                    acc += window * tap[b : b + 1]
                return acc

            acc = lax.fori_loop(0, TAPS // 8, step, jnp.zeros((HALF, 128), F32), unroll=4)
            conv[base : base + HALF, lane : lane + 128] = acc


def pack(layer, conv, gain, out):
    ones = jnp.full((8, CH), 1.0 / CH, F32)
    means = lax.dot_general(
        ones, conv[...], (((1,), (1,)), ((), ())), precision=lax.Precision.HIGHEST,
        preferred_element_type=F32,
    )[:1]
    extra = split_three(means) + split_three(gain[layer : layer + 1, :])
    out[TOK:, :] = jnp.concatenate(extra + [jnp.zeros((10, CH), F32)], axis=0).astype(BF)
    v = conv[...]
    out[:TOK, :] = (v - jnp.mean(v, axis=1, keepdims=True)).astype(BF)


def whole_kernel(layer, glu, taps, gain, out, ext, shifted, conv):
    ext[...] = glu[...].astype(F32)
    taps_over(layer, ext, taps, conv, shifted)
    pack(layer, conv, gain, out)


def late_kernel(layer, glu, taps, conv, ext, shifted):
    ext[...] = glu[...].astype(F32)
    taps_over(layer, ext, taps, conv, shifted)


def conv_kernel(layer, before, glu, late, taps, gain, out, ext, shifted, conv, packed, sems):
    ext[:TAPS, :] = before[...].astype(F32)
    ext[TAPS:, :] = glu[:HALF, :].astype(F32)
    taps_over(layer, ext, taps, conv.at[:HALF], shifted)
    conv[HALF:, :] = late[...]
    pack(layer, conv, gain, packed)
    send_all(packed, out, sems)


def out_kernel(n, *refs):
    parts, rest = refs[:n], refs[n:]
    x, source, out, means, scale, acts, held, wt, sems = rest
    weights = pltpu.make_async_copy(source, wt, sems.at[1])
    weights.start()
    mine = x if len(x.shape) == 2 else x.at[lax.axis_index("x")]
    fetch = pltpu.make_async_copy(mine, held, sems.at[0])
    fetch.start()
    pick = (lax.broadcasted_iota(jnp.int32, (16, 128), 0) < 3).astype(BF)
    total = jnp.zeros((TOK, 128), F32)
    for k in range(NX):
        m = lax.dot_general(
            part_of(parts, k)[0][TOK:, :], pick, (((0,), (0,)), ((), ())),
            preferred_element_type=F32,
        )
        means[k] = m
        total += m
    for k in range(NX):
        means[k] = means[k] - total / NX

    def shifted_part(k, rows):
        ref, owner = part_of(parts, k)
        v = ref[rows, :].astype(F32)
        shift = means[k, rows, :]
        return jnp.concatenate([v[:, :128] + shift, v[:, 128:] + shift], axis=1), owner

    def squares(i, _):
        rows = pl.ds(pl.multiple_of(i * 16, 16), 16)
        square = jnp.zeros((16, 128), F32)
        for k in range(NX):
            v, _ = shifted_part(k, rows)
            sq = v * v
            square += sq[:, :128] + sq[:, 128:]
        scale[rows, :] = square
        return 0

    lax.fori_loop(0, TOK // 16, squares, 0, unroll=4)
    spread = jnp.sum(scale[...], axis=1, keepdims=True) / C
    scale[...] = jnp.broadcast_to(lax.rsqrt(spread + 1e-05), (TOK, 128))
    gains = []
    for k in range(NX):
        tail = part_of(parts, k)[0][TOK:, :].astype(F32)
        gains.append(tail[3:4] + tail[4:5] + tail[5:6])

    def activate(i, _):
        rows = pl.ds(pl.multiple_of(i * 16, 16), 16)
        factor = jnp.concatenate([scale[rows, :]] * 2, axis=1)
        for k in range(NX):
            v, owner = shifted_part(k, rows)
            u = v * factor * gains[k]
            acts[owner, rows, :] = (u / (1.0 + jnp.exp(-u))).astype(BF)
        return 0

    lax.fori_loop(0, TOK // 16, activate, 0, unroll=4)
    weights.wait()
    branch = jnp.zeros((TOK, FEAT), F32)
    for k in range(NX):
        branch += lax.dot_general(
            acts[k], wt[k].reshape(FEAT, CH), (((1,), (1,)), ((), ())),
            preferred_element_type=F32,
        )
    fetch.wait()
    new = (held[...].astype(F32) + branch).astype(BF)
    if len(out.shape) == 2:
        out[...] = new
    else:
        held[...] = new
        send_all(held, out, sems)


def in_hbm(v):
    return v if INTERPRET else pltpu.with_memory_space_constraint(v, pltpu.HBM)


def call(body, out, ins, scratch, flops, place=pltpu.VMEM):
    spec = pl.BlockSpec(memory_space=place)
    return pl.pallas_call(
        body,
        out_shape=out,
        in_specs=[pl.BlockSpec(memory_space=pltpu.VMEM)] * len(ins),
        out_specs=spec,
        scratch_shapes=scratch,
        cost_estimate=pl.CostEstimate(flops=flops, transcendentals=0, bytes_accessed=1 << 20),
        compiler_params=pltpu.CompilerParams(vmem_limit_bytes=14 << 20),
        interpret=INTERPRET,
    )(*ins)


def normalise(layer, parts, gain):
    def body(*refs):
        norm_kernel(layer, len(parts), *refs)

    shape = (NX, parts[0].shape[-2], FEAT)
    return call(
        body,
        pltpu.HBM(shape, BF),
        [*parts, gain],
        [pltpu.VMEM((shape[1], 128), F32), pltpu.VMEM(shape, BF), pltpu.SemaphoreType.DMA(())],
        8 * NX * TOK * FEAT,
        pltpu.HBM,
    )


def mix(parts, gain, mine, other, far):
    def body(*refs):
        mix_kernel(len(parts), *refs)

    rows = parts[0].shape[-2]
    weights = pltpu.VMEM((NZ, NY, 2, 16, CH), BF)
    scratch = [weights, weights, pltpu.VMEM((NX, rows, FEAT), BF)]
    if far:
        scratch += [pltpu.VMEM(other.shape, BF), pltpu.SemaphoreType.DMA((2,))]
    else:
        scratch.append(pltpu.VMEM((TOK, 128), F32))
    place = pltpu.HBM if far else pltpu.VMEM
    spots = [place] * len(parts) + [pltpu.VMEM, pltpu.VMEM, place]
    return pl.pallas_call(
        body,
        out_shape=jax.ShapeDtypeStruct((rows, CH), BF),
        in_specs=[pl.BlockSpec(memory_space=spot) for spot in spots],
        out_specs=pl.BlockSpec(memory_space=pltpu.VMEM),
        scratch_shapes=scratch,
        cost_estimate=pl.CostEstimate(
            flops=4 * NX * TOK * FEAT * CH, transcendentals=0, bytes_accessed=1 << 20
        ),
        compiler_params=pltpu.CompilerParams(vmem_limit_bytes=14 << 20),
        interpret=INTERPRET,
    )(*([in_hbm(v) for v in parts] if far else parts), gain, mine, in_hbm(other) if far else other)


def arrange_kernel(mine, other, out, wt, sem):
    def fill(zy, yz):
        for z in range(NZ):
            k, i = divmod(z, NZ // NX)
            wt[k, i, :, 0] = zy[z, :, 32:, :]
            wt[k, i, :, 1] = yz[:, z, 32:, :]

    @pl.when(core_here() == 0)
    def _():
        fill(mine, other)

    @pl.when(core_here() == 1)
    def _():
        fill(other, mine)

    done = pltpu.make_async_copy(wt, out, sem)
    done.start()
    done.wait()


def arrange(mine, other):
    shape = (NX, 2, NY, 2, 16, CH)
    return call(
        arrange_kernel,
        pltpu.HBM(shape, BF),
        [mine, other],
        [pltpu.VMEM(shape, BF), pltpu.SemaphoreType.DMA(())],
        1 << 26,
        pltpu.HBM,
    )


def conv_late(layer, glu, taps):
    def body(*refs):
        late_kernel(layer, *refs)

    return call(
        body,
        jax.ShapeDtypeStruct((HALF, CH), F32),
        [glu, taps],
        [pltpu.VMEM((TOK, CH), F32), pltpu.VMEM((8, SPAN, CH), F32)],
        2 * HALF * CH * TAPS,
    )


def conv_whole(layer, glu, taps, gain):
    def body(*refs):
        whole_kernel(layer, *refs)

    return call(
        body,
        jax.ShapeDtypeStruct((PACK, CH), BF),
        [glu, taps, gain],
        [
            pltpu.VMEM((TAPS + TOK, CH), F32),
            pltpu.VMEM((8, TOK + TAPS - 8, CH), F32),
            pltpu.VMEM((TOK, CH), F32),
        ],
        2 * TOK * CH * TAPS,
    )


def convolve(layer, before, glu, late, taps, gain):
    def body(*refs):
        conv_kernel(layer, *refs)

    return call(
        body,
        pltpu.HBM((NX, PACK, CH), BF),
        [before, glu, late, taps, gain],
        [
            pltpu.VMEM((TAPS + HALF, CH), F32),
            pltpu.VMEM((8, SPAN, CH), F32),
            pltpu.VMEM((TOK, CH), F32),
            pltpu.VMEM((PACK, CH), BF),
            pltpu.SemaphoreType.DMA((NX,)),
        ],
        2 * HALF * CH * TAPS,
        pltpu.HBM,
    )


def spread(layer, once):
    def body(*refs):
        spread_kernel(layer, *refs)

    return call(
        body,
        pltpu.HBM((NZ, NZ, 48, CH), BF),
        [once],
        [pltpu.SemaphoreType.DMA((NZ,))],
        1 << 26,
        pltpu.HBM,
    )


def project(parts, x, wt, to_all):
    def body(*refs):
        out_kernel(len(parts), *refs)

    shape = jax.ShapeDtypeStruct((TOK, FEAT), BF)
    copies = pltpu.HBM((NX, TOK, FEAT), BF)
    inside, far = pl.BlockSpec(memory_space=pltpu.VMEM), pl.BlockSpec(memory_space=pltpu.HBM)
    return pl.pallas_call(
        body,
        out_shape=copies if to_all else shape,
        in_specs=[inside] * len(parts) + [far, far],
        out_specs=far if to_all else inside,
        scratch_shapes=[
            pltpu.VMEM((NX, TOK, 128), F32),
            pltpu.VMEM((TOK, 128), F32),
            pltpu.VMEM((NX, TOK, CH), BF),
            pltpu.VMEM((TOK, FEAT), BF),
            pltpu.VMEM(wt.shape, BF),
            pltpu.SemaphoreType.DMA((NX,)),
        ],
        cost_estimate=pl.CostEstimate(
            flops=2 * NX * TOK * CH * FEAT, transcendentals=0, bytes_accessed=1 << 20
        ),
        compiler_params=pltpu.CompilerParams(vmem_limit_bytes=14 << 20),
        interpret=INTERPRET,
    )(*parts, in_hbm(x), in_hbm(wt))


def shards(stream, norm_gain, w_value, w_gate, conv_taps, channel_gain, w_out):
    gain = norm_gain.reshape(LAYERS * NX, 1, FEAT)
    out_t = to_column_owner(jnp.swapaxes(w_out, 1, 2))
    blocks = jnp.concatenate([w_value, w_gate, out_t], axis=1)

    x = stream
    count = lax.axis_size("sp")
    chain = [(i, i + 1) for i in range(count - 1)]
    extended = jnp.concatenate([lax.ppermute(x, "sp", chain)[TOK - TAPS :], x])
    once = lines(blocks)
    extended = after(extended, blocks)
    parts = [extended, along_x(extended, 2)]
    parts[1:1] = [along_x(extended, 1)]
    parts.append(along_x(extended, 3))
    ready = spread(0, once)
    gathered = plane(ready)
    ready = spread(1, once)
    normed = normalise(0, parts, gain)
    other = swap_cores(gathered)
    following = plane(after(ready, gathered))
    glu = mix([normed], gain, gathered, other, True)
    packed = conv_whole(0, glu, conv_taps, channel_gain)
    parts = from_all_x(packed)
    wt = arrange(after(gathered, packed), other)
    x = project(parts, x, wt, False)

    xs = from_all_x(x)
    other = swap_cores(following)
    glu = mix(xs, gain, following, other, False)
    before = lax.ppermute(glu[TOK - TAPS :], "sp", chain)
    late = conv_late(1, glu, conv_taps)
    wt = arrange(after(following, late), other)
    copies = convolve(1, before, glu, late, conv_taps, channel_gain)
    parts = exchange_x(copies)
    x = project(parts, x, wt, False)
    return x


def solution(mesh):
    flat = Mesh(mesh.devices, ("sp", "x"))
    in_specs = (
        P("sp", "x"),
        P(),
        P(None, "sp", "x"),
        P(None, "sp", "x"),
        P(None, None, "x"),
        P(None, "x"),
        P(None, "x", "sp"),
    )

    return jax.shard_map(shards, mesh=flat, in_specs=in_specs, out_specs=P("sp", "x"), check_vma=False)
```
